512 devices in a mesh: sp: 128 (over z, x, core), tp: 4 (over y).
Axes of the slice: x: 4, y: 4, z: 16, core: 2. Of those that a mesh axis runs over, the one named last changes fastest.
Arguments:
- tokens: bfloat16 [65536, 2048], P('sp', 'tp'), may hold values from -6 to 6
- norm_gain: float32 [2048], replicated, may hold values from 0.1 to 1.9
- proj_state: bfloat16 [2048, 1024], P('sp', 'tp'), may hold values from -0.125 to 0.125
- proj_value: bfloat16 [2048, 1024], P('sp', 'tp'), may hold values from -0.125 to 0.125
- proj_gate: bfloat16 [2048, 1024], P('sp', 'tp'), may hold values from -0.125 to 0.125
- eigen_real: float32 [64, 64], P('tp')
- eigen_imag: float32 [64, 64], P('tp')
- log_step: float32 [64], P('tp')
- decay_shift: float32 [64, 65536], P('tp', 'sp'), may hold values from -2.2 to 0
- state_input: float32 [2, 64, 16, 64], P(None, 'tp'), may hold values from -1 to 1
- state_readout_matrices: float32 [2, 64, 16, 64], P(None, 'tp'), may hold values from -0.5 to 0.5
- skip_gain: float32 [1024], P('tp'), may hold values from -5 to 5
- init_state: float32 [2, 64, 64], P(None, 'tp'), may hold values from -5 to 5
- conv_taps: float32 [31, 1024], P(None, 'tp')
- channel_gain: float32 [1024], P('tp'), may hold values from 0.1 to 1.9
- merge_state: bfloat16 [1024, 2048], P('tp', 'sp'), may hold values from -0.125 to 0.125
- merge_conv: bfloat16 [1024, 2048], P('tp', 'sp'), may hold values from -0.125 to 0.125
Outputs:
- mixed: bfloat16 [65536, 2048], P(('sp', 'tp'))
The draws below stay inside these ranges and needn't reach their ends.
All inputs are finite; a program needn't handle non-finite values.
Results may differ from the reference program's by a relative error of at most 0.011.
Values may be sent and summed in bfloat16 or wider, within the bound.
No kernel may reach another device: no remote copies, remote signals or barrier semaphores. Data moves between devices by JAX's collectives and lax.ppermute only.
A program may use at most 128 MiB of HBM per device.

```python
import math
import jax
import jax.numpy as jnp
from jax import lax

D = 2048
SSM_W = 1024
GROUP = 16
STATE = 64
CONV_W = 1024
KERNEL = 31
TOK_DEV = 512
GROUPS = 64
TOKENS = 65536
N_TP = 4


def speeds(key):
    base = jax.random.fold_in(key, 101)
    first, second, third = jax.random.split(base, 3)
    fast = jax.random.randint(first, (GROUPS,), 0, 2) == 0
    reach = jax.random.uniform(second, (GROUPS,), jnp.float32, 30.0, 100.0)
    rate = jnp.where(fast, 0.5 / reach, 0.2 / TOKENS)
    step = 2.0 * jnp.sqrt(2.0 * rate) * jax.random.uniform(third, (GROUPS,), jnp.float32, 0.7, 1.4)
    return (rate, step)


def draw_log_step(key, part):
    rate, step = speeds(key)
    return jnp.log(step).astype(jnp.float32)


def draw_eigen_real(key, part):
    rate, step = speeds(key)
    factor = jax.random.uniform(jax.random.fold_in(key, 202), (GROUPS, STATE), jnp.float32, 0.8, 1.25)
    return (-rate[:, None] * factor / step[:, None]).astype(jnp.float32)


def draw_eigen_imag(key, part):
    rate, step = speeds(key)
    first, second = jax.random.split(jax.random.fold_in(key, 303))
    angle = jax.random.uniform(first, (GROUPS, STATE), jnp.float32, 0.05, 0.4)
    signs = (2 * jax.random.randint(second, (GROUPS, STATE), 0, 2) - 1).astype(jnp.float32)
    return (signs * angle / step[:, None]).astype(jnp.float32)


def draw_decay_shift(key, part):
    rate, step = speeds(key)
    first, second, third = jax.random.split(jax.random.fold_in(key, 404), 3)
    factor = jax.random.uniform(first, (GROUPS, TOKENS // 32), jnp.float32, 0.0, 2.0)
    shift = -rate[:, None] * jnp.repeat(factor, 32, axis=1, total_repeat_length=TOKENS)
    places = jax.random.randint(second, (GROUPS, 3), 0, TOKENS)
    depth = jax.random.uniform(third, (GROUPS, 3), jnp.float32, 0.22, 0.69)
    rows_index = jnp.broadcast_to(jnp.arange(GROUPS)[:, None], (GROUPS, 3))
    shift = shift.at[rows_index, places].add(-depth)
    return shift.astype(jnp.float32)


def draw_conv_taps(key, part):
    first, second = jax.random.split(jax.random.fold_in(key, 505))
    place = jnp.arange(CONV_W).astype(jnp.float32) / max(CONV_W - 1, 1)
    noise = jax.random.normal(first, (KERNEL, CONV_W), jnp.float32)
    ramp = jnp.exp(math.log(3.0) * place)
    scale = jnp.exp(jax.random.uniform(second, (CONV_W,), jnp.float32, 0.0, math.log(10.0)))
    return (noise * scale * ramp / math.sqrt(KERNEL)).astype(jnp.float32)


def levels(own_key, extent, cuts, least, largest):
    level = 1.0
    for axis_at, parts in cuts:
        heights = jax.random.uniform(jax.random.fold_in(jax.random.fold_in(own_key, 6), axis_at), (parts,), jnp.float32, least / len(cuts), largest / len(cuts))
        level = level * jnp.repeat(jnp.exp(heights), extent[axis_at] // parts).reshape((-1,) + (1,) * (len(extent) - 1 - axis_at))
    return level


def bell_draw(stream_key, dims, width, most, shards=(), held_as=jnp.bfloat16):
    factor_of = levels(stream_key, dims, shards, -0.22, 0.18) if shards else 1.0
    array = jax.random.normal(stream_key, dims, jnp.float32) * width * factor_of
    return jnp.minimum(jnp.maximum(array, -most), most).astype(held_as)


def setup_inputs(seed: int = 0) -> dict:
    splits = jax.random.split(jax.random.key(seed), 18)
    tokens = bell_draw(splits[0], (TOKENS, D), 1.0, 6.0, ((0, 128), (1, 4)))
    norm_gain = jnp.clip(1.0 + 0.18 * jax.random.normal(splits[1], (D,), jnp.float32), 0.1, 1.9)
    proj_state = bell_draw(splits[2], (D, SSM_W), D ** -0.5, 0.125, ((0, 128), (1, 4)))
    proj_value = bell_draw(splits[3], (D, CONV_W), D ** -0.5, 0.125, ((0, 128), (1, 4)))
    proj_gate = bell_draw(splits[4], (D, CONV_W), D ** -0.5, 0.125, ((0, 128), (1, 4)))
    eigen_real = draw_eigen_real(jax.random.fold_in(splits[17], 71), 0)
    eigen_imag = draw_eigen_imag(jax.random.fold_in(splits[17], 71), 0)
    log_step = draw_log_step(jax.random.fold_in(splits[17], 71), 0)
    decay_shift = draw_decay_shift(jax.random.fold_in(splits[17], 71), 0)
    state_input = bell_draw(splits[9], (2, GROUPS, GROUP, STATE), 0.18, 1.0, ((1, 4),), jnp.float32)
    state_readout_matrices = bell_draw(splits[10], (2, GROUPS, GROUP, STATE), 0.09, 0.5, ((1, 4),), jnp.float32)
    skip_gain = bell_draw(splits[11], (SSM_W,), 1.0, 5.0, ((0, 4),), jnp.float32)
    init_state = bell_draw(splits[12], (2, GROUPS, STATE), 1.0, 5.0, ((1, 4),), jnp.float32)
    conv_taps = draw_conv_taps(jax.random.fold_in(splits[17], 71), 0)
    channel_gain = jnp.clip(1.0 + 0.18 * jax.random.normal(splits[14], (CONV_W,), jnp.float32), 0.1, 1.9)
    merge_state = bell_draw(splits[15], (SSM_W, D), (SSM_W + CONV_W) ** -0.5, 0.125, ((0, 4), (1, 128)))
    merge_conv = bell_draw(splits[16], (CONV_W, D), (SSM_W + CONV_W) ** -0.5, 0.125, ((0, 4), (1, 128)))
    return {"tokens": tokens, "norm_gain": norm_gain, "proj_state": proj_state, "proj_value": proj_value, "proj_gate": proj_gate, "eigen_real": eigen_real, "eigen_imag": eigen_imag, "log_step": log_step, "decay_shift": decay_shift, "state_input": state_input, "state_readout_matrices": state_readout_matrices, "skip_gain": skip_gain, "init_state": init_state, "conv_taps": conv_taps, "channel_gain": channel_gain, "merge_state": merge_state, "merge_conv": merge_conv}


epsilon = 1e-06
exact_precision = lax.Precision.HIGHEST

def round_half(value):
    return lax.optimization_barrier(value.astype(jnp.bfloat16))

def input_matrix(eigen_real, eigen_imag, step, state_input):
    base = eigen_real * step[:, None]
    theta = eigen_imag * step[:, None]
    magnitude = jnp.exp(base)
    near_re = magnitude * jnp.cos(theta) - 1.0
    near_im = magnitude * jnp.sin(theta)
    modulus = eigen_real * eigen_real + eigen_imag * eigen_imag
    ratio_re = (near_re * eigen_real + near_im * eigen_imag) / modulus
    ratio_im = (near_im * eigen_real - near_re * eigen_imag) / modulus
    in_re = state_input[0]
    in_im = state_input[1]
    discrete_decay_real = ratio_re[:, None, :] * in_re - ratio_im[:, None, :] * in_im
    discrete_decay_imaginary = ratio_re[:, None, :] * in_im + ratio_im[:, None, :] * in_re
    return (discrete_decay_real, discrete_decay_imaginary)

def block_states(c_re, c_im, delta_real, delta_imaginary, shift, base, theta, counts, lower):
    level = jnp.cumsum(shift, axis=0)[:, :, None] + counts * base
    angle = counts * theta
    cosine = jnp.cos(angle)
    sine = jnp.sin(angle)
    grow = jnp.exp(level)
    shrink = jnp.exp(-level)
    w_re = shrink * (cosine * delta_real + sine * delta_imaginary)
    w_im = shrink * (cosine * delta_imaginary - sine * delta_real)
    length, groups, states = delta_real.shape
    stacked = jnp.concatenate([w_re, w_im], axis=1).reshape(length, 2 * groups * states)
    summed = jnp.dot(lower, stacked, precision=exact_precision).reshape(length, 2 * groups, states)
    t_re = summed[:, :groups] + c_re
    t_im = summed[:, groups:] + c_im
    input_real = grow * (cosine * t_re - sine * t_im)
    input_imaginary = grow * (cosine * t_im + sine * t_re)
    return (input_real, input_imaginary)

def state_branch(u_in, eigen_real, eigen_imag, log_step, decay_shift, state_input, state_readout_matrices, skip_gain, init_state):
    step = jnp.exp(log_step)
    base = eigen_real * step[:, None]
    theta = eigen_imag * step[:, None]
    discrete_decay_real, discrete_decay_imaginary = input_matrix(eigen_real, eigen_imag, step, state_input)
    length = min(32, TOK_DEV)
    blocks = TOKENS // length
    values = u_in.reshape(blocks, length, GROUPS, GROUP)
    shifts = decay_shift.T.reshape(blocks, length, GROUPS)
    counts = (jnp.arange(length) + 1).astype(jnp.float32)[:, None, None]
    lower = (jnp.arange(length)[:, None] >= jnp.arange(length)[None, :]).astype(jnp.float32)
    output_real = state_readout_matrices[0]
    output_imaginary = state_readout_matrices[1]
    skips = skip_gain.reshape(GROUPS, GROUP)

    def advance(carry, inputs):
        block_u, block_shift = inputs
        float_values = block_u.astype(jnp.float32)
        delta_real = jnp.einsum('ovi,viu->ovu', float_values, discrete_decay_real, precision=exact_precision)
        delta_imaginary = jnp.einsum('ovi,viu->ovu', float_values, discrete_decay_imaginary, precision=exact_precision)
        input_real, input_imaginary = block_states(carry[0], carry[1], delta_real, delta_imaginary, block_shift, base, theta, counts, lower)
        final_output = jnp.einsum('lan,arn->lar', input_real, output_real, precision=exact_precision) - jnp.einsum('lan,arn->lar', input_imaginary, output_imaginary, precision=exact_precision)
        final_output = final_output + skips * float_values
        return ((input_real[-1], input_imaginary[-1]), jax.nn.gelu(final_output).astype(jnp.bfloat16))
    start = (init_state[0].astype(jnp.float32), init_state[1].astype(jnp.float32))
    _, outs = lax.scan(advance, start, (values, shifts))
    return outs.reshape(TOKENS, SSM_W)

def conv_branch(value, gate, conv_taps, channel_gain):
    glu = round_half(value.astype(jnp.float32) * jax.nn.sigmoid(gate.astype(jnp.float32)))
    reach = KERNEL - 1
    count = glu.shape[0]
    extended = jnp.concatenate([jnp.zeros((reach, CONV_W), jnp.bfloat16), glu], axis=0).astype(jnp.float32)
    raw = jnp.zeros((count, CONV_W), jnp.float32)
    for offset in range(KERNEL):
        raw = raw + conv_taps[offset] * extended[offset:offset + count]
    first = lax.optimization_barrier(jnp.sum(raw, axis=1, keepdims=True))
    second = lax.optimization_barrier(jnp.sum(raw * raw, axis=1, keepdims=True))
    middle = first / CONV_W
    spread = second / CONV_W - middle * middle
    scaled = (raw - middle) * lax.rsqrt(spread + epsilon) * channel_gain
    return jax.nn.silu(scaled).astype(jnp.bfloat16)

def reference(tokens, norm_gain, proj_state, proj_value, proj_gate, eigen_real, eigen_imag, log_step, decay_shift, state_input, state_readout_matrices, skip_gain, init_state, conv_taps, channel_gain, merge_state, merge_conv):
    wide = tokens.astype(jnp.float32)
    normed = (wide * lax.rsqrt(lax.optimization_barrier(jnp.mean(wide * wide, axis=1, keepdims=True)) + epsilon) * norm_gain).astype(jnp.bfloat16)
    u_in = round_half(jnp.dot(normed, proj_state, preferred_element_type=jnp.float32))
    value = round_half(jnp.dot(normed, proj_value, preferred_element_type=jnp.float32))
    gate = round_half(jnp.dot(normed, proj_gate, preferred_element_type=jnp.float32))
    ssm_out = state_branch(u_in, eigen_real, eigen_imag, log_step, decay_shift, state_input, state_readout_matrices, skip_gain, init_state)
    conv_out = conv_branch(value, gate, conv_taps, channel_gain)
    state_part = SSM_W // N_TP
    conv_part = CONV_W // N_TP
    total = jnp.zeros((TOKENS, D), jnp.float32)
    for index in range(N_TP):
        term = jnp.dot(ssm_out[:, index * state_part:(index + 1) * state_part], merge_state[index * state_part:(index + 1) * state_part], preferred_element_type=jnp.float32)
        term = term + jnp.dot(conv_out[:, index * conv_part:(index + 1) * conv_part], merge_conv[index * conv_part:(index + 1) * conv_part], preferred_element_type=jnp.float32)
        total = total + round_half(term).astype(jnp.float32)
    return total.astype(jnp.bfloat16)
```

```python
import jax
import jax.numpy as jnp
from jax import lax
from jax.experimental import pallas as pl
from jax.experimental.pallas import tpu as pltpu
from jax.sharding import Mesh
from jax.sharding import PartitionSpec as P

CONV_W = 1024
SP = ("z", "x", "c")
SP_TP = ("z", "x", "c", "tp")
CHUNK = 32
EPS = 1e-06
EXACT = lax.Precision.HIGHEST
F32 = jnp.float32
BF16 = jnp.bfloat16


def copies(value, axis):
    peers = lax.axis_size(axis)
    return lax.all_to_all(
        jnp.broadcast_to(value[None], (peers, *value.shape)), axis, 0, 0, tiled=True
    )


def next_along(block, axis):
    count = lax.axis_size(axis)
    return lax.ppermute(block, axis, [(i, i + 1) for i in range(count - 1)])


def partner(block):
    return lax.ppermute(block, "c", [(0, 1), (1, 0)])


def after(value, *others):
    return lax.optimization_barrier((value, *others))[0]


def along_z(piece):
    return copies(piece, "z")


def along_x(planes):
    return copies(planes, "x")


def whole_specs(arrays):
    return [pl.BlockSpec(memory_space=pltpu.VMEM) for _ in arrays]


def call(body, outs, arrays, scalars=(), scratch=(), **costs):
    return pl.pallas_call(
        body,
        out_shape=outs,
        in_specs=[pl.BlockSpec(memory_space=pltpu.SMEM) for _ in scalars] + whole_specs(arrays),
        out_specs=jax.tree.map(lambda _: pl.BlockSpec(memory_space=pltpu.VMEM), outs),
        scratch_shapes=list(scratch),
        cost_estimate=pl.CostEstimate(**costs) if costs else None,
    )(*scalars, *arrays)


def natural_order(core_ref, own_ref, other_ref, into_ref):
    peers_x, peers_z, rows, _ = own_ref.shape

    def place(first, second):
        for z in range(peers_z):
            for x in range(peers_x):
                for c, source in enumerate((first, second)):
                    at = ((z * peers_x + x) * 2 + c) * rows
                    into_ref[at : at + rows, :] = source[x, z]

    @pl.when(core_ref[0] == 0)
    def _():
        place(own_ref, other_ref)

    @pl.when(core_ref[0] == 1)
    def _():
        place(other_ref, own_ref)


def dot_rows(a, b):
    return lax.dot_general(a, b, (((1,), (1,)), ((), ())), preferred_element_type=F32)


def state_in_kernel(core_ref, normed_ref, own_ref, other_ref, out_ref, weight_ref):
    natural_order(core_ref, own_ref, other_ref, weight_ref)
    out_ref[...] = jnp.dot(
        normed_ref[...], weight_ref[...], preferred_element_type=F32
    ).astype(BF16)


def glu_kernel(core_ref, normed_ref, own_ref, other_ref, out_ref, weight_ref):
    natural_order(core_ref, own_ref, other_ref, weight_ref)
    width = out_ref.shape[1]
    both = jnp.dot(normed_ref[...], weight_ref[...], preferred_element_type=F32)
    value = both[:, :width].astype(BF16).astype(F32)
    gate = both[:, width:].astype(BF16).astype(F32)
    out_ref[...] = (value * jax.nn.sigmoid(gate)).astype(BF16)


def scan_kernel(
    u_ref,
    grow_ref,
    shrink_ref,
    in_ref,
    out_mat_ref,
    fwd_re_ref,
    fwd_im_ref,
    inv_re_ref,
    inv_im_ref,
    hop_re_ref,
    hop_im_ref,
    lower_ref,
    skip_ref,
    y_ref,
    last_ref,
    cum_re_ref,
    cum_im_ref,
    end_re_ref,
    end_im_ref,
):
    count, width = u_ref.shape
    states = fwd_re_ref.shape[1]
    chunks = count // CHUNK
    block = lower_ref.shape[0]
    slab = 256
    u = u_ref[...].astype(F32)
    scaled = (u * shrink_ref[...]).astype(BF16)

    def chunked(value):
        return value.reshape(chunks, CHUNK, slab)

    def summed(value):
        value = value.reshape(count, slab).astype(BF16)
        return jnp.concatenate(
            [
                jnp.dot(lower_ref[...], value[k : k + block], preferred_element_type=F32)
                for k in range(0, count, block)
            ]
        )

    def first_pass(j, _):
        at = pl.ds(pl.multiple_of(j * slab, slab), slab)
        at_im = pl.ds(pl.multiple_of(states + j * slab, slab), slab)
        d_re = chunked(jnp.dot(scaled, in_ref[:, at], preferred_element_type=F32))
        d_im = chunked(jnp.dot(scaled, in_ref[:, at_im], preferred_element_type=F32))
        i_re, i_im = inv_re_ref[:, at][None], inv_im_ref[:, at][None]
        cum_re = summed(i_re * d_re - i_im * d_im)
        cum_im = summed(i_re * d_im + i_im * d_re)
        cum_re_ref[:, at] = cum_re
        cum_im_ref[:, at] = cum_im
        end_re_ref[:, at] = chunked(cum_re)[:, CHUNK - 1]
        end_im_ref[:, at] = chunked(cum_im)[:, CHUNK - 1]
        return 0

    lax.fori_loop(0, states // slab, first_pass, 0)

    h_re, h_im = hop_re_ref[0], hop_im_ref[0]
    t_re, t_im = end_re_ref[...], end_im_ref[...]
    s_re = h_re * t_re - h_im * t_im
    s_im = h_re * t_im + h_im * t_re
    for level in range(1, hop_re_ref.shape[0]):
        h_re, h_im = hop_re_ref[level], hop_im_ref[level]
        p_re, p_im = pltpu.roll(s_re, 1 << (level - 1), 0), pltpu.roll(s_im, 1 << (level - 1), 0)
        s_re, s_im = s_re + h_re * p_re - h_im * p_im, s_im + h_re * p_im + h_im * p_re
    lanes = last_ref.shape[1]
    for k in range(states // lanes):
        last_ref[k : k + 1, :] = s_re[chunks - 1 :, k * lanes : (k + 1) * lanes]
        row = states // lanes + k
        last_ref[row : row + 1, :] = s_im[chunks - 1 :, k * lanes : (k + 1) * lanes]
    begins = lax.broadcasted_iota(jnp.int32, s_re.shape, 0) > 0
    end_re_ref[...] = jnp.where(begins, pltpu.roll(s_re, 1, 0), 0.0)
    end_im_ref[...] = jnp.where(begins, pltpu.roll(s_im, 1, 0), 0.0)
    y_ref[...] = jnp.zeros(y_ref.shape, F32)

    def second_pass(j, _):
        at = pl.ds(pl.multiple_of(j * slab, slab), slab)
        at_im = pl.ds(pl.multiple_of(states + j * slab, slab), slab)
        t_re = chunked(cum_re_ref[:, at]) + end_re_ref[:, at][:, None]
        t_im = chunked(cum_im_ref[:, at]) + end_im_ref[:, at][:, None]
        f_re, f_im = fwd_re_ref[:, at][None], fwd_im_ref[:, at][None]
        x_re = (f_re * t_re - f_im * t_im).reshape(count, slab).astype(BF16)
        x_im = (f_re * t_im + f_im * t_re).reshape(count, slab).astype(BF16)
        y_ref[...] += dot_rows(x_re, out_mat_ref[:, at]) + dot_rows(x_im, out_mat_ref[:, at_im])
        return 0

    lax.fori_loop(0, states // slab, second_pass, 0)
    y_ref[...] = y_ref[...] * grow_ref[...] + skip_ref[...] * u


def merge_kernel(
    core_ref,
    y_ref,
    power_ref,
    h_re_ref,
    h_im_ref,
    read_re_ref,
    read_im_ref,
    conv_ref,
    own_ref,
    other_ref,
    out_ref,
    weight_ref,
):
    natural_order(core_ref, own_ref, other_ref, weight_ref)
    width = y_ref.shape[1]
    h_re, h_im = h_re_ref[...], h_im_ref[...]
    c_re, c_im = read_re_ref[...], read_im_ref[...]
    blend = jnp.concatenate(
        [(c_re * h_re - c_im * h_im).astype(BF16), (-c_re * h_im - c_im * h_re).astype(BF16)], axis=1
    )
    total = y_ref[...] + dot_rows(power_ref[...], blend)
    ssm = jax.nn.gelu(total).astype(BF16)
    both = jnp.concatenate([ssm, conv_ref[...]], axis=1)
    out_ref[...] = dot_rows(both, weight_ref[...]).astype(BF16)


def input_matrix(eigen_real, eigen_imag, step, state_input):
    base = eigen_real * step[:, None]
    theta = eigen_imag * step[:, None]
    magnitude = jnp.exp(base)
    near_re = magnitude * jnp.cos(theta) - 1.0
    near_im = magnitude * jnp.sin(theta)
    modulus = eigen_real * eigen_real + eigen_imag * eigen_imag
    ratio_re = (near_re * eigen_real + near_im * eigen_imag) / modulus
    ratio_im = (near_im * eigen_real - near_re * eigen_imag) / modulus
    in_re, in_im = state_input[0], state_input[1]
    return (
        ratio_re[:, None, :] * in_re - ratio_im[:, None, :] * in_im,
        ratio_re[:, None, :] * in_im + ratio_im[:, None, :] * in_re,
    )


def on_diagonal(blocks):
    groups, rows, cols = blocks.shape
    tiled = jnp.tile(blocks.reshape(groups * rows, cols), (1, groups))
    row_group = lax.broadcasted_iota(jnp.int32, tiled.shape, 0) // rows
    col_group = lax.broadcasted_iota(jnp.int32, tiled.shape, 1) // cols
    return jnp.where(row_group == col_group, tiled, 0.0)


def spread_over(groups, each):
    row = lax.broadcasted_iota(jnp.int32, (groups, groups * each), 0)
    col = lax.broadcasted_iota(jnp.int32, (groups, groups * each), 1) // each
    return (row == col).astype(F32)


def squared(re, im):
    return re * re - im * im, 2.0 * re * im


def times(a, b):
    return a[0] * b[0] - a[1] * b[1], a[0] * b[1] + a[1] * b[0]


def tables(eigen_real, eigen_imag, log_step, decay_shift, state_input, readout):
    groups, states = eigen_real.shape
    lanes = groups * states
    count = decay_shift.shape[1]
    chunks = count // CHUNK
    step = jnp.exp(log_step)
    base = (eigen_real * step[:, None]).reshape(1, lanes)
    theta = (eigen_imag * step[:, None]).reshape(1, lanes)
    inside = jnp.arange(1, CHUNK + 1, dtype=F32)[:, None]
    level, angle = inside * base, inside * theta
    cosine, sine = jnp.cos(angle), jnp.sin(angle)
    grow, shrink = jnp.exp(level), jnp.exp(-level)
    forward = (grow * cosine, grow * sine)
    inverse = (shrink * cosine, -shrink * sine)
    shift = decay_shift.T
    lower = jnp.tril(jnp.ones((CHUNK, CHUNK), F32))
    partial = jnp.einsum(
        "ls,csg->clg", lower, shift.reshape(chunks, CHUNK, groups), precision=EXACT
    )
    sums = partial[:, -1]
    earlier = jnp.tril(jnp.ones((chunks, chunks), F32), -1)
    before = jnp.dot(earlier, sums, precision=EXACT)
    whole = (partial + before[:, None]).reshape(count, groups)
    partial = partial.reshape(count, groups)
    spread = spread_over(groups, states)
    wide = jnp.dot(whole, spread, precision=EXACT)
    narrow = jnp.dot(partial, spread_over(groups, 16), precision=EXACT)
    chunk_rot = (jnp.cos(CHUNK * theta), jnp.sin(CHUNK * theta))
    rots = [chunk_rot]
    while (1 << len(rots)) <= chunks:
        rots.append(squared(*rots[-1]))
    index = jnp.arange(chunks)
    hops = [(jnp.exp(CHUNK * base + jnp.dot(sums, spread, precision=EXACT)), rots[0])]
    distance, place = 1, 0
    while distance < chunks:
        window = (
            (index[:, None] >= index[None, :]) & (index[:, None] - index[None, :] < distance)
        ).astype(F32)
        near = jnp.dot(jnp.dot(window, sums, precision=EXACT), spread, precision=EXACT)
        size = jnp.where(index[:, None] >= distance, jnp.exp(distance * CHUNK * base + near), 0.0)
        hops.append((size, rots[place]))
        distance, place = distance * 2, place + 1
    hop_re = jnp.stack([size * rot[0] for size, rot in hops])
    hop_im = jnp.stack([size * rot[1] for size, rot in hops])
    starts = index.astype(F32)[:, None] * CHUNK * theta
    turn = times(
        (jnp.cos(starts)[:, None], jnp.sin(starts)[:, None]), (cosine[None], sine[None])
    )
    counts = jnp.arange(1, count + 1, dtype=F32)[:, None]
    size = jnp.exp(counts * base + wide)
    power = jnp.concatenate(
        [(size * t.reshape(count, lanes)).astype(BF16) for t in turn], axis=1
    )
    b_re, b_im = input_matrix(eigen_real, eigen_imag, step, state_input)
    into = jnp.concatenate([on_diagonal(b_re), on_diagonal(b_im)], axis=1).astype(BF16)
    c_re, c_im = on_diagonal(readout[0]), on_diagonal(readout[1])
    out = jnp.concatenate([c_re, -c_im], axis=1).astype(BF16)
    block = min(count, 256)
    at = jnp.arange(block)
    lower_block = (
        (at[:, None] >= at[None, :]) & (at[:, None] // CHUNK == at[None, :] // CHUNK)
    ).astype(BF16)
    device = dict(
        base=base.reshape(-1, 128),
        turn=tuple(r.reshape(-1, 128) for r in rots[-1]),
        shift=wide[-1].reshape(-1, 128),
    )
    scan = (jnp.exp(narrow), jnp.exp(-narrow), into, out, *forward, *inverse, hop_re, hop_im, lower_block)
    return scan, power, (c_re.astype(BF16), c_im.astype(BF16)), device, count


def pulled(packed, rows):
    return packed[:rows], packed[rows : 2 * rows], packed[2 * rows :]


def carry_in(last, device, count, init_state):
    rows = device["base"].shape[0]
    base, turn = device["base"], device["turn"]
    plane = ("x", "c")
    packed = jnp.concatenate([last, device["shift"]])
    near = copies(packed, plane)
    peers, place = lax.axis_size(plane), lax.axis_index(plane)
    zero = jnp.zeros_like(base)
    run = (zero, zero)
    before, shift_before = run, zero
    shift_run = zero
    for k in range(peers):
        re, im, shift = pulled(near[k], rows)
        size = jnp.exp(count * base + shift)
        moved = times((size * turn[0], size * turn[1]), run)
        run = (moved[0] + re, moved[1] + im)
        shift_run = shift_run + shift
        passed = k < place
        before = jax.tree.map(lambda new, old: jnp.where(passed, new, old), run, before)
        shift_before = jnp.where(passed, shift_run, shift_before)
    far = copies(jnp.concatenate([*run, shift_run]), "z")
    plane_turn, at = turn, 1
    while at < peers:
        plane_turn, at = squared(*plane_turn), at * 2
    h = tuple(s.reshape(-1, 128) for s in (init_state[0], init_state[1]))
    for k in range(lax.axis_size("z")):
        re, im, shift = pulled(far[k], rows)
        size = jnp.exp(peers * count * base + shift)
        moved = times((size * plane_turn[0], size * plane_turn[1]), h)
        passed = k < lax.axis_index("z")
        h = tuple(jnp.where(passed, m + s, o) for m, s, o in zip(moved, (re, im), h))
    turns = (jnp.ones_like(base), zero)
    for k in range(peers):
        passed = k < place
        turns = tuple(jnp.where(passed, new, old) for new, old in zip(times(turns, turn), turns))
    size = jnp.exp(place * count * base + shift_before)
    moved = times((size * turns[0], size * turns[1]), h)
    return moved[0] + before[0], moved[1] + before[1]


def summed_over(arrays, axis):
    line = jnp.concatenate([a.reshape(-1) for a in arrays]).reshape(-1, 128)
    total = jnp.sum(copies(line, axis), axis=0).reshape(-1)
    done, at = [], 0
    for a in arrays:
        done.append(total[at : at + a.size].reshape(a.shape))
        at += a.size
    return done


def conv_branch(glu, conv_taps, channel_gain):
    reach = conv_taps.shape[0] - 1
    count = glu.shape[0]
    before = next_along(glu[count - 32 :], SP)[32 - reach :]
    extended = jnp.concatenate([before, glu], axis=0).astype(F32)
    raw = jnp.zeros(glu.shape, F32)
    for offset in range(reach + 1):
        raw = raw + conv_taps[offset] * extended[offset : offset + count]
    first, second = summed_over(
        (jnp.sum(raw, axis=1, keepdims=True), jnp.sum(raw * raw, axis=1, keepdims=True)), "tp"
    )
    middle = first / CONV_W
    spread = second / CONV_W - middle * middle
    scaled = (raw - middle) * lax.rsqrt(spread + EPS) * channel_gain
    return jax.nn.silu(scaled).astype(BF16)


def per_device(
    tokens,
    norm_gain,
    proj_state,
    proj_value,
    proj_gate,
    eigen_real,
    eigen_imag,
    log_step,
    decay_shift,
    state_input,
    readout,
    skip_gain,
    init_state,
    conv_taps,
    channel_gain,
    merge_state,
    merge_conv,
):
    core = lax.axis_index("c").reshape(1).astype(jnp.int32)
    parts = lax.axis_size("tp")
    blocks = copies(tokens, "tp")
    count = tokens.shape[0]
    width = proj_state.shape[1]
    in_z = along_z(proj_state)
    vg_z = along_z(jnp.concatenate([proj_value, proj_gate], axis=1))
    merge_z = along_z(jnp.concatenate([merge_state.T, merge_conv.T], axis=1))
    in_x = along_x(in_z)
    vg_x = along_x(vg_z)
    merge_x = along_x(merge_z)

    scan_tables, power, reads, device, _ = tables(
        eigen_real, eigen_imag, log_step, decay_shift, state_input, readout
    )

    whole = jnp.moveaxis(blocks, 0, 1).reshape(count, -1)
    wide = whole.astype(F32)
    normed = (
        wide * lax.rsqrt(jnp.mean(wide * wide, axis=1, keepdims=True) + EPS) * norm_gain
    ).astype(BF16)

    depth = normed.shape[1]
    u_in = call(
        state_in_kernel,
        jax.ShapeDtypeStruct((count, width), BF16),
        (normed, in_x, partner(in_x)),
        scalars=(core,),
        scratch=(pltpu.VMEM((depth, width), BF16),),
        flops=2 * count * depth * width,
        bytes_accessed=4 * depth * count,
        transcendentals=0,
    )
    lanes = eigen_real.size
    chunks = count // CHUNK
    y_local, last = call(
        scan_kernel,
        (
            jax.ShapeDtypeStruct((count, width), F32),
            jax.ShapeDtypeStruct((2 * lanes // 128, 128), F32),
        ),
        (u_in, *scan_tables, skip_gain.reshape(1, -1)),
        scratch=(
            pltpu.VMEM((count, lanes), F32),
            pltpu.VMEM((count, lanes), F32),
            pltpu.VMEM((chunks, lanes), F32),
            pltpu.VMEM((chunks, lanes), F32),
        ),
        flops=12 * count * width * lanes,
        bytes_accessed=8 * count * lanes,
        transcendentals=0,
    )
    h_re, h_im = carry_in(last, device, count, init_state)

    glu = call(
        glu_kernel,
        jax.ShapeDtypeStruct((count, width), BF16),
        (normed, vg_x, partner(vg_x)),
        scalars=(core,),
        scratch=(pltpu.VMEM((depth, 2 * width), BF16),),
        flops=4 * count * depth * width,
        bytes_accessed=4 * depth * count,
        transcendentals=0,
    )
    conv_out = conv_branch(glu, conv_taps, channel_gain)

    product = call(
        merge_kernel,
        jax.ShapeDtypeStruct((count, depth), BF16),
        (
            y_local,
            power,
            h_re.reshape(1, -1),
            h_im.reshape(1, -1),
            *reads,
            conv_out,
            merge_x,
            partner(merge_x),
        ),
        scalars=(core,),
        scratch=(pltpu.VMEM((depth, 2 * width), BF16),),
        flops=4 * count * depth * width,
        bytes_accessed=4 * depth * count,
        transcendentals=0,
    )
    arrived = lax.all_to_all(
        product.reshape(parts, count // parts, depth), "tp", split_axis=0, concat_axis=0, tiled=True
    )
    return arrived.astype(F32).sum(axis=0).astype(BF16)


def finer_mesh(mesh):
    cores = 2
    return Mesh(mesh.devices.reshape(16, 4, cores, mesh.shape["tp"]), SP_TP)


def solution(mesh):
    return jax.shard_map(
        per_device,
        mesh=finer_mesh(mesh),
        in_specs=(
            P(SP, "tp"),
            P(),
            P(SP, "tp"),
            P(SP, "tp"),
            P(SP, "tp"),
            P("tp", None),
            P("tp", None),
            P("tp"),
            P("tp", SP),
            P(None, "tp", None, None),
            P(None, "tp", None, None),
            P("tp"),
            P(None, "tp", None),
            P(None, "tp"),
            P("tp"),
            P("tp", SP),
            P("tp", SP),
        ),
        out_specs=P(SP_TP, None),
        check_vma=False,
    )
```

```python
import jax
import jax.numpy as jnp
from jax import lax
from jax.experimental import pallas as pl
from jax.experimental.pallas import tpu as pltpu
from jax.sharding import Mesh
from jax.sharding import PartitionSpec as P

CONV_W = 1024
SP = ("z", "x", "c")
SP_TP = ("z", "x", "c", "tp")
CHUNK = 32
EPS = 1e-06
EXACT = lax.Precision.HIGHEST
F32 = jnp.float32
BF16 = jnp.bfloat16


def copies(value, axis):
    peers = lax.axis_size(axis)
    return lax.all_to_all(
        jnp.broadcast_to(value[None], (peers, *value.shape)), axis, 0, 0, tiled=True
    )


def next_along(block, axis):
    count = lax.axis_size(axis)
    return lax.ppermute(block, axis, [(i, i + 1) for i in range(count - 1)])


def partner(block):
    return lax.ppermute(block, "c", [(0, 1), (1, 0)])


def after(value, *others):
    return lax.optimization_barrier((value, *others))[0]


def from_ahead(block, axis, distance):
    count = lax.axis_size(axis)
    return lax.ppermute(block, axis, [(i, (i - distance) % count) for i in range(count)])


def along_z(piece):
    return copies(piece, "z")


def along_x(planes):
    peers = lax.axis_size("x")
    return jnp.stack([planes] + [from_ahead(planes, "x", d) for d in range(1, peers)])


def whole_specs(arrays):
    return [pl.BlockSpec(memory_space=pltpu.VMEM) for _ in arrays]


def call(body, outs, arrays, scalars=(), scratch=(), mib=16, **costs):
    return pl.pallas_call(
        body,
        compiler_params=pltpu.CompilerParams(vmem_limit_bytes=mib * 2**20),
        out_shape=outs,
        in_specs=[pl.BlockSpec(memory_space=pltpu.SMEM) for _ in scalars] + whole_specs(arrays),
        out_specs=jax.tree.map(lambda _: pl.BlockSpec(memory_space=pltpu.VMEM), outs),
        scratch_shapes=list(scratch),
        cost_estimate=pl.CostEstimate(**costs) if costs else None,
    )(*scalars, *arrays)


def natural_order(place_ref, own_ref, other_ref, into_ref, turned):
    peers_x, _, rows, _ = own_ref.shape
    blocks = into_ref.shape[0] // rows
    core, place_x, part = place_ref[0], place_ref[1], place_ref[2]
    first = part * turned

    def place(by_core):
        for k in range(blocks):
            at = lax.rem(first + k, blocks)
            x = lax.rem(lax.div(at, 2) - place_x + 2 * peers_x, peers_x)
            into_ref[k * rows : (k + 1) * rows, :] = by_core[k % 2][x, lax.div(at, 2 * peers_x)]

    @pl.when(core == 0)
    def _():
        place((own_ref, other_ref))

    @pl.when(core == 1)
    def _():
        place((other_ref, own_ref))


def dot_rows(a, b):
    return lax.dot_general(a, b, (((1,), (1,)), ((), ())), preferred_element_type=F32)


def norm_kernel(place_ref, own_ref, ahead_ref, top_ref, bottom_ref, behind_ref, gain_ref, out_ref):
    parts, count, depth = out_ref.shape
    half = count // 2
    part = place_ref[2]

    def rows_of(at, opposite_ref):
        rows = pl.ds(at, half)
        blocks = [
            ref.astype(F32)
            for ref in (own_ref[rows], ahead_ref[rows], opposite_ref[...], behind_ref[rows])
        ]
        power = sum(jnp.sum(block * block, axis=1, keepdims=True) for block in blocks)
        scale = lax.rsqrt(power / (parts * depth) + EPS)
        for p, block in enumerate(blocks):
            gain = gain_ref[lax.rem(part + p, parts)]
            out_ref[p, rows] = (block * scale * gain).astype(BF16)

    rows_of(0, top_ref)
    rows_of(half, bottom_ref)


def projected(normed_ref, weight_ref):
    parts, _, depth = normed_ref.shape
    return sum(
        jnp.dot(
            normed_ref[p],
            weight_ref[p * depth : (p + 1) * depth],
            preferred_element_type=F32,
        )
        for p in range(parts)
    )


def state_in_kernel(place_ref, normed_ref, own_ref, other_ref, out_ref, weight_ref):
    parts = normed_ref.shape[0]
    turned = weight_ref.shape[0] // own_ref.shape[2] // parts
    natural_order(place_ref, own_ref, other_ref, weight_ref, turned)
    out_ref[...] = projected(normed_ref, weight_ref).astype(BF16)


def glu_kernel(place_ref, normed_ref, own_ref, other_ref, out_ref, weight_ref):
    parts = normed_ref.shape[0]
    turned = weight_ref.shape[0] // own_ref.shape[2] // parts
    natural_order(place_ref, own_ref, other_ref, weight_ref, turned)
    width = out_ref.shape[1]
    both = projected(normed_ref, weight_ref)
    value = both[:, :width].astype(BF16).astype(F32)
    gate = both[:, width:].astype(BF16).astype(F32)
    out_ref[...] = (value * jax.nn.sigmoid(gate)).astype(BF16)


def squared(re, im):
    return re * re - im * im, 2.0 * re * im


def times(a, b):
    return a[0] * b[0] - a[1] * b[1], a[0] * b[1] + a[1] * b[0]


def exact_dot(a, b):
    return jnp.dot(a, b, preferred_element_type=F32, precision=EXACT)


def spread_over(groups, each):
    row = lax.broadcasted_iota(jnp.int32, (groups, groups * each), 0)
    col = lax.broadcasted_iota(jnp.int32, (groups, groups * each), 1) // each
    return (row == col).astype(F32)


def write_diagonal(out_ref, at, blocks, groups):
    rows, cols = blocks.shape
    pair = jnp.concatenate([blocks, blocks], axis=1)
    row_group = lax.broadcasted_iota(jnp.int32, pair.shape, 0) // (rows // groups)
    col_group = lax.broadcasted_iota(jnp.int32, pair.shape, 1) // cols
    for k in range(groups // 2):
        mine = row_group == col_group + 2 * k
        out_ref[:, at + 2 * k * cols : at + 2 * (k + 1) * cols] = jnp.where(mine, pair, 0.0).astype(BF16)


def table_kernel(
    shift_ref,
    base_ref,
    cos_ref,
    sin_ref,
    start_cos_ref,
    start_sin_ref,
    b_re_ref,
    b_im_ref,
    c_re_ref,
    c_im_ref,
    grow_ref,
    shrink_ref,
    into_ref,
    out_ref,
    hop_re_ref,
    hop_im_ref,
    power_ref,
    total_ref,
):
    groups, count = shift_ref.shape
    lanes = base_ref.shape[1]
    width = grow_ref.shape[1]
    chunks = count // CHUNK
    base = base_ref[...]
    row = lax.broadcasted_iota(jnp.int32, (count, count), 0)
    col = lax.broadcasted_iota(jnp.int32, (count, count), 1)
    earlier = row >= col
    inside = earlier & (row // CHUNK == col // CHUNK)

    def run(which):
        return lax.dot_general(
            which.astype(F32),
            shift_ref[...],
            (((1,), (1,)), ((), ())),
            precision=EXACT,
            preferred_element_type=F32,
        )

    partial, whole = run(inside), run(earlier)
    narrow = exact_dot(partial, spread_over(groups, width // groups))
    grow_ref[...] = jnp.exp(narrow)
    shrink_ref[...] = jnp.exp(-narrow)
    spread = spread_over(groups, lanes // groups)
    wide = exact_dot(whole, spread)
    wide_last = wide[count - 1 :]
    for k in range(lanes // 128):
        total_ref[k : k + 1, :] = wide_last[:, k * 128 : (k + 1) * 128]
    sums = jnp.concatenate([partial[(c + 1) * CHUNK - 1 : (c + 1) * CHUNK] for c in range(chunks)])
    near = exact_dot(sums, spread)
    index = lax.broadcasted_iota(jnp.int32, (chunks, lanes), 0)
    size = jnp.exp(CHUNK * base + near)
    turn = (start_cos_ref[1:2], start_sin_ref[1:2])
    hop_re_ref[0], hop_im_ref[0] = size * turn[0], size * turn[1]
    distance, level = 1, 1
    while distance < chunks:
        size = jnp.where(index >= distance, jnp.exp(distance * CHUNK * base + near), 0.0)
        turn = (start_cos_ref[distance : distance + 1], start_sin_ref[distance : distance + 1])
        hop_re_ref[level], hop_im_ref[level] = size * turn[0], size * turn[1]
        near = near + jnp.where(index >= distance, pltpu.roll(near, distance, 0), 0.0)
        distance, level = distance * 2, level + 1
    counts = lax.broadcasted_iota(jnp.int32, (CHUNK, 1), 0).astype(F32)
    inner = (cos_ref[...], sin_ref[...])
    for c in range(chunks):
        at = slice(c * CHUNK, (c + 1) * CHUNK)
        size = jnp.exp((counts + (c * CHUNK + 1)) * base + wide[at])
        turn = times((start_cos_ref[c : c + 1], start_sin_ref[c : c + 1]), inner)
        power_ref[at, :lanes] = (size * turn[0]).astype(BF16)
        power_ref[at, lanes:] = (size * turn[1]).astype(BF16)
    write_diagonal(into_ref, 0, b_re_ref[...], groups)
    write_diagonal(into_ref, lanes, b_im_ref[...], groups)
    write_diagonal(out_ref, 0, c_re_ref[...], groups)
    write_diagonal(out_ref, lanes, -c_im_ref[...], groups)


def scan_kernel(
    u_ref,
    grow_ref,
    shrink_ref,
    in_ref,
    out_mat_ref,
    fwd_re_ref,
    fwd_im_ref,
    inv_re_ref,
    inv_im_ref,
    hop_re_ref,
    hop_im_ref,
    lower_ref,
    skip_ref,
    y_ref,
    last_ref,
    cum_re_ref,
    cum_im_ref,
    end_re_ref,
    end_im_ref,
):
    count, width = u_ref.shape
    states = fwd_re_ref.shape[1]
    chunks = count // CHUNK
    block = lower_ref.shape[0]
    slab = 256
    u = u_ref[...].astype(F32)
    scaled = (u * shrink_ref[...]).astype(BF16)

    def chunked(value):
        return value.reshape(chunks, CHUNK, slab)

    def summed(value):
        value = value.reshape(count, slab).astype(BF16)
        return jnp.concatenate(
            [
                jnp.dot(lower_ref[...], value[k : k + block], preferred_element_type=F32)
                for k in range(0, count, block)
            ]
        )

    def first_pass(j, _):
        at = pl.ds(pl.multiple_of(j * slab, slab), slab)
        at_im = pl.ds(pl.multiple_of(states + j * slab, slab), slab)
        d_re = chunked(jnp.dot(scaled, in_ref[:, at], preferred_element_type=F32))
        d_im = chunked(jnp.dot(scaled, in_ref[:, at_im], preferred_element_type=F32))
        i_re, i_im = inv_re_ref[:, at][None], inv_im_ref[:, at][None]
        cum_re = summed(i_re * d_re - i_im * d_im)
        cum_im = summed(i_re * d_im + i_im * d_re)
        cum_re_ref[:, at] = cum_re
        cum_im_ref[:, at] = cum_im
        end_re_ref[:, at] = chunked(cum_re)[:, CHUNK - 1]
        end_im_ref[:, at] = chunked(cum_im)[:, CHUNK - 1]
        return 0

    lax.fori_loop(0, states // slab, first_pass, 0)

    h_re, h_im = hop_re_ref[0], hop_im_ref[0]
    t_re, t_im = end_re_ref[...], end_im_ref[...]
    s_re = h_re * t_re - h_im * t_im
    s_im = h_re * t_im + h_im * t_re
    for level in range(1, hop_re_ref.shape[0]):
        h_re, h_im = hop_re_ref[level], hop_im_ref[level]
        p_re, p_im = pltpu.roll(s_re, 1 << (level - 1), 0), pltpu.roll(s_im, 1 << (level - 1), 0)
        s_re, s_im = s_re + h_re * p_re - h_im * p_im, s_im + h_re * p_im + h_im * p_re
    lanes = last_ref.shape[1]
    for k in range(states // lanes):
        last_ref[k : k + 1, :] = s_re[chunks - 1 :, k * lanes : (k + 1) * lanes]
        row = states // lanes + k
        last_ref[row : row + 1, :] = s_im[chunks - 1 :, k * lanes : (k + 1) * lanes]
    begins = lax.broadcasted_iota(jnp.int32, s_re.shape, 0) > 0
    end_re_ref[...] = jnp.where(begins, pltpu.roll(s_re, 1, 0), 0.0)
    end_im_ref[...] = jnp.where(begins, pltpu.roll(s_im, 1, 0), 0.0)
    y_ref[...] = jnp.zeros(y_ref.shape, F32)

    def second_pass(j, _):
        at = pl.ds(pl.multiple_of(j * slab, slab), slab)
        at_im = pl.ds(pl.multiple_of(states + j * slab, slab), slab)
        t_re = chunked(cum_re_ref[:, at]) + end_re_ref[:, at][:, None]
        t_im = chunked(cum_im_ref[:, at]) + end_im_ref[:, at][:, None]
        f_re, f_im = fwd_re_ref[:, at][None], fwd_im_ref[:, at][None]
        x_re = (f_re * t_re - f_im * t_im).reshape(count, slab).astype(BF16)
        x_im = (f_re * t_im + f_im * t_re).reshape(count, slab).astype(BF16)
        y_ref[...] += dot_rows(x_re, out_mat_ref[:, at]) + dot_rows(x_im, out_mat_ref[:, at_im])
        return 0

    lax.fori_loop(0, states // slab, second_pass, 0)
    y_ref[...] = y_ref[...] * grow_ref[...] + skip_ref[...] * u


def merge_kernel(
    place_ref,
    y_ref,
    power_ref,
    h_re_ref,
    h_im_ref,
    read_ref,
    conv_ref,
    own_ref,
    other_ref,
    out_ref,
    weight_ref,
):
    natural_order(place_ref, own_ref, other_ref, weight_ref, 0)
    lanes = h_re_ref.shape[1]
    h_re, h_im = h_re_ref[...], h_im_ref[...]
    c_re, c_im = read_ref[:, :lanes].astype(F32), read_ref[:, lanes:].astype(F32)
    total = (
        y_ref[...]
        + dot_rows(power_ref[:, :lanes], (c_re * h_re + c_im * h_im).astype(BF16))
        + dot_rows(power_ref[:, lanes:], (c_im * h_re - c_re * h_im).astype(BF16))
    )
    ssm = jax.nn.gelu(total).astype(BF16)
    both = jnp.concatenate([ssm, conv_ref[...]], axis=1)
    out_ref[...] = dot_rows(both, weight_ref[...]).astype(BF16)


def input_matrix(eigen_real, eigen_imag, step, state_input):
    base = eigen_real * step[:, None]
    theta = eigen_imag * step[:, None]
    magnitude = jnp.exp(base)
    near_re = magnitude * jnp.cos(theta) - 1.0
    near_im = magnitude * jnp.sin(theta)
    modulus = eigen_real * eigen_real + eigen_imag * eigen_imag
    ratio_re = (near_re * eigen_real + near_im * eigen_imag) / modulus
    ratio_im = (near_im * eigen_real - near_re * eigen_imag) / modulus
    in_re, in_im = state_input[0], state_input[1]
    return (
        ratio_re[:, None, :] * in_re - ratio_im[:, None, :] * in_im,
        ratio_re[:, None, :] * in_im + ratio_im[:, None, :] * in_re,
    )


def tables(eigen_real, eigen_imag, log_step, decay_shift, state_input, readout, width):
    groups, states = eigen_real.shape
    lanes = groups * states
    count = decay_shift.shape[1]
    chunks = count // CHUNK
    step = jnp.exp(log_step)
    base = (eigen_real * step[:, None]).reshape(1, lanes)
    theta = (eigen_imag * step[:, None]).reshape(1, lanes)
    inside = jnp.arange(1, CHUNK + 1, dtype=F32)[:, None]
    level, angle = inside * base, inside * theta
    cosine, sine = jnp.cos(angle), jnp.sin(angle)
    grow, shrink = jnp.exp(level), jnp.exp(-level)
    forward = (grow * cosine, grow * sine)
    inverse = (shrink * cosine, -shrink * sine)
    starts = jnp.arange(chunks).astype(F32)[:, None] * CHUNK * theta
    start_cos, start_sin = jnp.cos(starts), jnp.sin(starts)
    whole_turn = (start_cos[chunks // 2], start_sin[chunks // 2])
    b_re, b_im = input_matrix(eigen_real, eigen_imag, step, state_input)
    rows = (groups * state_input.shape[2], states)
    levels = 1 + (chunks - 1).bit_length()
    block = min(count, 256)
    at = jnp.arange(block)
    lower_block = (
        (at[:, None] >= at[None, :]) & (at[:, None] // CHUNK == at[None, :] // CHUNK)
    ).astype(BF16)
    grow, shrink, into, out, hop_re, hop_im, power, total = call(
        table_kernel,
        (
            jax.ShapeDtypeStruct((count, width), F32),
            jax.ShapeDtypeStruct((count, width), F32),
            jax.ShapeDtypeStruct((width, 2 * lanes), BF16),
            jax.ShapeDtypeStruct((width, 2 * lanes), BF16),
            jax.ShapeDtypeStruct((levels, chunks, lanes), F32),
            jax.ShapeDtypeStruct((levels, chunks, lanes), F32),
            jax.ShapeDtypeStruct((count, 2 * lanes), BF16),
            jax.ShapeDtypeStruct((lanes // 128, 128), F32),
        ),
        (
            decay_shift,
            base,
            cosine,
            sine,
            start_cos,
            start_sin,
            b_re.reshape(rows),
            b_im.reshape(rows),
            readout[0].reshape(rows),
            readout[1].reshape(rows),
        ),
        mib=24,
        flops=20 * count * count * groups,
        bytes_accessed=8 * count * lanes,
        transcendentals=count * lanes,
    )
    device = dict(
        base=base.reshape(-1, 128),
        turn=squared(*(r.reshape(-1, 128) for r in whole_turn)),
        shift=total,
    )
    scan = (grow, shrink, into, out, *forward, *inverse, hop_re, hop_im, lower_block)
    return scan, power, out, device


def pulled(packed, rows):
    return packed[:rows], packed[rows : 2 * rows], packed[2 * rows :]


def carry_in(last, device, count, init_state):
    rows = device["base"].shape[0]
    base, turn = device["base"], device["turn"]
    plane = ("x", "c")
    packed = jnp.concatenate([last, device["shift"]])
    near = copies(packed, plane)
    peers, place = lax.axis_size(plane), lax.axis_index(plane)
    zero = jnp.zeros_like(base)
    run = (zero, zero)
    before, shift_before = run, zero
    shift_run = zero
    for k in range(peers):
        re, im, shift = pulled(near[k], rows)
        size = jnp.exp(count * base + shift)
        moved = times((size * turn[0], size * turn[1]), run)
        run = (moved[0] + re, moved[1] + im)
        shift_run = shift_run + shift
        passed = k < place
        before = jax.tree.map(lambda new, old: jnp.where(passed, new, old), run, before)
        shift_before = jnp.where(passed, shift_run, shift_before)
    far = copies(jnp.concatenate([*run, shift_run]), "z")
    plane_turn, at = turn, 1
    while at < peers:
        plane_turn, at = squared(*plane_turn), at * 2
    h = tuple(s.reshape(-1, 128) for s in (init_state[0], init_state[1]))
    for k in range(lax.axis_size("z")):
        re, im, shift = pulled(far[k], rows)
        size = jnp.exp(peers * count * base + shift)
        moved = times((size * plane_turn[0], size * plane_turn[1]), h)
        passed = k < lax.axis_index("z")
        h = tuple(jnp.where(passed, m + s, o) for m, s, o in zip(moved, (re, im), h))
    turns = (jnp.ones_like(base), zero)
    for k in range(peers):
        passed = k < place
        turns = tuple(jnp.where(passed, new, old) for new, old in zip(times(turns, turn), turns))
    size = jnp.exp(place * count * base + shift_before)
    moved = times((size * turns[0], size * turns[1]), h)
    return moved[0] + before[0], moved[1] + before[1]


def summed_over(arrays, axis):
    line = jnp.concatenate([a.reshape(-1) for a in arrays]).reshape(-1, 128)
    total = jnp.sum(copies(line, axis), axis=0).reshape(-1)
    done, at = [], 0
    for a in arrays:
        done.append(total[at : at + a.size].reshape(a.shape))
        at += a.size
    return done


def conv_branch(glu, conv_taps, channel_gain):
    reach = conv_taps.shape[0] - 1
    count = glu.shape[0]
    before = next_along(glu[count - 32 :], SP)[32 - reach :]
    extended = jnp.concatenate([before, glu], axis=0).astype(F32)
    raw = jnp.zeros(glu.shape, F32)
    for offset in range(reach + 1):
        raw = raw + conv_taps[offset] * extended[offset : offset + count]
    first, second = summed_over(
        (jnp.sum(raw, axis=1, keepdims=True), jnp.sum(raw * raw, axis=1, keepdims=True)), "tp"
    )
    middle = first / CONV_W
    spread = second / CONV_W - middle * middle
    scaled = (raw - middle) * lax.rsqrt(spread + EPS) * channel_gain
    return jax.nn.silu(scaled).astype(BF16)


def per_device(
    tokens,
    norm_gain,
    proj_state,
    proj_value,
    proj_gate,
    eigen_real,
    eigen_imag,
    log_step,
    decay_shift,
    state_input,
    readout,
    skip_gain,
    init_state,
    conv_taps,
    channel_gain,
    merge_state,
    merge_conv,
):
    place = jnp.stack([lax.axis_index("c"), lax.axis_index("x"), lax.axis_index("tp")]).astype(jnp.int32)
    parts = lax.axis_size("tp")
    count, depth_part = tokens.shape
    depth = depth_part * parts
    half = count // 2
    width = proj_state.shape[1]
    ahead = from_ahead(tokens, "tp", 1)
    behind = from_ahead(tokens, "tp", -1)
    in_z = along_z(proj_state)
    vg_z = along_z(jnp.concatenate([proj_value, proj_gate], axis=1))
    merge_z = along_z(jnp.concatenate([merge_state.T, merge_conv.T], axis=1))
    top = from_ahead(ahead[:half], "tp", 1)
    bottom = from_ahead(behind[half:], "tp", -1)
    in_x = along_x(in_z)
    vg_x = along_x(vg_z)
    merge_x = along_x(merge_z)

    scan_tables, power, reads, device = tables(
        eigen_real, eigen_imag, log_step, decay_shift, state_input, readout, width
    )
    normed = call(
        norm_kernel,
        jax.ShapeDtypeStruct((parts, count, depth_part), BF16),
        (tokens, ahead, top, bottom, behind, norm_gain.reshape(parts, 1, depth_part)),
        scalars=(place,),
        mib=12,
        flops=8 * count * depth,
        bytes_accessed=4 * count * depth,
        transcendentals=count,
    )

    u_in = call(
        state_in_kernel,
        jax.ShapeDtypeStruct((count, width), BF16),
        (normed, in_x, partner(in_x)),
        scalars=(place,),
        scratch=(pltpu.VMEM((depth, width), BF16),),
        mib=12,
        flops=2 * count * depth * width,
        bytes_accessed=4 * depth * count,
        transcendentals=0,
    )
    lanes = eigen_real.size
    chunks = count // CHUNK
    y_local, last = call(
        scan_kernel,
        (
            jax.ShapeDtypeStruct((count, width), F32),
            jax.ShapeDtypeStruct((2 * lanes // 128, 128), F32),
        ),
        (u_in, *scan_tables, skip_gain.reshape(1, -1)),
        scratch=(
            pltpu.VMEM((count, lanes), F32),
            pltpu.VMEM((count, lanes), F32),
            pltpu.VMEM((chunks, lanes), F32),
            pltpu.VMEM((chunks, lanes), F32),
        ),
        mib=24,
        flops=12 * count * width * lanes,
        bytes_accessed=8 * count * lanes,
        transcendentals=0,
    )
    h_re, h_im = carry_in(last, device, count, init_state)

    glu = call(
        glu_kernel,
        jax.ShapeDtypeStruct((count, width), BF16),
        (normed, vg_x, partner(vg_x)),
        scalars=(place,),
        scratch=(pltpu.VMEM((depth, 2 * width), BF16),),
        flops=4 * count * depth * width,
        bytes_accessed=4 * depth * count,
        transcendentals=0,
    )
    conv_out = conv_branch(glu, conv_taps, channel_gain)

    product = call(
        merge_kernel,
        jax.ShapeDtypeStruct((count, depth), BF16),
        (
            y_local,
            power,
            h_re.reshape(1, -1),
            h_im.reshape(1, -1),
            reads,
            conv_out,
            merge_x,
            partner(merge_x),
        ),
        scalars=(place,),
        scratch=(pltpu.VMEM((depth, 2 * width), BF16),),
        flops=4 * count * depth * width,
        bytes_accessed=4 * depth * count,
        transcendentals=0,
    )
    arrived = lax.all_to_all(
        product.reshape(parts, count // parts, depth), "tp", split_axis=0, concat_axis=0, tiled=True
    )
    return arrived.astype(F32).sum(axis=0).astype(BF16)


def finer_mesh(mesh):
    cores = 2
    return Mesh(mesh.devices.reshape(16, 4, cores, mesh.shape["tp"]), SP_TP)


def solution(mesh):
    return jax.shard_map(
        per_device,
        mesh=finer_mesh(mesh),
        in_specs=(
            P(SP, "tp"),
            P(),
            P(SP, "tp"),
            P(SP, "tp"),
            P(SP, "tp"),
            P("tp", None),
            P("tp", None),
            P("tp"),
            P("tp", SP),
            P(None, "tp", None, None),
            P(None, "tp", None, None),
            P("tp"),
            P(None, "tp", None),
            P(None, "tp"),
            P("tp"),
            P("tp", SP),
            P("tp", SP),
        ),
        out_specs=P(SP_TP, None),
        check_vma=False,
    )
```

```python
import jax
import jax.numpy as jnp
from jax import lax
from jax.experimental import pallas as pl
from jax.experimental.pallas import tpu as pltpu
from jax.sharding import Mesh
from jax.sharding import PartitionSpec as P


CONV_W = 1024
SP = ("z", "x", "c")
SP_TP = ("z", "x", "c", "tp")
CHUNK = 32
EPS = 1e-06
EXACT = lax.Precision.HIGHEST
F32 = jnp.float32
BF16 = jnp.bfloat16


def copies(value, axis):
    peers = lax.axis_size(axis)
    return lax.all_to_all(
        jnp.broadcast_to(value[None], (peers, *value.shape)), axis, 0, 0, tiled=True
    )


def next_along(block, axis):
    count = lax.axis_size(axis)
    return lax.ppermute(block, axis, [(i, i + 1) for i in range(count - 1)])


def partner(block):
    return lax.ppermute(block, "c", [(0, 1), (1, 0)])


def from_ahead(block, axis, distance):
    count = lax.axis_size(axis)
    return lax.ppermute(block, axis, [(i, (i - distance) % count) for i in range(count)])


def from_own_on(planes, axis):
    peers = lax.axis_size(axis)
    return jnp.stack([planes] + [from_ahead(planes, axis, d) for d in range(1, peers)])


def whole_specs(arrays):
    return [pl.BlockSpec(memory_space=pltpu.VMEM) for _ in arrays]


def call(body, outs, arrays, scalars=(), scratch=(), mib=16, **costs):
    return pl.pallas_call(
        body,
        compiler_params=pltpu.CompilerParams(vmem_limit_bytes=mib * 2**20),
        out_shape=outs,
        in_specs=[pl.BlockSpec(memory_space=pltpu.SMEM) for _ in scalars] + whole_specs(arrays),
        out_specs=jax.tree.map(lambda _: pl.BlockSpec(memory_space=pltpu.VMEM), outs),
        scratch_shapes=list(scratch),
        cost_estimate=pl.CostEstimate(**costs) if costs else None,
    )(*scalars, *arrays)


def natural_order(place_ref, own_ref, other_ref, into_ref, turned, first_lane=0, from_own_x=False):
    peers_x, _, rows, _ = own_ref.shape
    blocks = into_ref.shape[0] // rows
    lanes = slice(first_lane, first_lane + into_ref.shape[1])
    core, part = place_ref[0], place_ref[2]
    place_x = place_ref[1] if from_own_x else 0
    first = part * turned

    def place(by_core):
        for k in range(blocks):
            at = lax.rem(first + k, blocks)
            x = lax.rem(lax.div(at, 2) - place_x + 2 * peers_x, peers_x)
            into_ref[k * rows : (k + 1) * rows, :] = by_core[k % 2][
                x, lax.div(at, 2 * peers_x), :, lanes
            ]

    @pl.when(core == 0)
    def _():
        place((own_ref, other_ref))

    @pl.when(core == 1)
    def _():
        place((other_ref, own_ref))


def dot_rows(a, b):
    return lax.dot_general(a, b, (((1,), (1,)), ((), ())), preferred_element_type=F32)


def norm_kernel(place_ref, own_ref, ahead_ref, top_ref, bottom_ref, behind_ref, gain_ref, out_ref):
    parts, count, depth = out_ref.shape
    half = count // 2
    part = place_ref[2]

    def rows_of(at, opposite_ref):
        rows = pl.ds(at, half)
        blocks = [
            ref.astype(F32)
            for ref in (own_ref[rows], ahead_ref[rows], opposite_ref[...], behind_ref[rows])
        ]
        power = sum(jnp.sum(block * block, axis=1, keepdims=True) for block in blocks)
        scale = lax.rsqrt(power / (parts * depth) + EPS)
        for p, block in enumerate(blocks):
            gain = gain_ref[lax.rem(part + p, parts)]
            out_ref[p, rows] = (block * scale * gain).astype(BF16)

    rows_of(0, top_ref)
    rows_of(half, bottom_ref)


def projected(normed_ref, weight_ref):
    parts, _, depth = normed_ref.shape
    return sum(
        jnp.dot(
            normed_ref[p],
            weight_ref[p * depth : (p + 1) * depth],
            preferred_element_type=F32,
        )
        for p in range(parts)
    )


def state_in_kernel(place_ref, normed_ref, own_ref, other_ref, out_ref, weight_ref):
    parts = normed_ref.shape[0]
    turned = weight_ref.shape[0] // own_ref.shape[2] // parts
    natural_order(place_ref, own_ref, other_ref, weight_ref, turned)
    out_ref[...] = projected(normed_ref, weight_ref).astype(BF16)


def glu_kernel(place_ref, normed_ref, own_ref, other_ref, out_ref, weight_ref):
    parts = normed_ref.shape[0]
    turned = weight_ref.shape[0] // own_ref.shape[2] // parts
    width = out_ref.shape[1]
    natural_order(place_ref, own_ref, other_ref, weight_ref, turned, first_lane=width)
    both = projected(normed_ref, weight_ref)
    value = both[:, :width].astype(BF16).astype(F32)
    gate = both[:, width:].astype(BF16).astype(F32)
    out_ref[...] = (value * jax.nn.sigmoid(gate)).astype(BF16)


def squared(re, im):
    return re * re - im * im, 2.0 * re * im


def times(a, b):
    return a[0] * b[0] - a[1] * b[1], a[0] * b[1] + a[1] * b[0]


def exact_dot(a, b):
    return jnp.dot(a, b, preferred_element_type=F32, precision=EXACT)


def spread_over(groups, each):
    row = lax.broadcasted_iota(jnp.int32, (groups, groups * each), 0)
    col = lax.broadcasted_iota(jnp.int32, (groups, groups * each), 1) // each
    return (row == col).astype(F32)


def write_diagonal(out_ref, at, blocks, groups):
    rows, cols = blocks.shape
    pair = jnp.concatenate([blocks, blocks], axis=1)
    row_group = lax.broadcasted_iota(jnp.int32, pair.shape, 0) // (rows // groups)
    col_group = lax.broadcasted_iota(jnp.int32, pair.shape, 1) // cols
    for k in range(groups // 2):
        mine = row_group == col_group + 2 * k
        out_ref[:, at + 2 * k * cols : at + 2 * (k + 1) * cols] = jnp.where(mine, pair, 0.0).astype(BF16)


def table_kernel(
    shift_ref,
    base_ref,
    cos_ref,
    sin_ref,
    start_cos_ref,
    start_sin_ref,
    b_re_ref,
    b_im_ref,
    c_re_ref,
    c_im_ref,
    grow_ref,
    shrink_ref,
    into_ref,
    out_ref,
    hop_re_ref,
    hop_im_ref,
    power_ref,
    total_ref,
):
    groups, count = shift_ref.shape
    lanes = base_ref.shape[1]
    width = grow_ref.shape[1]
    chunks = count // CHUNK
    base = base_ref[...]
    row = lax.broadcasted_iota(jnp.int32, (count, count), 0)
    col = lax.broadcasted_iota(jnp.int32, (count, count), 1)
    earlier = row >= col
    inside = earlier & (row // CHUNK == col // CHUNK)

    def run(which):
        return lax.dot_general(
            which.astype(F32),
            shift_ref[...],
            (((1,), (1,)), ((), ())),
            precision=EXACT,
            preferred_element_type=F32,
        )

    partial, whole = run(inside), run(earlier)
    narrow = exact_dot(partial, spread_over(groups, width // groups))
    grow_ref[...] = jnp.exp(narrow)
    shrink_ref[...] = jnp.exp(-narrow)
    spread = spread_over(groups, lanes // groups)
    wide = exact_dot(whole, spread)
    wide_last = wide[count - 1 :]
    for k in range(lanes // 128):
        total_ref[k : k + 1, :] = wide_last[:, k * 128 : (k + 1) * 128]
    sums = jnp.concatenate([partial[(c + 1) * CHUNK - 1 : (c + 1) * CHUNK] for c in range(chunks)])
    near = exact_dot(sums, spread)
    index = lax.broadcasted_iota(jnp.int32, (chunks, lanes), 0)
    size = jnp.exp(CHUNK * base + near)
    turn = (start_cos_ref[1:2], start_sin_ref[1:2])
    hop_re_ref[0], hop_im_ref[0] = size * turn[0], size * turn[1]
    distance, level = 1, 1
    while distance < chunks:
        size = jnp.where(index >= distance, jnp.exp(distance * CHUNK * base + near), 0.0)
        turn = (start_cos_ref[distance : distance + 1], start_sin_ref[distance : distance + 1])
        hop_re_ref[level], hop_im_ref[level] = size * turn[0], size * turn[1]
        near = near + jnp.where(index >= distance, pltpu.roll(near, distance, 0), 0.0)
        distance, level = distance * 2, level + 1
    counts = lax.broadcasted_iota(jnp.int32, (CHUNK, 1), 0).astype(F32)
    inner = (cos_ref[...], sin_ref[...])
    for c in range(chunks):
        at = slice(c * CHUNK, (c + 1) * CHUNK)
        size = jnp.exp((counts + (c * CHUNK + 1)) * base + wide[at])
        turn = times((start_cos_ref[c : c + 1], start_sin_ref[c : c + 1]), inner)
        power_ref[at, :lanes] = (size * turn[0]).astype(BF16)
        power_ref[at, lanes:] = (size * turn[1]).astype(BF16)
    write_diagonal(into_ref, 0, b_re_ref[...], groups)
    write_diagonal(into_ref, lanes, b_im_ref[...], groups)
    write_diagonal(out_ref, 0, c_re_ref[...], groups)
    write_diagonal(out_ref, lanes, -c_im_ref[...], groups)


def scan_kernel(
    u_ref,
    grow_ref,
    shrink_ref,
    in_ref,
    out_mat_ref,
    fwd_re_ref,
    fwd_im_ref,
    inv_re_ref,
    inv_im_ref,
    hop_re_ref,
    hop_im_ref,
    lower_ref,
    skip_ref,
    y_ref,
    last_ref,
    cum_re_ref,
    cum_im_ref,
    end_re_ref,
    end_im_ref,
):
    count, _ = u_ref.shape
    states = fwd_re_ref.shape[1]
    chunks = count // CHUNK
    block = lower_ref.shape[0]
    slab = 256
    u = u_ref[...].astype(F32)
    scaled = (u * shrink_ref[...]).astype(BF16)

    def chunked(value):
        return value.reshape(chunks, CHUNK, slab)

    def summed(value):
        value = value.reshape(count, slab).astype(BF16)
        return jnp.concatenate(
            [
                jnp.dot(lower_ref[...], value[k : k + block], preferred_element_type=F32)
                for k in range(0, count, block)
            ]
        )

    def first_pass(j, _):
        at = pl.ds(pl.multiple_of(j * slab, slab), slab)
        at_im = pl.ds(pl.multiple_of(states + j * slab, slab), slab)
        d_re = chunked(jnp.dot(scaled, in_ref[:, at], preferred_element_type=F32))
        d_im = chunked(jnp.dot(scaled, in_ref[:, at_im], preferred_element_type=F32))
        i_re, i_im = inv_re_ref[:, at][None], inv_im_ref[:, at][None]
        cum_re = summed(i_re * d_re - i_im * d_im)
        cum_im = summed(i_re * d_im + i_im * d_re)
        cum_re_ref[:, at] = cum_re
        cum_im_ref[:, at] = cum_im
        end_re_ref[:, at] = chunked(cum_re)[:, CHUNK - 1]
        end_im_ref[:, at] = chunked(cum_im)[:, CHUNK - 1]
        return 0

    lax.fori_loop(0, states // slab, first_pass, 0)

    h_re, h_im = hop_re_ref[0], hop_im_ref[0]
    t_re, t_im = end_re_ref[...], end_im_ref[...]
    s_re = h_re * t_re - h_im * t_im
    s_im = h_re * t_im + h_im * t_re
    for level in range(1, hop_re_ref.shape[0]):
        h_re, h_im = hop_re_ref[level], hop_im_ref[level]
        p_re, p_im = pltpu.roll(s_re, 1 << (level - 1), 0), pltpu.roll(s_im, 1 << (level - 1), 0)
        s_re, s_im = s_re + h_re * p_re - h_im * p_im, s_im + h_re * p_im + h_im * p_re
    lanes = last_ref.shape[1]
    for k in range(states // lanes):
        last_ref[k : k + 1, :] = s_re[chunks - 1 :, k * lanes : (k + 1) * lanes]
        row = states // lanes + k
        last_ref[row : row + 1, :] = s_im[chunks - 1 :, k * lanes : (k + 1) * lanes]
    begins = lax.broadcasted_iota(jnp.int32, s_re.shape, 0) > 0
    end_re_ref[...] = jnp.where(begins, pltpu.roll(s_re, 1, 0), 0.0)
    end_im_ref[...] = jnp.where(begins, pltpu.roll(s_im, 1, 0), 0.0)
    y_ref[...] = jnp.zeros(y_ref.shape, F32)

    def second_pass(j, _):
        at = pl.ds(pl.multiple_of(j * slab, slab), slab)
        at_im = pl.ds(pl.multiple_of(states + j * slab, slab), slab)
        t_re = chunked(cum_re_ref[:, at]) + end_re_ref[:, at][:, None]
        t_im = chunked(cum_im_ref[:, at]) + end_im_ref[:, at][:, None]
        f_re, f_im = fwd_re_ref[:, at][None], fwd_im_ref[:, at][None]
        x_re = (f_re * t_re - f_im * t_im).reshape(count, slab).astype(BF16)
        x_im = (f_re * t_im + f_im * t_re).reshape(count, slab).astype(BF16)
        y_ref[...] += dot_rows(x_re, out_mat_ref[:, at]) + dot_rows(x_im, out_mat_ref[:, at_im])
        return 0

    lax.fori_loop(0, states // slab, second_pass, 0)
    y_ref[...] = y_ref[...] * grow_ref[...] + skip_ref[...] * u


def merge_kernel(
    place_ref,
    y_ref,
    power_ref,
    h_re_ref,
    h_im_ref,
    read_ref,
    conv_ref,
    own_ref,
    other_ref,
    out_ref,
    weight_ref,
):
    natural_order(place_ref, own_ref, other_ref, weight_ref, 0, from_own_x=True)
    lanes = h_re_ref.shape[1]
    h_re, h_im = h_re_ref[...], h_im_ref[...]
    c_re, c_im = read_ref[:, :lanes].astype(F32), read_ref[:, lanes:].astype(F32)
    total = (
        y_ref[...]
        + dot_rows(power_ref[:, :lanes], (c_re * h_re + c_im * h_im).astype(BF16))
        + dot_rows(power_ref[:, lanes:], (c_im * h_re - c_re * h_im).astype(BF16))
    )
    ssm = jax.nn.gelu(total).astype(BF16)
    both = jnp.concatenate([ssm, conv_ref[...]], axis=1)
    out_ref[...] = dot_rows(both, weight_ref[...]).astype(BF16)


def input_matrix(eigen_real, eigen_imag, step, state_input):
    base = eigen_real * step[:, None]
    theta = eigen_imag * step[:, None]
    magnitude = jnp.exp(base)
    near_re = magnitude * jnp.cos(theta) - 1.0
    near_im = magnitude * jnp.sin(theta)
    modulus = eigen_real * eigen_real + eigen_imag * eigen_imag
    ratio_re = (near_re * eigen_real + near_im * eigen_imag) / modulus
    ratio_im = (near_im * eigen_real - near_re * eigen_imag) / modulus
    in_re, in_im = state_input[0], state_input[1]
    return (
        ratio_re[:, None, :] * in_re - ratio_im[:, None, :] * in_im,
        ratio_re[:, None, :] * in_im + ratio_im[:, None, :] * in_re,
    )


def tables(eigen_real, eigen_imag, log_step, decay_shift, state_input, readout, width):
    groups, states = eigen_real.shape
    lanes = groups * states
    count = decay_shift.shape[1]
    chunks = count // CHUNK
    step = jnp.exp(log_step)
    base = (eigen_real * step[:, None]).reshape(1, lanes)
    theta = (eigen_imag * step[:, None]).reshape(1, lanes)
    inside = jnp.arange(1, CHUNK + 1, dtype=F32)[:, None]
    level, angle = inside * base, inside * theta
    cosine, sine = jnp.cos(angle), jnp.sin(angle)
    grow, shrink = jnp.exp(level), jnp.exp(-level)
    forward = (grow * cosine, grow * sine)
    inverse = (shrink * cosine, -shrink * sine)
    starts = jnp.arange(chunks).astype(F32)[:, None] * CHUNK * theta
    start_cos, start_sin = jnp.cos(starts), jnp.sin(starts)
    whole_turn = (start_cos[chunks // 2], start_sin[chunks // 2])
    b_re, b_im = input_matrix(eigen_real, eigen_imag, step, state_input)
    rows = (groups * state_input.shape[2], states)
    levels = 1 + (chunks - 1).bit_length()
    block = min(count, 256)
    at = jnp.arange(block)
    lower_block = (
        (at[:, None] >= at[None, :]) & (at[:, None] // CHUNK == at[None, :] // CHUNK)
    ).astype(BF16)
    grow, shrink, into, out, hop_re, hop_im, power, total = call(
        table_kernel,
        (
            jax.ShapeDtypeStruct((count, width), F32),
            jax.ShapeDtypeStruct((count, width), F32),
            jax.ShapeDtypeStruct((width, 2 * lanes), BF16),
            jax.ShapeDtypeStruct((width, 2 * lanes), BF16),
            jax.ShapeDtypeStruct((levels, chunks, lanes), F32),
            jax.ShapeDtypeStruct((levels, chunks, lanes), F32),
            jax.ShapeDtypeStruct((count, 2 * lanes), BF16),
            jax.ShapeDtypeStruct((lanes // 128, 128), F32),
        ),
        (
            decay_shift,
            base,
            cosine,
            sine,
            start_cos,
            start_sin,
            b_re.reshape(rows),
            b_im.reshape(rows),
            readout[0].reshape(rows),
            readout[1].reshape(rows),
        ),
        mib=24,
        flops=20 * count * count * groups,
        bytes_accessed=8 * count * lanes,
        transcendentals=count * lanes,
    )
    device = dict(
        base=base.reshape(-1, 128),
        turn=squared(*(r.reshape(-1, 128) for r in whole_turn)),
        shift=total,
    )
    scan = (grow, shrink, into, out, *forward, *inverse, hop_re, hop_im, lower_block)
    return scan, power, out, device


def pulled(packed, rows):
    return packed[:rows], packed[rows : 2 * rows], packed[2 * rows :]


def carry_in(last, device, count, init_state):
    rows = device["base"].shape[0]
    base, turn = device["base"], device["turn"]
    plane = ("x", "c")
    packed = jnp.concatenate([last, device["shift"]])
    near = copies(packed, plane)
    peers, place = lax.axis_size(plane), lax.axis_index(plane)
    zero = jnp.zeros_like(base)
    run = (zero, zero)
    before, shift_before = run, zero
    shift_run = zero
    for k in range(peers):
        re, im, shift = pulled(near[k], rows)
        size = jnp.exp(count * base + shift)
        moved = times((size * turn[0], size * turn[1]), run)
        run = (moved[0] + re, moved[1] + im)
        shift_run = shift_run + shift
        passed = k < place
        before = jax.tree.map(lambda new, old: jnp.where(passed, new, old), run, before)
        shift_before = jnp.where(passed, shift_run, shift_before)
    far = copies(jnp.concatenate([*run, shift_run]), "z")
    plane_turn, at = turn, 1
    while at < peers:
        plane_turn, at = squared(*plane_turn), at * 2
    h = tuple(s.reshape(-1, 128) for s in (init_state[0], init_state[1]))
    for k in range(lax.axis_size("z")):
        re, im, shift = pulled(far[k], rows)
        size = jnp.exp(peers * count * base + shift)
        moved = times((size * plane_turn[0], size * plane_turn[1]), h)
        passed = k < lax.axis_index("z")
        h = tuple(jnp.where(passed, m + s, o) for m, s, o in zip(moved, (re, im), h))
    turns = (jnp.ones_like(base), zero)
    for k in range(peers):
        passed = k < place
        turns = tuple(jnp.where(passed, new, old) for new, old in zip(times(turns, turn), turns))
    size = jnp.exp(place * count * base + shift_before)
    moved = times((size * turns[0], size * turns[1]), h)
    return moved[0] + before[0], moved[1] + before[1]


def summed_over(arrays, axis):
    line = jnp.concatenate([a.reshape(-1) for a in arrays]).reshape(-1, 128)
    others = [from_ahead(line, axis, d) for d in range(1, lax.axis_size(axis))]
    total = sum(others, line).reshape(-1)
    done, at = [], 0
    for a in arrays:
        done.append(total[at : at + a.size].reshape(a.shape))
        at += a.size
    return done


def conv_branch(glu, conv_taps, channel_gain):
    reach = conv_taps.shape[0] - 1
    count = glu.shape[0]
    before = next_along(glu[count - 32 :], SP)
    before = before[32 - reach :]
    extended = jnp.concatenate([before, glu], axis=0).astype(F32)
    raw = jnp.zeros(glu.shape, F32)
    for offset in range(reach + 1):
        raw = raw + conv_taps[offset] * extended[offset : offset + count]
    first, second = summed_over(
        (jnp.sum(raw, axis=1, keepdims=True), jnp.sum(raw * raw, axis=1, keepdims=True)), "tp"
    )
    middle = first / CONV_W
    spread = second / CONV_W - middle * middle
    scaled = (raw - middle) * lax.rsqrt(spread + EPS) * channel_gain
    return jax.nn.silu(scaled).astype(BF16)


def mixer(
    tokens,
    norm_gain,
    proj_state,
    proj_value,
    proj_gate,
    eigen_real,
    eigen_imag,
    log_step,
    decay_shift,
    state_input,
    readout,
    skip_gain,
    init_state,
    conv_taps,
    channel_gain,
    merge_state,
    merge_conv,
):
    place = jnp.stack([lax.axis_index("c"), lax.axis_index("x"), lax.axis_index("tp")]).astype(jnp.int32)
    parts = lax.axis_size("tp")
    count, depth_part = tokens.shape
    depth = depth_part * parts
    half = count // 2
    width = proj_state.shape[1]
    merged = jnp.concatenate([merge_state, merge_conv]).T
    planes = copies(
        jnp.concatenate([proj_state, proj_value, proj_gate, merged], axis=1), "z"
    )
    ahead = from_ahead(tokens, "tp", 1)
    behind = from_ahead(tokens, "tp", -1)
    top = from_ahead(ahead[:half], "tp", 1)
    bottom = from_ahead(behind[half:], "tp", -1)
    scan_tables, power, reads, device = tables(
        eigen_real, eigen_imag, log_step, decay_shift, state_input, readout, width
    )
    normed = call(
        norm_kernel,
        jax.ShapeDtypeStruct((parts, count, depth_part), BF16),
        (tokens, ahead, top, bottom, behind, norm_gain.reshape(parts, 1, depth_part)),
        scalars=(place,),
        mib=12,
        flops=8 * count * depth,
        bytes_accessed=4 * count * depth,
        transcendentals=count,
    )
    planes, normed, _ = lax.optimization_barrier((planes, normed, device["shift"]))
    project_x = copies(planes[:, :, : 3 * width], "x")
    merge_x = from_own_on(planes[:, :, 3 * width :], "x")
    project_other = partner(project_x)
    merge_other = partner(merge_x)

    u_in = call(
        state_in_kernel,
        jax.ShapeDtypeStruct((count, width), BF16),
        (normed, project_x, project_other),
        scalars=(place,),
        scratch=(pltpu.VMEM((depth, width), BF16),),
        mib=12,
        flops=2 * count * depth * width,
        bytes_accessed=4 * depth * count,
        transcendentals=0,
    )
    lanes = eigen_real.size
    chunks = count // CHUNK
    y_local, last = call(
        scan_kernel,
        (
            jax.ShapeDtypeStruct((count, width), F32),
            jax.ShapeDtypeStruct((2 * lanes // 128, 128), F32),
        ),
        (u_in, *scan_tables, skip_gain.reshape(1, -1)),
        scratch=(
            pltpu.VMEM((count, lanes), F32),
            pltpu.VMEM((count, lanes), F32),
            pltpu.VMEM((chunks, lanes), F32),
            pltpu.VMEM((chunks, lanes), F32),
        ),
        mib=24,
        flops=12 * count * width * lanes,
        bytes_accessed=8 * count * lanes,
        transcendentals=0,
    )
    h_re, h_im = carry_in(last, device, count, init_state)

    glu = call(
        glu_kernel,
        jax.ShapeDtypeStruct((count, width), BF16),
        (normed, project_x, project_other),
        scalars=(place,),
        scratch=(pltpu.VMEM((depth, 2 * width), BF16),),
        flops=4 * count * depth * width,
        bytes_accessed=4 * depth * count,
        transcendentals=0,
    )
    conv_out = conv_branch(glu, conv_taps, channel_gain)

    product = call(
        merge_kernel,
        jax.ShapeDtypeStruct((count, depth), BF16),
        (
            y_local,
            power,
            h_re.reshape(1, -1),
            h_im.reshape(1, -1),
            reads,
            conv_out,
            merge_x,
            merge_other,
        ),
        scalars=(place,),
        scratch=(pltpu.VMEM((depth, 2 * width), BF16),),
        flops=4 * count * depth * width,
        bytes_accessed=4 * depth * count,
        transcendentals=0,
    )
    arrived = lax.all_to_all(
        product.reshape(parts, count // parts, depth), "tp", split_axis=0, concat_axis=0, tiled=True
    )
    return arrived.astype(F32).sum(axis=0).astype(BF16)


def finer_mesh(mesh):
    cores = 2
    return Mesh(mesh.devices.reshape(16, 4, cores, mesh.shape["tp"]), SP_TP)


def solution(mesh):
    return jax.shard_map(
        mixer,
        mesh=finer_mesh(mesh),
        in_specs=(
            P(SP, "tp"),
            P(),
            P(SP, "tp"),
            P(SP, "tp"),
            P(SP, "tp"),
            P("tp", None),
            P("tp", None),
            P("tp"),
            P("tp", SP),
            P(None, "tp", None, None),
            P(None, "tp", None, None),
            P("tp"),
            P(None, "tp", None),
            P(None, "tp"),
            P("tp"),
            P("tp", SP),
            P("tp", SP),
        ),
        out_specs=P(SP_TP, None),
        check_vma=False,
    )
```

```python
import jax
import jax.numpy as jnp
from jax import lax
from jax.experimental import pallas as pl
from jax.experimental.pallas import tpu as pltpu
from jax.sharding import Mesh
from jax.sharding import PartitionSpec as P


CONV_W = 1024
SP = ("z", "x", "c")
SP_TP = ("z", "x", "c", "tp")
CHUNK = 32
HALO = 32
EPS = 1e-06
EXACT = lax.Precision.HIGHEST
F32 = jnp.float32
BF16 = jnp.bfloat16


def copies(value, axis):
    peers = lax.axis_size(axis)
    return lax.all_to_all(
        jnp.broadcast_to(value[None], (peers, *value.shape)), axis, 0, 0, tiled=True
    )


def next_along(block, axis):
    count = lax.axis_size(axis)
    return lax.ppermute(block, axis, [(i, i + 1) for i in range(count - 1)])


def partner(block):
    return lax.ppermute(block, "c", [(0, 1), (1, 0)])


def from_ahead(block, axis, distance):
    count = lax.axis_size(axis)
    return lax.ppermute(block, axis, [(i, (i - distance) % count) for i in range(count)])


def from_own_on(planes, axis):
    peers = lax.axis_size(axis)
    return jnp.stack([planes] + [from_ahead(planes, axis, d) for d in range(1, peers)])


def far_from_core(*arrays):
    return [pltpu.with_memory_space_constraint(array, pltpu.HBM) for array in arrays]


def whole_specs(arrays):
    return [pl.BlockSpec(memory_space=pltpu.VMEM) for _ in arrays]


def call(body, outs, arrays, scalars=(), scratch=(), mib=16, space=pltpu.VMEM, **costs):
    return pl.pallas_call(
        body,
        compiler_params=pltpu.CompilerParams(vmem_limit_bytes=mib * 2**20),
        out_shape=outs,
        in_specs=[pl.BlockSpec(memory_space=pltpu.SMEM) for _ in scalars] + whole_specs(arrays),
        out_specs=jax.tree.map(lambda _: pl.BlockSpec(memory_space=space), outs),
        scratch_shapes=list(scratch),
        cost_estimate=pl.CostEstimate(**costs) if costs else None,
    )(*scalars, *arrays)


def natural_order(place_ref, own_ref, other_ref, into_ref, turned, first_lane=0, from_own_x=False):
    peers_x, _, rows, _ = own_ref.shape
    blocks = into_ref.shape[0] // rows
    lanes = slice(first_lane, first_lane + into_ref.shape[1])
    core, part = place_ref[0], place_ref[2]
    place_x = place_ref[1] if from_own_x else 0
    first = part * turned

    def place(by_core):
        for k in range(blocks):
            at = lax.rem(first + k, blocks)
            x = lax.rem(lax.div(at, 2) - place_x + 2 * peers_x, peers_x)
            into_ref[k * rows : (k + 1) * rows, :] = by_core[k % 2][
                x, lax.div(at, 2 * peers_x), :, lanes
            ]

    @pl.when(core == 0)
    def _():
        place((own_ref, other_ref))

    @pl.when(core == 1)
    def _():
        place((other_ref, own_ref))


def dot_rows(a, b):
    return lax.dot_general(a, b, (((1,), (1,)), ((), ())), preferred_element_type=F32)


def norm_kernel(place_ref, own_ref, ahead_ref, top_ref, bottom_ref, behind_ref, gain_ref, out_ref):
    parts, count, depth = out_ref.shape
    half = count // 2
    part = place_ref[2]

    def rows_of(at, opposite_ref):
        rows = pl.ds(at, half)
        blocks = [
            block.astype(F32)
            for block in (own_ref[rows], ahead_ref[rows], opposite_ref[...], behind_ref[rows])
        ]
        power = sum(jnp.sum(block * block, axis=1, keepdims=True) for block in blocks)
        scale = lax.rsqrt(power / (parts * depth) + EPS)
        for p, block in enumerate(blocks):
            gain = gain_ref[lax.rem(part + p, parts)]
            out_ref[p, rows] = (block * scale * gain).astype(BF16)

    rows_of(0, top_ref)
    rows_of(half, bottom_ref)


def projected(normed_ref, weight_ref, rows):
    parts, _, depth = normed_ref.shape
    return sum(
        jnp.dot(
            normed_ref[p, rows],
            weight_ref[p * depth : (p + 1) * depth],
            preferred_element_type=F32,
        )
        for p in range(parts)
    )


def state_in_kernel(place_ref, normed_ref, own_ref, other_ref, out_ref, weight_ref):
    parts, rows, _ = normed_ref.shape
    turned = weight_ref.shape[0] // own_ref.shape[2] // parts
    natural_order(place_ref, own_ref, other_ref, weight_ref, turned)
    out_ref[...] = projected(normed_ref, weight_ref, slice(HALO, rows)).astype(BF16)


def conv_kernel(
    place_ref, normed_ref, own_ref, other_ref, taps_ref, raw_ref, sums_ref, weight_ref, glu_ref, shifted_ref
):
    parts, rows, _ = normed_ref.shape
    count, width = raw_ref.shape
    turned = weight_ref.shape[0] // own_ref.shape[2] // parts
    natural_order(place_ref, own_ref, other_ref, weight_ref, turned, first_lane=width)
    both = projected(normed_ref, weight_ref, slice(0, rows))
    value = both[:, :width].astype(BF16).astype(F32)
    gate = both[:, width:].astype(BF16).astype(F32)
    glu_ref[:rows] = (value * jax.nn.sigmoid(gate)).astype(BF16).astype(F32)
    glu_ref[rows:] = jnp.zeros((glu_ref.shape[0] - rows, width), F32)
    taps = taps_ref.shape[0]
    sublanes = 8
    for k in range(sublanes):
        shifted_ref[k] = glu_ref[k : k + rows]
    first = HALO - (taps - 1)
    step = 64

    def some_rows(n, _):
        at = pl.multiple_of(n * step, step)
        total = jnp.zeros((step, width), F32)
        for k in range(taps):
            shift, whole = (first + k) % sublanes, (first + k) // sublanes * sublanes
            total = total + taps_ref[k : k + 1] * shifted_ref[shift, pl.ds(at + whole, step)]
        raw_ref[pl.ds(at, step)] = total
        return 0

    lax.fori_loop(0, count // step, some_rows, 0)
    raw = raw_ref[...]
    ones = jnp.ones((8, width), F32)

    def across(value):
        return lax.dot_general(
            ones, value, (((1,), (1,)), ((), ())), precision=EXACT, preferred_element_type=F32
        )[:1]

    sums_ref[0:1] = across(raw)
    sums_ref[1:2] = across(raw * raw)


def squared(re, im):
    return re * re - im * im, 2.0 * re * im


def times(a, b):
    return a[0] * b[0] - a[1] * b[1], a[0] * b[1] + a[1] * b[0]


def exact_dot(a, b):
    return jnp.dot(a, b, preferred_element_type=F32, precision=EXACT)


def spread_over(groups, each):
    row = lax.broadcasted_iota(jnp.int32, (groups, groups * each), 0)
    col = lax.broadcasted_iota(jnp.int32, (groups, groups * each), 1) // each
    return (row == col).astype(F32)


def write_diagonal(out_ref, at, blocks, groups):
    rows, cols = blocks.shape
    pair = jnp.concatenate([blocks, blocks], axis=1)
    row_group = lax.broadcasted_iota(jnp.int32, pair.shape, 0) // (rows // groups)
    col_group = lax.broadcasted_iota(jnp.int32, pair.shape, 1) // cols
    for k in range(groups // 2):
        mine = row_group == col_group + 2 * k
        out_ref[:, at + 2 * k * cols : at + 2 * (k + 1) * cols] = jnp.where(mine, pair, 0.0).astype(BF16)


def table_kernel(*refs):
    inputs, hbm, vmem, done = refs[:10], refs[10:18], refs[18:26], refs[26]

    def send(*which):
        for k in which:
            pltpu.make_async_copy(vmem[k], hbm[k], done.at[k]).start()

    fill_tables(send, *inputs, *vmem)
    for k in range(len(vmem)):
        pltpu.make_async_copy(vmem[k], hbm[k], done.at[k]).wait()


def fill_tables(
    send,
    shift_ref,
    base_ref,
    cos_ref,
    sin_ref,
    start_cos_ref,
    start_sin_ref,
    b_re_ref,
    b_im_ref,
    c_re_ref,
    c_im_ref,
    grow_ref,
    shrink_ref,
    into_ref,
    out_ref,
    hop_re_ref,
    hop_im_ref,
    power_ref,
    total_ref,
):
    groups, count = shift_ref.shape
    lanes = base_ref.shape[1]
    width = grow_ref.shape[1]
    chunks = count // CHUNK
    base = base_ref[...]
    row = lax.broadcasted_iota(jnp.int32, (count, count), 0)
    col = lax.broadcasted_iota(jnp.int32, (count, count), 1)
    earlier = row >= col
    inside = earlier & (row // CHUNK == col // CHUNK)

    def run(which):
        return lax.dot_general(
            which.astype(F32),
            shift_ref[...],
            (((1,), (1,)), ((), ())),
            precision=EXACT,
            preferred_element_type=F32,
        )

    partial, whole = run(inside), run(earlier)
    narrow = exact_dot(partial, spread_over(groups, width // groups))
    grow_ref[...] = jnp.exp(narrow)
    shrink_ref[...] = jnp.exp(-narrow)
    spread = spread_over(groups, lanes // groups)
    wide = exact_dot(whole, spread)
    wide_last = wide[count - 1 :]
    send(0, 1)
    for k in range(lanes // 128):
        total_ref[k : k + 1, :] = wide_last[:, k * 128 : (k + 1) * 128]
    sums = jnp.concatenate([partial[(c + 1) * CHUNK - 1 : (c + 1) * CHUNK] for c in range(chunks)])
    near = exact_dot(sums, spread)
    index = lax.broadcasted_iota(jnp.int32, (chunks, lanes), 0)
    size = jnp.exp(CHUNK * base + near)
    turn = (start_cos_ref[1:2], start_sin_ref[1:2])
    hop_re_ref[0], hop_im_ref[0] = size * turn[0], size * turn[1]
    distance, level = 1, 1
    while distance < chunks:
        size = jnp.where(index >= distance, jnp.exp(distance * CHUNK * base + near), 0.0)
        turn = (start_cos_ref[distance : distance + 1], start_sin_ref[distance : distance + 1])
        hop_re_ref[level], hop_im_ref[level] = size * turn[0], size * turn[1]
        near = near + jnp.where(index >= distance, pltpu.roll(near, distance, 0), 0.0)
        distance, level = distance * 2, level + 1
    send(4, 5, 7)
    counts = lax.broadcasted_iota(jnp.int32, (CHUNK, 1), 0).astype(F32)
    inner = (cos_ref[...], sin_ref[...])
    for c in range(chunks):
        at = slice(c * CHUNK, (c + 1) * CHUNK)
        size = jnp.exp((counts + (c * CHUNK + 1)) * base + wide[at])
        turn = times((start_cos_ref[c : c + 1], start_sin_ref[c : c + 1]), inner)
        power_ref[at, :lanes] = (size * turn[0]).astype(BF16)
        power_ref[at, lanes:] = (size * turn[1]).astype(BF16)
    send(6)
    write_diagonal(into_ref, 0, b_re_ref[...], groups)
    write_diagonal(into_ref, lanes, b_im_ref[...], groups)
    send(2)
    write_diagonal(out_ref, 0, c_re_ref[...], groups)
    write_diagonal(out_ref, lanes, -c_im_ref[...], groups)
    send(3)


def scan_kernel(
    u_ref,
    grow_ref,
    shrink_ref,
    in_ref,
    out_mat_ref,
    fwd_re_ref,
    fwd_im_ref,
    inv_re_ref,
    inv_im_ref,
    hop_re_ref,
    hop_im_ref,
    lower_ref,
    skip_ref,
    y_ref,
    last_ref,
    cum_re_ref,
    cum_im_ref,
    end_re_ref,
    end_im_ref,
):
    count, _ = u_ref.shape
    states = fwd_re_ref.shape[1]
    chunks = count // CHUNK
    block = lower_ref.shape[0]
    slab = 256
    u = u_ref[...].astype(F32)
    scaled = (u * shrink_ref[...]).astype(BF16)

    def chunked(value):
        return value.reshape(chunks, CHUNK, slab)

    def summed(value):
        value = value.reshape(count, slab).astype(BF16)
        return jnp.concatenate(
            [
                jnp.dot(lower_ref[...], value[k : k + block], preferred_element_type=F32)
                for k in range(0, count, block)
            ]
        )

    def first_pass(j, _):
        at = pl.ds(pl.multiple_of(j * slab, slab), slab)
        at_im = pl.ds(pl.multiple_of(states + j * slab, slab), slab)
        d_re = chunked(jnp.dot(scaled, in_ref[:, at], preferred_element_type=F32))
        d_im = chunked(jnp.dot(scaled, in_ref[:, at_im], preferred_element_type=F32))
        i_re, i_im = inv_re_ref[:, at][None], inv_im_ref[:, at][None]
        cum_re = summed(i_re * d_re - i_im * d_im)
        cum_im = summed(i_re * d_im + i_im * d_re)
        cum_re_ref[:, at] = cum_re
        cum_im_ref[:, at] = cum_im
        end_re_ref[:, at] = chunked(cum_re)[:, CHUNK - 1]
        end_im_ref[:, at] = chunked(cum_im)[:, CHUNK - 1]
        return 0

    lax.fori_loop(0, states // slab, first_pass, 0)

    h_re, h_im = hop_re_ref[0], hop_im_ref[0]
    t_re, t_im = end_re_ref[...], end_im_ref[...]
    s_re = h_re * t_re - h_im * t_im
    s_im = h_re * t_im + h_im * t_re
    for level in range(1, hop_re_ref.shape[0]):
        h_re, h_im = hop_re_ref[level], hop_im_ref[level]
        p_re, p_im = pltpu.roll(s_re, 1 << (level - 1), 0), pltpu.roll(s_im, 1 << (level - 1), 0)
        s_re, s_im = s_re + h_re * p_re - h_im * p_im, s_im + h_re * p_im + h_im * p_re
    lanes = last_ref.shape[1]
    for k in range(states // lanes):
        last_ref[k : k + 1, :] = s_re[chunks - 1 :, k * lanes : (k + 1) * lanes]
        row = states // lanes + k
        last_ref[row : row + 1, :] = s_im[chunks - 1 :, k * lanes : (k + 1) * lanes]
    begins = lax.broadcasted_iota(jnp.int32, s_re.shape, 0) > 0
    end_re_ref[...] = jnp.where(begins, pltpu.roll(s_re, 1, 0), 0.0)
    end_im_ref[...] = jnp.where(begins, pltpu.roll(s_im, 1, 0), 0.0)
    y_ref[...] = jnp.zeros(y_ref.shape, F32)

    def second_pass(j, _):
        at = pl.ds(pl.multiple_of(j * slab, slab), slab)
        at_im = pl.ds(pl.multiple_of(states + j * slab, slab), slab)
        t_re = chunked(cum_re_ref[:, at]) + end_re_ref[:, at][:, None]
        t_im = chunked(cum_im_ref[:, at]) + end_im_ref[:, at][:, None]
        f_re, f_im = fwd_re_ref[:, at][None], fwd_im_ref[:, at][None]
        x_re = (f_re * t_re - f_im * t_im).reshape(count, slab).astype(BF16)
        x_im = (f_re * t_im + f_im * t_re).reshape(count, slab).astype(BF16)
        y_ref[...] += dot_rows(x_re, out_mat_ref[:, at]) + dot_rows(x_im, out_mat_ref[:, at_im])
        return 0

    lax.fori_loop(0, states // slab, second_pass, 0)
    y_ref[...] = y_ref[...] * grow_ref[...] + skip_ref[...] * u


def merge_kernel(
    place_ref,
    y_ref,
    power_ref,
    h_re_ref,
    h_im_ref,
    read_ref,
    conv_ref,
    own_ref,
    other_ref,
    out_ref,
    weight_ref,
):
    natural_order(place_ref, own_ref, other_ref, weight_ref, 0, from_own_x=True)
    lanes = h_re_ref.shape[1]
    h_re, h_im = h_re_ref[...], h_im_ref[...]
    c_re, c_im = read_ref[:, :lanes].astype(F32), read_ref[:, lanes:].astype(F32)
    total = (
        y_ref[...]
        + dot_rows(power_ref[:, :lanes], (c_re * h_re + c_im * h_im).astype(BF16))
        + dot_rows(power_ref[:, lanes:], (c_im * h_re - c_re * h_im).astype(BF16))
    )
    ssm = jax.nn.gelu(total).astype(BF16)
    both = jnp.concatenate([ssm, conv_ref[...]], axis=1)
    out_ref[...] = dot_rows(both, weight_ref[...]).astype(BF16)


def input_matrix(eigen_real, eigen_imag, step, state_input):
    base = eigen_real * step[:, None]
    theta = eigen_imag * step[:, None]
    magnitude = jnp.exp(base)
    near_re = magnitude * jnp.cos(theta) - 1.0
    near_im = magnitude * jnp.sin(theta)
    modulus = eigen_real * eigen_real + eigen_imag * eigen_imag
    ratio_re = (near_re * eigen_real + near_im * eigen_imag) / modulus
    ratio_im = (near_im * eigen_real - near_re * eigen_imag) / modulus
    in_re, in_im = state_input[0], state_input[1]
    return (
        ratio_re[:, None, :] * in_re - ratio_im[:, None, :] * in_im,
        ratio_re[:, None, :] * in_im + ratio_im[:, None, :] * in_re,
    )


def tables(eigen_real, eigen_imag, log_step, decay_shift, state_input, readout, width):
    groups, states = eigen_real.shape
    lanes = groups * states
    count = decay_shift.shape[1]
    chunks = count // CHUNK
    step = jnp.exp(log_step)
    base = (eigen_real * step[:, None]).reshape(1, lanes)
    theta = (eigen_imag * step[:, None]).reshape(1, lanes)
    inside = jnp.arange(1, CHUNK + 1, dtype=F32)[:, None]
    level, angle = inside * base, inside * theta
    cosine, sine = jnp.cos(angle), jnp.sin(angle)
    grow, shrink = jnp.exp(level), jnp.exp(-level)
    forward = (grow * cosine, grow * sine)
    inverse = (shrink * cosine, -shrink * sine)
    starts = jnp.arange(chunks).astype(F32)[:, None] * CHUNK * theta
    start_cos, start_sin = jnp.cos(starts), jnp.sin(starts)
    whole_turn = (start_cos[chunks // 2], start_sin[chunks // 2])
    b_re, b_im = input_matrix(eigen_real, eigen_imag, step, state_input)
    rows = (groups * state_input.shape[2], states)
    levels = 1 + (chunks - 1).bit_length()
    block = min(count, 256)
    at = jnp.arange(block)
    lower_block = (
        (at[:, None] >= at[None, :]) & (at[:, None] // CHUNK == at[None, :] // CHUNK)
    ).astype(BF16)
    outs = (
        pltpu.HBM((count, width), F32),
        pltpu.HBM((count, width), F32),
        pltpu.HBM((width, 2 * lanes), BF16),
        pltpu.HBM((width, 2 * lanes), BF16),
        pltpu.HBM((levels, chunks, lanes), F32),
        pltpu.HBM((levels, chunks, lanes), F32),
        pltpu.HBM((count, 2 * lanes), BF16),
        pltpu.HBM((lanes // 128, 128), F32),
    )
    grow, shrink, into, out, hop_re, hop_im, power, total = call(
        table_kernel,
        outs,
        (
            decay_shift,
            base,
            cosine,
            sine,
            start_cos,
            start_sin,
            b_re.reshape(rows),
            b_im.reshape(rows),
            readout[0].reshape(rows),
            readout[1].reshape(rows),
        ),
        scratch=[pltpu.VMEM(o.shape, o.dtype) for o in outs] + [pltpu.SemaphoreType.DMA((len(outs),))],
        mib=24,
        space=pltpu.HBM,
        flops=20 * count * count * groups,
        bytes_accessed=8 * count * lanes,
        transcendentals=count * lanes,
    )
    device = dict(
        base=base.reshape(-1, 128),
        turn=squared(*(r.reshape(-1, 128) for r in whole_turn)),
        shift=total,
    )
    scan = (grow, shrink, into, out, *forward, *inverse, hop_re, hop_im, lower_block)
    return scan, power, out, device


def pulled(packed, rows):
    return packed[:rows], packed[rows : 2 * rows], packed[2 * rows :]


def carry_in(last, device, count, h):
    rows = device["base"].shape[0]
    base, turn = device["base"], device["turn"]
    plane = ("x", "c")
    packed = jnp.concatenate([last, device["shift"]])
    near = copies(packed, plane)
    peers, place = lax.axis_size(plane), lax.axis_index(plane)
    zero = jnp.zeros_like(base)
    run = (zero, zero)
    before, shift_before = run, zero
    shift_run = zero
    for k in range(peers):
        re, im, shift = pulled(near[k], rows)
        size = jnp.exp(count * base + shift)
        moved = times((size * turn[0], size * turn[1]), run)
        run = (moved[0] + re, moved[1] + im)
        shift_run = shift_run + shift
        passed = k < place
        before = jax.tree.map(lambda new, old: jnp.where(passed, new, old), run, before)
        shift_before = jnp.where(passed, shift_run, shift_before)
    far = copies(jnp.concatenate([*run, shift_run]), "z")
    plane_turn, at = turn, 1
    while at < peers:
        plane_turn, at = squared(*plane_turn), at * 2
    for k in range(lax.axis_size("z")):
        re, im, shift = pulled(far[k], rows)
        size = jnp.exp(peers * count * base + shift)
        moved = times((size * plane_turn[0], size * plane_turn[1]), h)
        passed = k < lax.axis_index("z")
        h = tuple(jnp.where(passed, m + s, o) for m, s, o in zip(moved, (re, im), h))
    turns = (jnp.ones_like(base), zero)
    for k in range(peers):
        passed = k < place
        turns = tuple(jnp.where(passed, new, old) for new, old in zip(times(turns, turn), turns))
    size = jnp.exp(place * count * base + shift_before)
    moved = times((size * turns[0], size * turns[1]), h)
    return moved[0] + before[0], moved[1] + before[1]


def conv_finish(raw, sums, channel_gain):
    others = [from_ahead(sums, "tp", d) for d in range(1, lax.axis_size("tp"))]
    first, second = (row[:, None] for row in sum(others, sums))
    middle = first / CONV_W
    spread = second / CONV_W - middle * middle
    scaled = (raw - middle) * lax.rsqrt(spread + EPS) * channel_gain
    return jax.nn.silu(scaled).astype(BF16)


def mixer(
    tokens,
    norm_gain,
    proj_state,
    proj_value,
    proj_gate,
    eigen_real,
    eigen_imag,
    log_step,
    decay_shift,
    state_input,
    readout,
    skip_gain,
    init_state,
    conv_taps,
    channel_gain,
    merge_state,
    merge_conv,
):
    place = jnp.stack([lax.axis_index("c"), lax.axis_index("x"), lax.axis_index("tp")]).astype(jnp.int32)
    parts = lax.axis_size("tp")
    count, depth_part = tokens.shape
    depth = depth_part * parts
    rows = count + HALO
    half = rows // 2
    width = proj_state.shape[1]
    merged = jnp.concatenate([merge_state, merge_conv]).T
    planes = copies(
        jnp.concatenate([proj_state, proj_value, proj_gate, merged], axis=1), "z"
    )
    extended = jnp.concatenate([next_along(tokens[count - HALO :], SP), tokens])
    ahead = from_ahead(extended, "tp", 1)
    behind = from_ahead(extended, "tp", -1)
    top = from_ahead(ahead[:half], "tp", 1)
    bottom = from_ahead(behind[half:], "tp", -1)
    scan_tables, power, reads, device = tables(
        eigen_real, eigen_imag, log_step, decay_shift, state_input, readout, width
    )
    start = tuple(s.reshape(-1, 128) for s in (init_state[0], init_state[1]))
    planes, total, start = lax.optimization_barrier((planes, device["shift"], start))
    device["shift"] = total
    project_x = copies(planes[:, :, : 3 * width], "x")
    merge_x = from_own_on(planes[:, :, 3 * width :], "x")
    project_other = partner(project_x)
    merge_other = partner(merge_x)

    normed = call(
        norm_kernel,
        jax.ShapeDtypeStruct((parts, rows, depth_part), BF16),
        (*far_from_core(extended, ahead, top, bottom, behind), norm_gain.reshape(parts, 1, depth_part)),
        scalars=(place,),
        mib=12,
        flops=8 * count * depth,
        bytes_accessed=4 * count * depth,
        transcendentals=count,
    )
    u_in = call(
        state_in_kernel,
        jax.ShapeDtypeStruct((count, width), BF16),
        (normed, project_x, project_other),
        scalars=(place,),
        scratch=(pltpu.VMEM((depth, width), BF16),),
        mib=12,
        flops=2 * count * depth * width,
        bytes_accessed=4 * depth * count,
        transcendentals=0,
    )
    lanes = eigen_real.size
    chunks = count // CHUNK
    y_local, last = call(
        scan_kernel,
        (
            pltpu.HBM((count, width), F32),
            jax.ShapeDtypeStruct((2 * lanes // 128, 128), F32),
        ),
        (u_in, *scan_tables, skip_gain.reshape(1, -1)),
        scratch=(
            pltpu.VMEM((count, lanes), F32),
            pltpu.VMEM((count, lanes), F32),
            pltpu.VMEM((chunks, lanes), F32),
            pltpu.VMEM((chunks, lanes), F32),
        ),
        mib=24,
        flops=12 * count * width * lanes,
        bytes_accessed=8 * count * lanes,
        transcendentals=0,
    )
    h_re, h_im = carry_in(last, device, count, start)

    raw, sums = call(
        conv_kernel,
        (
            pltpu.HBM((count, width), F32),
            jax.ShapeDtypeStruct((2, count), F32),
        ),
        (normed, project_x, project_other, conv_taps),
        scalars=(place,),
        scratch=(
            pltpu.VMEM((depth, 2 * width), BF16),
            pltpu.VMEM((rows + 8, width), F32),
            pltpu.VMEM((8, rows, width), F32),
        ),
        mib=20,
        flops=4 * count * depth * width,
        bytes_accessed=4 * depth * count,
        transcendentals=0,
    )
    conv_out = conv_finish(raw, sums, channel_gain)

    product = call(
        merge_kernel,
        jax.ShapeDtypeStruct((count, depth), BF16),
        (
            y_local,
            power,
            h_re.reshape(1, -1),
            h_im.reshape(1, -1),
            reads,
            conv_out,
            merge_x,
            merge_other,
        ),
        scalars=(place,),
        scratch=(pltpu.VMEM((depth, 2 * width), BF16),),
        flops=4 * count * depth * width,
        bytes_accessed=4 * depth * count,
        transcendentals=0,
    )
    arrived = lax.all_to_all(
        product.reshape(parts, count // parts, depth), "tp", split_axis=0, concat_axis=0, tiled=True
    )
    return arrived.astype(F32).sum(axis=0).astype(BF16)


def finer_mesh(mesh):
    cores = 2
    return Mesh(mesh.devices.reshape(16, 4, cores, mesh.shape["tp"]), SP_TP)


def solution(mesh):
    return jax.shard_map(
        mixer,
        mesh=finer_mesh(mesh),
        in_specs=(
            P(SP, "tp"),
            P(),
            P(SP, "tp"),
            P(SP, "tp"),
            P(SP, "tp"),
            P("tp", None),
            P("tp", None),
            P("tp"),
            P("tp", SP),
            P(None, "tp", None, None),
            P(None, "tp", None, None),
            P("tp"),
            P(None, "tp", None),
            P(None, "tp"),
            P("tp"),
            P("tp", SP),
            P("tp", SP),
        ),
        out_specs=P(SP_TP, None),
        check_vma=False,
    )
```

```python
import functools

import jax
import jax.numpy as jnp
from jax import lax
from jax.experimental import pallas as pl
from jax.experimental.pallas import tpu as pltpu
from jax.sharding import Mesh
from jax.sharding import PartitionSpec as P


CONV_W = 1024
SP = ("z", "x", "c")
SP_TP = ("z", "x", "c", "tp")
CHUNK = 32
HALO = 32
EPS = 1e-06
EXACT = lax.Precision.HIGHEST
F32 = jnp.float32
BF16 = jnp.bfloat16


def copies(value, axis):
    peers = lax.axis_size(axis)
    return lax.all_to_all(
        jnp.broadcast_to(value[None], (peers, *value.shape)), axis, 0, 0, tiled=True
    )


def next_along(block, axis):
    count = lax.axis_size(axis)
    return lax.ppermute(block, axis, [(i, i + 1) for i in range(count - 1)])


def partner(block):
    return lax.ppermute(block, "c", [(0, 1), (1, 0)])


def from_ahead(block, axis, distance):
    count = lax.axis_size(axis)
    return lax.ppermute(block, axis, [(i, (i - distance) % count) for i in range(count)])


def from_own_on(planes, axis):
    peers = lax.axis_size(axis)
    return jnp.stack([planes] + [from_ahead(planes, axis, d) for d in range(1, peers)])


def far_from_core(*arrays):
    return [pltpu.with_memory_space_constraint(array, pltpu.HBM) for array in arrays]


def whole_specs(arrays):
    return [pl.BlockSpec(memory_space=pltpu.VMEM) for _ in arrays]


def call(body, outs, arrays, scalars=(), scratch=(), mib=16, space=pltpu.VMEM, **costs):
    return pl.pallas_call(
        body,
        compiler_params=pltpu.CompilerParams(vmem_limit_bytes=mib * 2**20),
        out_shape=outs,
        in_specs=[pl.BlockSpec(memory_space=pltpu.SMEM) for _ in scalars] + whole_specs(arrays),
        out_specs=jax.tree.map(lambda _: pl.BlockSpec(memory_space=space), outs),
        scratch_shapes=list(scratch),
        cost_estimate=pl.CostEstimate(**costs) if costs else None,
    )(*scalars, *arrays)


def natural_order(place_ref, own_ref, other_ref, into_ref, turned, first_lane=0, from_own_x=False):
    peers_x, _, rows, _ = own_ref.shape
    blocks = into_ref.shape[0] // rows
    lanes = slice(first_lane, first_lane + into_ref.shape[1])
    core, part = place_ref[0], place_ref[2]
    place_x = place_ref[1] if from_own_x else 0
    first = part * turned

    def place(by_core):
        for k in range(blocks):
            at = lax.rem(first + k, blocks)
            x = lax.rem(lax.div(at, 2) - place_x + 2 * peers_x, peers_x)
            into_ref[k * rows : (k + 1) * rows, :] = by_core[k % 2][
                x, lax.div(at, 2 * peers_x), :, lanes
            ]

    @pl.when(core == 0)
    def _():
        place((own_ref, other_ref))

    @pl.when(core == 1)
    def _():
        place((other_ref, own_ref))


def dot_rows(a, b):
    return lax.dot_general(a, b, (((1,), (1,)), ((), ())), preferred_element_type=F32)


def norm_kernel(place_ref, own_ref, ahead_ref, top_ref, bottom_ref, behind_ref, gain_ref, out_ref):
    parts, count, depth = out_ref.shape
    half = count // 2
    part = place_ref[2]

    def rows_of(at, opposite_ref):
        rows = pl.ds(at, half)
        blocks = [
            block.astype(F32)
            for block in (own_ref[rows], ahead_ref[rows], opposite_ref[...], behind_ref[rows])
        ]
        power = sum(jnp.sum(block * block, axis=1, keepdims=True) for block in blocks)
        scale = lax.rsqrt(power / (parts * depth) + EPS)
        for p, block in enumerate(blocks):
            gain = gain_ref[lax.rem(part + p, parts)]
            out_ref[p, rows] = (block * scale * gain).astype(BF16)

    rows_of(0, top_ref)
    rows_of(half, bottom_ref)


def projected(normed_ref, weight_ref, rows):
    parts, _, depth = normed_ref.shape
    return sum(
        jnp.dot(
            normed_ref[p, rows],
            weight_ref[p * depth : (p + 1) * depth],
            preferred_element_type=F32,
        )
        for p in range(parts)
    )


def state_in_kernel(place_ref, normed_ref, own_ref, other_ref, out_ref, weight_ref):
    parts, rows, _ = normed_ref.shape
    turned = weight_ref.shape[0] // own_ref.shape[2] // parts
    natural_order(place_ref, own_ref, other_ref, weight_ref, turned)
    out_ref[...] = projected(normed_ref, weight_ref, slice(HALO, rows)).astype(BF16)


def conv_kernel(
    place_ref, normed_ref, own_ref, other_ref, taps_ref, raw_ref, sums_ref, weight_ref, glu_ref, shifted_ref
):
    parts, rows, _ = normed_ref.shape
    count, width = raw_ref.shape
    turned = weight_ref.shape[0] // own_ref.shape[2] // parts
    natural_order(place_ref, own_ref, other_ref, weight_ref, turned, first_lane=width)
    both = projected(normed_ref, weight_ref, slice(0, rows))
    value = both[:, :width].astype(BF16).astype(F32)
    gate = both[:, width:].astype(BF16).astype(F32)
    glu_ref[:rows] = (value * jax.nn.sigmoid(gate)).astype(BF16).astype(F32)
    glu_ref[rows:] = jnp.zeros((glu_ref.shape[0] - rows, width), F32)
    taps = taps_ref.shape[0]
    sublanes = 8
    for k in range(sublanes):
        shifted_ref[k] = glu_ref[k : k + rows]
    first = HALO - (taps - 1)
    step = 64

    def some_rows(n, _):
        at = pl.multiple_of(n * step, step)
        total = jnp.zeros((step, width), F32)
        for k in range(taps):
            shift, whole = (first + k) % sublanes, (first + k) // sublanes * sublanes
            total = total + taps_ref[k : k + 1] * shifted_ref[shift, pl.ds(at + whole, step)]
        raw_ref[pl.ds(at, step)] = total
        return 0

    lax.fori_loop(0, count // step, some_rows, 0)
    raw = raw_ref[...]
    ones = jnp.ones((8, width), F32)

    def across(value):
        return lax.dot_general(
            ones, value, (((1,), (1,)), ((), ())), precision=EXACT, preferred_element_type=F32
        )[:1]

    sums_ref[0:1] = across(raw)
    sums_ref[1:2] = across(raw * raw)


def squared(re, im):
    return re * re - im * im, 2.0 * re * im


def times(a, b):
    return a[0] * b[0] - a[1] * b[1], a[0] * b[1] + a[1] * b[0]


def exact_dot(a, b):
    return jnp.dot(a, b, preferred_element_type=F32, precision=EXACT)


def spread_over(groups, each):
    row = lax.broadcasted_iota(jnp.int32, (groups, groups * each), 0)
    col = lax.broadcasted_iota(jnp.int32, (groups, groups * each), 1) // each
    return (row == col).astype(F32)


def write_diagonal(out_ref, at, blocks, groups):
    rows, cols = blocks.shape
    pair = jnp.concatenate([blocks, blocks], axis=1)
    row_group = lax.broadcasted_iota(jnp.int32, pair.shape, 0) // (rows // groups)
    col_group = lax.broadcasted_iota(jnp.int32, pair.shape, 1) // cols
    for k in range(groups // 2):
        mine = row_group == col_group + 2 * k
        out_ref[:, at + 2 * k * cols : at + 2 * (k + 1) * cols] = jnp.where(mine, pair, 0.0).astype(BF16)


def table_kernel(*refs):
    inputs, hbm, vmem, done = refs[:10], refs[10:18], refs[18:26], refs[26]

    def send(*which):
        for k in which:
            pltpu.make_async_copy(vmem[k], hbm[k], done.at[k]).start()

    fill_tables(send, *inputs, *vmem)
    for k in range(len(vmem)):
        pltpu.make_async_copy(vmem[k], hbm[k], done.at[k]).wait()


def fill_tables(
    send,
    shift_ref,
    base_ref,
    cos_ref,
    sin_ref,
    start_cos_ref,
    start_sin_ref,
    b_re_ref,
    b_im_ref,
    c_re_ref,
    c_im_ref,
    grow_ref,
    shrink_ref,
    into_ref,
    out_ref,
    hop_re_ref,
    hop_im_ref,
    power_ref,
    total_ref,
):
    groups, count = shift_ref.shape
    lanes = base_ref.shape[1]
    width = grow_ref.shape[1]
    chunks = count // CHUNK
    base = base_ref[...]
    row = lax.broadcasted_iota(jnp.int32, (count, count), 0)
    col = lax.broadcasted_iota(jnp.int32, (count, count), 1)
    earlier = row >= col
    inside = earlier & (row // CHUNK == col // CHUNK)

    def run(which):
        return lax.dot_general(
            which.astype(F32),
            shift_ref[...],
            (((1,), (1,)), ((), ())),
            precision=EXACT,
            preferred_element_type=F32,
        )

    partial, whole = run(inside), run(earlier)
    narrow = exact_dot(partial, spread_over(groups, width // groups))
    grow_ref[...] = jnp.exp(narrow)
    shrink_ref[...] = jnp.exp(-narrow)
    spread = spread_over(groups, lanes // groups)
    wide = exact_dot(whole, spread)
    wide_last = wide[count - 1 :]
    send(0, 1)
    for k in range(lanes // 128):
        total_ref[k : k + 1, :] = wide_last[:, k * 128 : (k + 1) * 128]
    sums = jnp.concatenate([partial[(c + 1) * CHUNK - 1 : (c + 1) * CHUNK] for c in range(chunks)])
    near = exact_dot(sums, spread)
    index = lax.broadcasted_iota(jnp.int32, (chunks, lanes), 0)
    size = jnp.exp(CHUNK * base + near)
    turn = (start_cos_ref[1:2], start_sin_ref[1:2])
    hop_re_ref[0], hop_im_ref[0] = size * turn[0], size * turn[1]
    distance, level = 1, 1
    while distance < chunks:
        size = jnp.where(index >= distance, jnp.exp(distance * CHUNK * base + near), 0.0)
        turn = (start_cos_ref[distance : distance + 1], start_sin_ref[distance : distance + 1])
        hop_re_ref[level], hop_im_ref[level] = size * turn[0], size * turn[1]
        near = near + jnp.where(index >= distance, pltpu.roll(near, distance, 0), 0.0)
        distance, level = distance * 2, level + 1
    send(4, 5, 7)
    counts = lax.broadcasted_iota(jnp.int32, (CHUNK, 1), 0).astype(F32)
    inner = (cos_ref[...], sin_ref[...])
    for c in range(chunks):
        at = slice(c * CHUNK, (c + 1) * CHUNK)
        size = jnp.exp((counts + (c * CHUNK + 1)) * base + wide[at])
        turn = times((start_cos_ref[c : c + 1], start_sin_ref[c : c + 1]), inner)
        power_ref[at, :lanes] = (size * turn[0]).astype(BF16)
        power_ref[at, lanes:] = (size * turn[1]).astype(BF16)
    send(6)
    write_diagonal(into_ref, 0, b_re_ref[...], groups)
    write_diagonal(into_ref, lanes, b_im_ref[...], groups)
    send(2)
    write_diagonal(out_ref, 0, c_re_ref[...], groups)
    write_diagonal(out_ref, lanes, -c_im_ref[...], groups)
    send(3)


def scan_kernel(
    u_ref,
    grow_ref,
    shrink_ref,
    in_ref,
    out_mat_ref,
    fwd_re_ref,
    fwd_im_ref,
    inv_re_ref,
    inv_im_ref,
    hop_re_ref,
    hop_im_ref,
    lower_ref,
    skip_ref,
    y_ref,
    last_ref,
    cum_re_ref,
    cum_im_ref,
    end_re_ref,
    end_im_ref,
):
    count, _ = u_ref.shape
    states = fwd_re_ref.shape[1]
    chunks = count // CHUNK
    block = lower_ref.shape[0]
    slab = 256
    u = u_ref[...].astype(F32)
    scaled = (u * shrink_ref[...]).astype(BF16)

    def chunked(value):
        return value.reshape(chunks, CHUNK, slab)

    def summed(value):
        value = value.reshape(count, slab).astype(BF16)
        return jnp.concatenate(
            [
                jnp.dot(lower_ref[...], value[k : k + block], preferred_element_type=F32)
                for k in range(0, count, block)
            ]
        )

    def first_pass(j, _):
        at = pl.ds(pl.multiple_of(j * slab, slab), slab)
        at_im = pl.ds(pl.multiple_of(states + j * slab, slab), slab)
        d_re = chunked(jnp.dot(scaled, in_ref[:, at], preferred_element_type=F32))
        d_im = chunked(jnp.dot(scaled, in_ref[:, at_im], preferred_element_type=F32))
        i_re, i_im = inv_re_ref[:, at][None], inv_im_ref[:, at][None]
        cum_re = summed(i_re * d_re - i_im * d_im)
        cum_im = summed(i_re * d_im + i_im * d_re)
        cum_re_ref[:, at] = cum_re
        cum_im_ref[:, at] = cum_im
        end_re_ref[:, at] = chunked(cum_re)[:, CHUNK - 1]
        end_im_ref[:, at] = chunked(cum_im)[:, CHUNK - 1]
        return 0

    lax.fori_loop(0, states // slab, first_pass, 0)

    h_re, h_im = hop_re_ref[0], hop_im_ref[0]
    t_re, t_im = end_re_ref[...], end_im_ref[...]
    s_re = h_re * t_re - h_im * t_im
    s_im = h_re * t_im + h_im * t_re
    for level in range(1, hop_re_ref.shape[0]):
        h_re, h_im = hop_re_ref[level], hop_im_ref[level]
        p_re, p_im = pltpu.roll(s_re, 1 << (level - 1), 0), pltpu.roll(s_im, 1 << (level - 1), 0)
        s_re, s_im = s_re + h_re * p_re - h_im * p_im, s_im + h_re * p_im + h_im * p_re
    lanes = last_ref.shape[1]
    for k in range(states // lanes):
        last_ref[k : k + 1, :] = s_re[chunks - 1 :, k * lanes : (k + 1) * lanes]
        row = states // lanes + k
        last_ref[row : row + 1, :] = s_im[chunks - 1 :, k * lanes : (k + 1) * lanes]
    begins = lax.broadcasted_iota(jnp.int32, s_re.shape, 0) > 0
    end_re_ref[...] = jnp.where(begins, pltpu.roll(s_re, 1, 0), 0.0)
    end_im_ref[...] = jnp.where(begins, pltpu.roll(s_im, 1, 0), 0.0)
    y_ref[...] = jnp.zeros(y_ref.shape, F32)

    def second_pass(j, _):
        at = pl.ds(pl.multiple_of(j * slab, slab), slab)
        at_im = pl.ds(pl.multiple_of(states + j * slab, slab), slab)
        t_re = chunked(cum_re_ref[:, at]) + end_re_ref[:, at][:, None]
        t_im = chunked(cum_im_ref[:, at]) + end_im_ref[:, at][:, None]
        f_re, f_im = fwd_re_ref[:, at][None], fwd_im_ref[:, at][None]
        x_re = (f_re * t_re - f_im * t_im).reshape(count, slab).astype(BF16)
        x_im = (f_re * t_im + f_im * t_re).reshape(count, slab).astype(BF16)
        y_ref[...] += dot_rows(x_re, out_mat_ref[:, at]) + dot_rows(x_im, out_mat_ref[:, at_im])
        return 0

    lax.fori_loop(0, states // slab, second_pass, 0)
    y_ref[...] = y_ref[...] * grow_ref[...] + skip_ref[...] * u


def merge_kernel(
    distances,
    place_ref,
    y_ref,
    power_ref,
    h_re_ref,
    h_im_ref,
    read_ref,
    conv_ref,
    own_ref,
    other_ref,
    out_ref,
    weight_ref,
):
    natural_order(place_ref, own_ref, other_ref, weight_ref, 0, from_own_x=True)
    lanes = h_re_ref.shape[1]
    block = out_ref.shape[1]
    parts = y_ref.shape[0] // block
    h_re, h_im = h_re_ref[...], h_im_ref[...]
    c_re, c_im = read_ref[:, :lanes].astype(F32), read_ref[:, lanes:].astype(F32)
    blend_re = (c_re * h_re + c_im * h_im).astype(BF16)
    blend_im = (c_im * h_re - c_re * h_im).astype(BF16)
    for k, distance in enumerate(distances):
        rows = pl.ds(pl.multiple_of(lax.rem(place_ref[2] + distance, parts) * block, block), block)
        total = (
            y_ref[rows]
            + dot_rows(power_ref[rows, :lanes], blend_re)
            + dot_rows(power_ref[rows, lanes:], blend_im)
        )
        ssm = jax.nn.gelu(total).astype(BF16)
        both = jnp.concatenate([ssm, conv_ref[rows]], axis=1)
        out_ref[k] = dot_rows(both, weight_ref[...]).astype(BF16)


def input_matrix(eigen_real, eigen_imag, step, state_input):
    base = eigen_real * step[:, None]
    theta = eigen_imag * step[:, None]
    magnitude = jnp.exp(base)
    near_re = magnitude * jnp.cos(theta) - 1.0
    near_im = magnitude * jnp.sin(theta)
    modulus = eigen_real * eigen_real + eigen_imag * eigen_imag
    ratio_re = (near_re * eigen_real + near_im * eigen_imag) / modulus
    ratio_im = (near_im * eigen_real - near_re * eigen_imag) / modulus
    in_re, in_im = state_input[0], state_input[1]
    return (
        ratio_re[:, None, :] * in_re - ratio_im[:, None, :] * in_im,
        ratio_re[:, None, :] * in_im + ratio_im[:, None, :] * in_re,
    )


def tables(eigen_real, eigen_imag, log_step, decay_shift, state_input, readout, width):
    groups, states = eigen_real.shape
    lanes = groups * states
    count = decay_shift.shape[1]
    chunks = count // CHUNK
    step = jnp.exp(log_step)
    base = (eigen_real * step[:, None]).reshape(1, lanes)
    theta = (eigen_imag * step[:, None]).reshape(1, lanes)
    inside = jnp.arange(1, CHUNK + 1, dtype=F32)[:, None]
    level, angle = inside * base, inside * theta
    cosine, sine = jnp.cos(angle), jnp.sin(angle)
    grow, shrink = jnp.exp(level), jnp.exp(-level)
    forward = (grow * cosine, grow * sine)
    inverse = (shrink * cosine, -shrink * sine)
    starts = jnp.arange(chunks).astype(F32)[:, None] * CHUNK * theta
    start_cos, start_sin = jnp.cos(starts), jnp.sin(starts)
    whole_turn = (start_cos[chunks // 2], start_sin[chunks // 2])
    b_re, b_im = input_matrix(eigen_real, eigen_imag, step, state_input)
    rows = (groups * state_input.shape[2], states)
    levels = 1 + (chunks - 1).bit_length()
    block = min(count, 256)
    at = jnp.arange(block)
    lower_block = (
        (at[:, None] >= at[None, :]) & (at[:, None] // CHUNK == at[None, :] // CHUNK)
    ).astype(BF16)
    outs = (
        pltpu.HBM((count, width), F32),
        pltpu.HBM((count, width), F32),
        pltpu.HBM((width, 2 * lanes), BF16),
        pltpu.HBM((width, 2 * lanes), BF16),
        pltpu.HBM((levels, chunks, lanes), F32),
        pltpu.HBM((levels, chunks, lanes), F32),
        pltpu.HBM((count, 2 * lanes), BF16),
        pltpu.HBM((lanes // 128, 128), F32),
    )
    grow, shrink, into, out, hop_re, hop_im, power, total = call(
        table_kernel,
        outs,
        (
            decay_shift,
            base,
            cosine,
            sine,
            start_cos,
            start_sin,
            b_re.reshape(rows),
            b_im.reshape(rows),
            readout[0].reshape(rows),
            readout[1].reshape(rows),
        ),
        scratch=[pltpu.VMEM(o.shape, o.dtype) for o in outs] + [pltpu.SemaphoreType.DMA((len(outs),))],
        mib=24,
        space=pltpu.HBM,
        flops=20 * count * count * groups,
        bytes_accessed=8 * count * lanes,
        transcendentals=count * lanes,
    )
    device = dict(
        base=base.reshape(-1, 128),
        turn=squared(*(r.reshape(-1, 128) for r in whole_turn)),
        shift=total,
    )
    scan = (grow, shrink, into, out, *forward, *inverse, hop_re, hop_im, lower_block)
    return scan, power, out, device


def pulled(packed, rows):
    return packed[:rows], packed[rows : 2 * rows], packed[2 * rows :]


def carry_in(last, device, count, h):
    rows = device["base"].shape[0]
    base, turn = device["base"], device["turn"]
    plane = ("x", "c")
    packed = jnp.concatenate([last, device["shift"]])
    near = copies(packed, plane)
    peers, place = lax.axis_size(plane), lax.axis_index(plane)
    zero = jnp.zeros_like(base)
    run = (zero, zero)
    before, shift_before = run, zero
    shift_run = zero
    for k in range(peers):
        re, im, shift = pulled(near[k], rows)
        size = jnp.exp(count * base + shift)
        moved = times((size * turn[0], size * turn[1]), run)
        run = (moved[0] + re, moved[1] + im)
        shift_run = shift_run + shift
        passed = k < place
        before = jax.tree.map(lambda new, old: jnp.where(passed, new, old), run, before)
        shift_before = jnp.where(passed, shift_run, shift_before)
    far = copies(jnp.concatenate([*run, shift_run]), "z")
    plane_turn, at = turn, 1
    while at < peers:
        plane_turn, at = squared(*plane_turn), at * 2
    for k in range(lax.axis_size("z")):
        re, im, shift = pulled(far[k], rows)
        size = jnp.exp(peers * count * base + shift)
        moved = times((size * plane_turn[0], size * plane_turn[1]), h)
        passed = k < lax.axis_index("z")
        h = tuple(jnp.where(passed, m + s, o) for m, s, o in zip(moved, (re, im), h))
    turns = (jnp.ones_like(base), zero)
    for k in range(peers):
        passed = k < place
        turns = tuple(jnp.where(passed, new, old) for new, old in zip(times(turns, turn), turns))
    size = jnp.exp(place * count * base + shift_before)
    moved = times((size * turns[0], size * turns[1]), h)
    return moved[0] + before[0], moved[1] + before[1]


def conv_finish(raw, sums, channel_gain):
    others = [from_ahead(sums, "tp", d) for d in range(1, lax.axis_size("tp"))]
    first, second = (row[:, None] for row in sum(others, sums))
    middle = first / CONV_W
    spread = second / CONV_W - middle * middle
    scaled = (raw - middle) * lax.rsqrt(spread + EPS) * channel_gain
    return jax.nn.silu(scaled).astype(BF16)


def mixer(
    tokens,
    norm_gain,
    proj_state,
    proj_value,
    proj_gate,
    eigen_real,
    eigen_imag,
    log_step,
    decay_shift,
    state_input,
    readout,
    skip_gain,
    init_state,
    conv_taps,
    channel_gain,
    merge_state,
    merge_conv,
):
    place = jnp.stack([lax.axis_index("c"), lax.axis_index("x"), lax.axis_index("tp")]).astype(jnp.int32)
    parts = lax.axis_size("tp")
    count, depth_part = tokens.shape
    depth = depth_part * parts
    rows = count + HALO
    half = rows // 2
    width = proj_state.shape[1]
    merged = jnp.concatenate([merge_state, merge_conv]).T
    planes = copies(
        jnp.concatenate([proj_state, proj_value, proj_gate, merged], axis=1), "z"
    )
    extended = jnp.concatenate([next_along(tokens[count - HALO :], SP), tokens])
    ahead = from_ahead(extended, "tp", 1)
    behind = from_ahead(extended, "tp", -1)
    top = from_ahead(ahead[:half], "tp", 1)
    bottom = from_ahead(behind[half:], "tp", -1)
    scan_tables, power, reads, device = tables(
        eigen_real, eigen_imag, log_step, decay_shift, state_input, readout, width
    )
    start = tuple(s.reshape(-1, 128) for s in (init_state[0], init_state[1]))
    planes, total, start = lax.optimization_barrier((planes, device["shift"], start))
    device["shift"] = total
    project_x = copies(planes[:, :, : 3 * width], "x")
    merge_x = from_own_on(planes[:, :, 3 * width :], "x")
    project_other = partner(project_x)
    merge_other = partner(merge_x)

    normed = call(
        norm_kernel,
        jax.ShapeDtypeStruct((parts, rows, depth_part), BF16),
        (*far_from_core(extended, ahead, top, bottom, behind), norm_gain.reshape(parts, 1, depth_part)),
        scalars=(place,),
        mib=12,
        flops=8 * count * depth,
        bytes_accessed=4 * count * depth,
        transcendentals=count,
    )
    u_in = call(
        state_in_kernel,
        jax.ShapeDtypeStruct((count, width), BF16),
        (normed, project_x, project_other),
        scalars=(place,),
        scratch=(pltpu.VMEM((depth, width), BF16),),
        mib=12,
        flops=2 * count * depth * width,
        bytes_accessed=4 * depth * count,
        transcendentals=0,
    )
    lanes = eigen_real.size
    chunks = count // CHUNK
    y_local, last = call(
        scan_kernel,
        (
            pltpu.HBM((count, width), F32),
            jax.ShapeDtypeStruct((2 * lanes // 128, 128), F32),
        ),
        (u_in, *scan_tables, skip_gain.reshape(1, -1)),
        scratch=(
            pltpu.VMEM((count, lanes), F32),
            pltpu.VMEM((count, lanes), F32),
            pltpu.VMEM((chunks, lanes), F32),
            pltpu.VMEM((chunks, lanes), F32),
        ),
        mib=24,
        flops=12 * count * width * lanes,
        bytes_accessed=8 * count * lanes,
        transcendentals=0,
    )
    h_re, h_im = carry_in(last, device, count, start)

    raw, sums = call(
        conv_kernel,
        (
            pltpu.HBM((count, width), F32),
            jax.ShapeDtypeStruct((2, count), F32),
        ),
        (normed, project_x, project_other, conv_taps),
        scalars=(place,),
        scratch=(
            pltpu.VMEM((depth, 2 * width), BF16),
            pltpu.VMEM((rows + 8, width), F32),
            pltpu.VMEM((8, rows, width), F32),
        ),
        mib=20,
        flops=4 * count * depth * width,
        bytes_accessed=4 * depth * count,
        transcendentals=0,
    )
    conv_out = conv_finish(raw, sums, channel_gain)

    block = count // parts
    merge_inputs = (
        y_local,
        power,
        h_re.reshape(1, -1),
        h_im.reshape(1, -1),
        reads,
        conv_out,
        merge_x,
        merge_other,
    )

    def products(*distances):
        return call(
            functools.partial(merge_kernel, distances),
            jax.ShapeDtypeStruct((len(distances), block, depth), BF16),
            merge_inputs,
            scalars=(place,),
            scratch=(pltpu.VMEM((depth, 2 * width), BF16),),
            flops=4 * block * len(distances) * depth * width,
            bytes_accessed=4 * depth * count,
            transcendentals=0,
        )

    opposite = products(2)[0]
    through_ahead = from_ahead(opposite[: block // 2], "tp", 1)
    through_behind = from_ahead(opposite[block // 2 :], "tp", -1)
    mine, to_ahead, to_behind = products(0, 1, 3)
    empty = jnp.zeros((block // 2, depth), F32)
    to_behind = to_behind.astype(F32) + jnp.concatenate([through_ahead.astype(F32), empty])
    to_ahead = to_ahead.astype(F32) + jnp.concatenate([empty, through_behind.astype(F32)])
    from_next = from_ahead(to_behind.astype(BF16), "tp", 1)
    from_last = from_ahead(to_ahead.astype(BF16), "tp", -1)
    return (mine.astype(F32) + from_next.astype(F32) + from_last.astype(F32)).astype(BF16)


def finer_mesh(mesh):
    cores = 2
    return Mesh(mesh.devices.reshape(16, 4, cores, mesh.shape["tp"]), SP_TP)


def solution(mesh):
    return jax.shard_map(
        mixer,
        mesh=finer_mesh(mesh),
        in_specs=(
            P(SP, "tp"),
            P(),
            P(SP, "tp"),
            P(SP, "tp"),
            P(SP, "tp"),
            P("tp", None),
            P("tp", None),
            P("tp"),
            P("tp", SP),
            P(None, "tp", None, None),
            P(None, "tp", None, None),
            P("tp"),
            P(None, "tp", None),
            P(None, "tp"),
            P("tp"),
            P("tp", SP),
            P("tp", SP),
        ),
        out_specs=P(SP_TP, None),
        check_vma=False,
    )
```

```python
import functools

import jax
import jax.numpy as jnp
from jax import lax
from jax.experimental import pallas as pl
from jax.experimental.pallas import tpu as pltpu
from jax.sharding import Mesh
from jax.sharding import PartitionSpec as P


CONV_W = 1024
SP = ("z", "x", "c")
SP_TP = ("z", "x", "c", "tp")
CHUNK = 32
HALO = 32
EPS = 1e-06
EXACT = lax.Precision.HIGHEST
F32 = jnp.float32
BF16 = jnp.bfloat16


def copies(value, axis):
    peers = lax.axis_size(axis)
    return lax.all_to_all(
        jnp.broadcast_to(value[None], (peers, *value.shape)), axis, 0, 0, tiled=True
    )


def next_along(block, axis):
    count = lax.axis_size(axis)
    return lax.ppermute(block, axis, [(i, i + 1) for i in range(count - 1)])


def partner(block):
    return lax.ppermute(block, "c", [(0, 1), (1, 0)])


def from_ahead(block, axis, distance):
    count = lax.axis_size(axis)
    return lax.ppermute(block, axis, [(i, (i - distance) % count) for i in range(count)])


def far_from_core(*arrays):
    return [pltpu.with_memory_space_constraint(array, pltpu.HBM) for array in arrays]


def whole_specs(arrays):
    return [pl.BlockSpec(memory_space=pltpu.VMEM) for _ in arrays]


def call(body, outs, arrays, scalars=(), scratch=(), mib=16, space=pltpu.VMEM, **costs):
    return pl.pallas_call(
        body,
        compiler_params=pltpu.CompilerParams(vmem_limit_bytes=mib * 2**20),
        out_shape=outs,
        in_specs=[pl.BlockSpec(memory_space=pltpu.SMEM) for _ in scalars] + whole_specs(arrays),
        out_specs=jax.tree.map(lambda _: pl.BlockSpec(memory_space=space), outs),
        scratch_shapes=list(scratch),
        cost_estimate=pl.CostEstimate(**costs) if costs else None,
    )(*scalars, *arrays)


def natural_order(place_ref, own_ref, other_ref, into_ref, turned, first_lane=0):
    peers_x, _, rows, _ = own_ref.shape
    blocks = into_ref.shape[0] // rows
    lanes = slice(first_lane, first_lane + into_ref.shape[1])
    core, part = place_ref[0], place_ref[2]
    first = part * turned

    def place(by_core):
        for k in range(blocks):
            at = lax.rem(first + k, blocks)
            x = lax.rem(lax.div(at, 2), peers_x)
            into_ref[k * rows : (k + 1) * rows, :] = by_core[k % 2][
                x, lax.div(at, 2 * peers_x), :, lanes
            ]

    @pl.when(core == 0)
    def _():
        place((own_ref, other_ref))

    @pl.when(core == 1)
    def _():
        place((other_ref, own_ref))


def dot_rows(a, b):
    return lax.dot_general(a, b, (((1,), (1,)), ((), ())), preferred_element_type=F32)


def norm_kernel(place_ref, own_ref, ahead_ref, top_ref, bottom_ref, behind_ref, gain_ref, out_ref):
    parts, count, depth = out_ref.shape
    half = count // 2
    part = place_ref[2]

    def rows_of(at, opposite_ref):
        rows = pl.ds(at, half)
        blocks = [
            block.astype(F32)
            for block in (own_ref[rows], ahead_ref[rows], opposite_ref[...], behind_ref[rows])
        ]
        power = sum(jnp.sum(block * block, axis=1, keepdims=True) for block in blocks)
        scale = lax.rsqrt(power / (parts * depth) + EPS)
        for p, block in enumerate(blocks):
            gain = gain_ref[lax.rem(part + p, parts)]
            out_ref[p, rows] = (block * scale * gain).astype(BF16)

    rows_of(0, top_ref)
    rows_of(half, bottom_ref)


def projected(normed_ref, weight_ref, rows):
    parts, _, depth = normed_ref.shape
    return sum(
        jnp.dot(
            normed_ref[p, rows],
            weight_ref[p * depth : (p + 1) * depth],
            preferred_element_type=F32,
        )
        for p in range(parts)
    )


def state_in_kernel(place_ref, normed_ref, own_ref, other_ref, out_ref, weight_ref):
    parts, rows, _ = normed_ref.shape
    turned = weight_ref.shape[0] // own_ref.shape[2] // parts
    natural_order(place_ref, own_ref, other_ref, weight_ref, turned)
    out_ref[...] = projected(normed_ref, weight_ref, slice(HALO, rows)).astype(BF16)


def conv_kernel(
    place_ref, normed_ref, own_ref, other_ref, taps_ref, raw_ref, sums_ref, weight_ref, glu_ref, shifted_ref
):
    parts, rows, _ = normed_ref.shape
    count, width = raw_ref.shape
    turned = weight_ref.shape[0] // own_ref.shape[2] // parts
    natural_order(place_ref, own_ref, other_ref, weight_ref, turned, first_lane=width)
    both = projected(normed_ref, weight_ref, slice(0, rows))
    value = both[:, :width].astype(BF16).astype(F32)
    gate = both[:, width:].astype(BF16).astype(F32)
    glu_ref[:rows] = (value * jax.nn.sigmoid(gate)).astype(BF16).astype(F32)
    glu_ref[rows:] = jnp.zeros((glu_ref.shape[0] - rows, width), F32)
    taps = taps_ref.shape[0]
    sublanes = 8
    for k in range(sublanes):
        shifted_ref[k] = glu_ref[k : k + rows]
    first = HALO - (taps - 1)
    step = 64

    def some_rows(n, _):
        at = pl.multiple_of(n * step, step)
        total = jnp.zeros((step, width), F32)
        for k in range(taps):
            shift, whole = (first + k) % sublanes, (first + k) // sublanes * sublanes
            total = total + taps_ref[k : k + 1] * shifted_ref[shift, pl.ds(at + whole, step)]
        raw_ref[pl.ds(at, step)] = total
        return 0

    lax.fori_loop(0, count // step, some_rows, 0)
    raw = raw_ref[...]
    ones = jnp.ones((8, width), F32)

    def across(value):
        return lax.dot_general(
            ones, value, (((1,), (1,)), ((), ())), precision=EXACT, preferred_element_type=F32
        )[:1]

    sums_ref[0:1] = across(raw)
    sums_ref[1:2] = across(raw * raw)


def squared(re, im):
    return re * re - im * im, 2.0 * re * im


def times(a, b):
    return a[0] * b[0] - a[1] * b[1], a[0] * b[1] + a[1] * b[0]


def exact_dot(a, b):
    return jnp.dot(a, b, preferred_element_type=F32, precision=EXACT)


def spread_over(groups, each):
    row = lax.broadcasted_iota(jnp.int32, (groups, groups * each), 0)
    col = lax.broadcasted_iota(jnp.int32, (groups, groups * each), 1) // each
    return (row == col).astype(F32)


def write_diagonal(out_ref, at, blocks, groups):
    rows, cols = blocks.shape
    pair = jnp.concatenate([blocks, blocks], axis=1)
    row_group = lax.broadcasted_iota(jnp.int32, pair.shape, 0) // (rows // groups)
    col_group = lax.broadcasted_iota(jnp.int32, pair.shape, 1) // cols
    for k in range(groups // 2):
        mine = row_group == col_group + 2 * k
        out_ref[:, at + 2 * k * cols : at + 2 * (k + 1) * cols] = jnp.where(mine, pair, 0.0).astype(BF16)


def table_kernel(*refs):
    inputs, hbm, vmem, done = refs[:10], refs[10:18], refs[18:26], refs[26]

    def send(*which):
        for k in which:
            pltpu.make_async_copy(vmem[k], hbm[k], done.at[k]).start()

    fill_tables(send, *inputs, *vmem)
    for k in range(len(vmem)):
        pltpu.make_async_copy(vmem[k], hbm[k], done.at[k]).wait()


def fill_tables(
    send,
    shift_ref,
    base_ref,
    cos_ref,
    sin_ref,
    start_cos_ref,
    start_sin_ref,
    b_re_ref,
    b_im_ref,
    c_re_ref,
    c_im_ref,
    grow_ref,
    shrink_ref,
    into_ref,
    out_ref,
    hop_re_ref,
    hop_im_ref,
    power_ref,
    total_ref,
):
    groups, count = shift_ref.shape
    lanes = base_ref.shape[1]
    width = grow_ref.shape[1]
    chunks = count // CHUNK
    base = base_ref[...]
    row = lax.broadcasted_iota(jnp.int32, (count, count), 0)
    col = lax.broadcasted_iota(jnp.int32, (count, count), 1)
    earlier = row >= col
    inside = earlier & (row // CHUNK == col // CHUNK)

    def run(which):
        return lax.dot_general(
            which.astype(F32),
            shift_ref[...],
            (((1,), (1,)), ((), ())),
            precision=EXACT,
            preferred_element_type=F32,
        )

    partial, whole = run(inside), run(earlier)
    narrow = exact_dot(partial, spread_over(groups, width // groups))
    grow_ref[...] = jnp.exp(narrow)
    shrink_ref[...] = jnp.exp(-narrow)
    spread = spread_over(groups, lanes // groups)
    wide = exact_dot(whole, spread)
    send(0, 1)
    same = lax.broadcasted_iota(jnp.int32, (groups, 128), 0)
    same = same == lax.broadcasted_iota(jnp.int32, (groups, 128), 1)
    total_ref[...] = exact_dot(whole[count - 8 :], same.astype(F32))[7:]
    sums = jnp.concatenate([partial[(c + 1) * CHUNK - 1 : (c + 1) * CHUNK] for c in range(chunks)])
    near = exact_dot(sums, spread)
    index = lax.broadcasted_iota(jnp.int32, (chunks, lanes), 0)
    size = jnp.exp(CHUNK * base + near)
    turn = (start_cos_ref[1:2], start_sin_ref[1:2])
    hop_re_ref[0], hop_im_ref[0] = size * turn[0], size * turn[1]
    distance, level = 1, 1
    while distance < chunks:
        size = jnp.where(index >= distance, jnp.exp(distance * CHUNK * base + near), 0.0)
        turn = (start_cos_ref[distance : distance + 1], start_sin_ref[distance : distance + 1])
        hop_re_ref[level], hop_im_ref[level] = size * turn[0], size * turn[1]
        near = near + jnp.where(index >= distance, pltpu.roll(near, distance, 0), 0.0)
        distance, level = distance * 2, level + 1
    send(4, 5, 7)
    counts = lax.broadcasted_iota(jnp.int32, (CHUNK, 1), 0).astype(F32)
    inner = (cos_ref[...], sin_ref[...])
    for c in range(chunks):
        at = slice(c * CHUNK, (c + 1) * CHUNK)
        size = jnp.exp((counts + (c * CHUNK + 1)) * base + wide[at])
        turn = times((start_cos_ref[c : c + 1], start_sin_ref[c : c + 1]), inner)
        power_ref[at, :lanes] = (size * turn[0]).astype(BF16)
        power_ref[at, lanes:] = (size * turn[1]).astype(BF16)
    send(6)
    write_diagonal(into_ref, 0, b_re_ref[...], groups)
    write_diagonal(into_ref, lanes, b_im_ref[...], groups)
    send(2)
    write_diagonal(out_ref, 0, c_re_ref[...], groups)
    write_diagonal(out_ref, lanes, -c_im_ref[...], groups)
    send(3)


def scan_kernel(
    u_ref,
    grow_ref,
    shrink_ref,
    in_ref,
    out_mat_ref,
    fwd_re_ref,
    fwd_im_ref,
    inv_re_ref,
    inv_im_ref,
    hop_re_ref,
    hop_im_ref,
    lower_ref,
    skip_ref,
    shift_ref,
    y_ref,
    last_ref,
    cum_re_ref,
    cum_im_ref,
    end_re_ref,
    end_im_ref,
):
    count, _ = u_ref.shape
    states = fwd_re_ref.shape[1]
    chunks = count // CHUNK
    block = lower_ref.shape[0]
    slab = 256
    u = u_ref[...].astype(F32)
    scaled = (u * shrink_ref[...]).astype(BF16)

    def chunked(value):
        return value.reshape(chunks, CHUNK, slab)

    def summed(value):
        value = value.reshape(count, slab).astype(BF16)
        return jnp.concatenate(
            [
                jnp.dot(lower_ref[...], value[k : k + block], preferred_element_type=F32)
                for k in range(0, count, block)
            ]
        )

    def first_pass(j, _):
        at = pl.ds(pl.multiple_of(j * slab, slab), slab)
        at_im = pl.ds(pl.multiple_of(states + j * slab, slab), slab)
        d_re = chunked(jnp.dot(scaled, in_ref[:, at], preferred_element_type=F32))
        d_im = chunked(jnp.dot(scaled, in_ref[:, at_im], preferred_element_type=F32))
        i_re, i_im = inv_re_ref[:, at][None], inv_im_ref[:, at][None]
        cum_re = summed(i_re * d_re - i_im * d_im)
        cum_im = summed(i_re * d_im + i_im * d_re)
        cum_re_ref[:, at] = cum_re
        cum_im_ref[:, at] = cum_im
        end_re_ref[:, at] = chunked(cum_re)[:, CHUNK - 1]
        end_im_ref[:, at] = chunked(cum_im)[:, CHUNK - 1]
        return 0

    lax.fori_loop(0, states // slab, first_pass, 0)

    h_re, h_im = hop_re_ref[0], hop_im_ref[0]
    t_re, t_im = end_re_ref[...], end_im_ref[...]
    s_re = h_re * t_re - h_im * t_im
    s_im = h_re * t_im + h_im * t_re
    for level in range(1, hop_re_ref.shape[0]):
        h_re, h_im = hop_re_ref[level], hop_im_ref[level]
        p_re, p_im = pltpu.roll(s_re, 1 << (level - 1), 0), pltpu.roll(s_im, 1 << (level - 1), 0)
        s_re, s_im = s_re + h_re * p_re - h_im * p_im, s_im + h_re * p_im + h_im * p_re
    last_ref[:, :states] = s_re[chunks - 1 :]
    last_ref[:, states : 2 * states] = s_im[chunks - 1 :]
    last_ref[:, 2 * states :] = shift_ref[...]
    begins = lax.broadcasted_iota(jnp.int32, s_re.shape, 0) > 0
    end_re_ref[...] = jnp.where(begins, pltpu.roll(s_re, 1, 0), 0.0)
    end_im_ref[...] = jnp.where(begins, pltpu.roll(s_im, 1, 0), 0.0)
    y_ref[...] = jnp.zeros(y_ref.shape, F32)

    def second_pass(j, _):
        at = pl.ds(pl.multiple_of(j * slab, slab), slab)
        at_im = pl.ds(pl.multiple_of(states + j * slab, slab), slab)
        t_re = chunked(cum_re_ref[:, at]) + end_re_ref[:, at][:, None]
        t_im = chunked(cum_im_ref[:, at]) + end_im_ref[:, at][:, None]
        f_re, f_im = fwd_re_ref[:, at][None], fwd_im_ref[:, at][None]
        x_re = (f_re * t_re - f_im * t_im).reshape(count, slab).astype(BF16)
        x_im = (f_re * t_im + f_im * t_re).reshape(count, slab).astype(BF16)
        y_ref[...] += dot_rows(x_re, out_mat_ref[:, at]) + dot_rows(x_im, out_mat_ref[:, at_im])
        return 0

    lax.fori_loop(0, states // slab, second_pass, 0)
    y_ref[...] = y_ref[...] * grow_ref[...] + skip_ref[...] * u


def shares(rows_ref, rates_ref, count):
    peers, lanes = rows_ref.shape[0], rates_ref.shape[1]
    shifts = jnp.concatenate([rows_ref[k][:, 2 * lanes :] for k in range(peers)])
    groups = lanes // 64
    sizes = jnp.exp(
        count * rates_ref[0:1] + exact_dot(shifts[:, :groups], spread_over(groups, lanes // groups))
    )
    states = [(rows_ref[k][:, :lanes], rows_ref[k][:, lanes : 2 * lanes]) for k in range(peers)]
    return shifts, sizes, states


def near_kernel(count, place_ref, near_ref, rates_ref, packed_ref, prefix_ref):
    peers, lanes = near_ref.shape[0], rates_ref.shape[1]
    place = place_ref[1] * 2 + place_ref[0]
    shifts, sizes, states = shares(near_ref, rates_ref, count)
    turn = (rates_ref[1:2], rates_ref[2:3])
    zero = jnp.zeros((1, lanes), F32)
    run = before = (zero, zero)
    decay = (zero + 1.0, zero)
    for k in range(peers):
        step = (sizes[k : k + 1] * turn[0], sizes[k : k + 1] * turn[1])
        passed = k < place
        decay = tuple(jnp.where(passed, n, o) for n, o in zip(times(step, decay), decay))
        run = tuple(m + s for m, s in zip(times(step, run), states[k]))
        before = tuple(jnp.where(passed, n, o) for n, o in zip(run, before))
    packed_ref[:, :lanes], packed_ref[:, lanes : 2 * lanes] = run
    packed_ref[:, 2 * lanes :] = jnp.sum(shifts, axis=0, keepdims=True)
    for k, row in enumerate((*before, *decay)):
        prefix_ref[k : k + 1] = row


def merge_rows(distances, place_ref, h, y_ref, power_ref, read_ref, conv_ref, own_ref, other_ref, out_ref, weight_ref):
    natural_order(place_ref, own_ref, other_ref, weight_ref, 0)
    h_re, h_im = h
    lanes = h_re.shape[1]
    block = out_ref.shape[1]
    parts = y_ref.shape[0] // block
    c_re, c_im = read_ref[:, :lanes].astype(F32), read_ref[:, lanes:].astype(F32)
    blend_re = (c_re * h_re + c_im * h_im).astype(BF16)
    blend_im = (c_im * h_re - c_re * h_im).astype(BF16)
    for k, distance in enumerate(distances):
        rows = pl.ds(pl.multiple_of(lax.rem(place_ref[2] + distance, parts) * block, block), block)
        total = (
            y_ref[rows]
            + dot_rows(power_ref[rows, :lanes], blend_re)
            + dot_rows(power_ref[rows, lanes:], blend_im)
        )
        ssm = jax.nn.gelu(total).astype(BF16)
        both = jnp.concatenate([ssm, conv_ref[rows]], axis=1)
        out_ref[k] = dot_rows(both, weight_ref[...]).astype(BF16)


def opposite_kernel(count, place_ref, far_ref, rates_ref, prefix_ref, start_ref, *refs):
    *inputs, out_ref, h_ref, weight_ref = refs
    peers_z, peers_near = far_ref.shape[0], 2 * inputs[-1].shape[0]
    _, sizes, states = shares(far_ref, rates_ref, peers_near * count)
    turn = (rates_ref[1:2], rates_ref[2:3])
    for _ in range(peers_near.bit_length() - 1):
        turn = squared(*turn)
    h = (start_ref[0:1], start_ref[1:2])
    for k in range(peers_z):
        passed = k < place_ref[3]
        step = (sizes[k : k + 1] * turn[0], sizes[k : k + 1] * turn[1])
        moved = times(step, h)
        h = tuple(jnp.where(passed, m + s, o) for m, s, o in zip(moved, states[k], h))
    moved = times((prefix_ref[2:3], prefix_ref[3:4]), h)
    h = (moved[0] + prefix_ref[0:1], moved[1] + prefix_ref[1:2])
    h_ref[0:1], h_ref[1:2] = h
    merge_rows((2,), place_ref, h, *inputs, out_ref, weight_ref)


def rest_kernel(place_ref, h_ref, *refs):
    merge_rows((0, 1, 3), place_ref, (h_ref[0:1], h_ref[1:2]), *refs)


def input_matrix(eigen_real, eigen_imag, step, state_input):
    base = eigen_real * step[:, None]
    theta = eigen_imag * step[:, None]
    magnitude = jnp.exp(base)
    near_re = magnitude * jnp.cos(theta) - 1.0
    near_im = magnitude * jnp.sin(theta)
    modulus = eigen_real * eigen_real + eigen_imag * eigen_imag
    ratio_re = (near_re * eigen_real + near_im * eigen_imag) / modulus
    ratio_im = (near_im * eigen_real - near_re * eigen_imag) / modulus
    in_re, in_im = state_input[0], state_input[1]
    return (
        ratio_re[:, None, :] * in_re - ratio_im[:, None, :] * in_im,
        ratio_re[:, None, :] * in_im + ratio_im[:, None, :] * in_re,
    )


def tables(eigen_real, eigen_imag, log_step, decay_shift, state_input, readout, width):
    groups, states = eigen_real.shape
    lanes = groups * states
    count = decay_shift.shape[1]
    chunks = count // CHUNK
    step = jnp.exp(log_step)
    base = (eigen_real * step[:, None]).reshape(1, lanes)
    theta = (eigen_imag * step[:, None]).reshape(1, lanes)
    inside = jnp.arange(1, CHUNK + 1, dtype=F32)[:, None]
    level, angle = inside * base, inside * theta
    cosine, sine = jnp.cos(angle), jnp.sin(angle)
    grow, shrink = jnp.exp(level), jnp.exp(-level)
    forward = (grow * cosine, grow * sine)
    inverse = (shrink * cosine, -shrink * sine)
    starts = jnp.arange(chunks).astype(F32)[:, None] * CHUNK * theta
    start_cos, start_sin = jnp.cos(starts), jnp.sin(starts)
    whole_turn = (start_cos[chunks // 2], start_sin[chunks // 2])
    b_re, b_im = input_matrix(eigen_real, eigen_imag, step, state_input)
    rows = (groups * state_input.shape[2], states)
    levels = 1 + (chunks - 1).bit_length()
    block = min(count, 256)
    at = jnp.arange(block)
    lower_block = (
        (at[:, None] >= at[None, :]) & (at[:, None] // CHUNK == at[None, :] // CHUNK)
    ).astype(BF16)
    outs = (
        pltpu.HBM((count, width), F32),
        pltpu.HBM((count, width), F32),
        pltpu.HBM((width, 2 * lanes), BF16),
        pltpu.HBM((width, 2 * lanes), BF16),
        pltpu.HBM((levels, chunks, lanes), F32),
        pltpu.HBM((levels, chunks, lanes), F32),
        pltpu.HBM((count, 2 * lanes), BF16),
        pltpu.HBM((1, 128), F32),
    )
    grow, shrink, into, out, hop_re, hop_im, power, total = call(
        table_kernel,
        outs,
        (
            decay_shift,
            base,
            cosine,
            sine,
            start_cos,
            start_sin,
            b_re.reshape(rows),
            b_im.reshape(rows),
            readout[0].reshape(rows),
            readout[1].reshape(rows),
        ),
        scratch=[pltpu.VMEM(o.shape, o.dtype) for o in outs] + [pltpu.SemaphoreType.DMA((len(outs),))],
        mib=24,
        space=pltpu.HBM,
        flops=20 * count * count * groups,
        bytes_accessed=8 * count * lanes,
        transcendentals=count * lanes,
    )
    turn = squared(*(r.reshape(1, -1) for r in whole_turn))
    device = dict(rates=jnp.concatenate([base, *turn]), shift=total)
    scan = (grow, shrink, into, out, *forward, *inverse, hop_re, hop_im, lower_block)
    return scan, power, out, device


def conv_finish(raw, sums, channel_gain):
    for pairs in (((0, 1), (2, 3)), ((0, 3), (1, 2))):
        route = [*pairs, *((b, a) for a, b in pairs)]
        sums = sums + lax.ppermute(sums, "tp", route)
    first, second = (row[:, None] for row in sums)
    middle = first / CONV_W
    spread = second / CONV_W - middle * middle
    scaled = (raw - middle) * lax.rsqrt(spread + EPS) * channel_gain
    return jax.nn.silu(scaled).astype(BF16)


def mixer(
    tokens,
    norm_gain,
    proj_state,
    proj_value,
    proj_gate,
    eigen_real,
    eigen_imag,
    log_step,
    decay_shift,
    state_input,
    readout,
    skip_gain,
    init_state,
    conv_taps,
    channel_gain,
    merge_state,
    merge_conv,
):
    place = jnp.stack([lax.axis_index(axis) for axis in ("c", "x", "tp", "z")]).astype(jnp.int32)
    parts = lax.axis_size("tp")
    count, depth_part = tokens.shape
    depth = depth_part * parts
    rows = count + HALO
    half = rows // 2
    width = proj_state.shape[1]
    merged = jnp.concatenate([merge_state, merge_conv]).T
    planes = copies(
        jnp.concatenate([proj_state, proj_value, proj_gate, merged], axis=1), "z"
    )
    extended = jnp.concatenate([next_along(tokens[count - HALO :], SP), tokens])
    ahead = from_ahead(extended, "tp", 1)
    behind = from_ahead(extended, "tp", -1)
    top = from_ahead(ahead[:half], "tp", 1)
    bottom = from_ahead(behind[half:], "tp", -1)
    scan_tables, power, reads, device = tables(
        eigen_real, eigen_imag, log_step, decay_shift, state_input, readout, width
    )
    planes, total, rates, start = lax.optimization_barrier(
        (planes, device["shift"], device["rates"], init_state.reshape(2, -1))
    )
    device = dict(shift=total, rates=rates)
    project_x = copies(planes[:, :, : 3 * width], "x")
    normed = call(
        norm_kernel,
        jax.ShapeDtypeStruct((parts, rows, depth_part), BF16),
        (*far_from_core(extended, ahead, top, bottom, behind), norm_gain.reshape(parts, 1, depth_part)),
        scalars=(place,),
        mib=12,
        flops=8 * count * depth,
        bytes_accessed=4 * count * depth,
        transcendentals=count,
    )
    project_x, normed = lax.optimization_barrier((project_x, normed))
    project_other = partner(project_x)
    merge_x = copies(planes[:, :, 3 * width :], "x")
    u_in = call(
        state_in_kernel,
        jax.ShapeDtypeStruct((count, width), BF16),
        (normed, project_x, project_other),
        scalars=(place,),
        scratch=(pltpu.VMEM((depth, width), BF16),),
        mib=12,
        flops=2 * count * depth * width,
        bytes_accessed=4 * depth * count,
        transcendentals=0,
    )
    lanes = eigen_real.size
    chunks = count // CHUNK
    y_local, last = call(
        scan_kernel,
        (
            pltpu.HBM((count, width), F32),
            jax.ShapeDtypeStruct((1, 2 * lanes + 128), F32),
        ),
        (u_in, *scan_tables, skip_gain.reshape(1, -1), device["shift"]),
        scratch=(
            pltpu.VMEM((count, lanes), F32),
            pltpu.VMEM((count, lanes), F32),
            pltpu.VMEM((chunks, lanes), F32),
            pltpu.VMEM((chunks, lanes), F32),
        ),
        mib=24,
        flops=12 * count * width * lanes,
        bytes_accessed=8 * count * lanes,
        transcendentals=0,
    )
    last, merge_x = lax.optimization_barrier((last, merge_x))
    near = copies(last, ("x", "c"))
    merge_other = partner(merge_x)
    packed, prefix = call(
        functools.partial(near_kernel, count),
        (
            jax.ShapeDtypeStruct((1, 2 * lanes + 128), F32),
            jax.ShapeDtypeStruct((4, lanes), F32),
        ),
        (near, device["rates"]),
        scalars=(place,),
        mib=4,
        flops=100 * lanes,
        bytes_accessed=64 * lanes,
        transcendentals=8 * lanes,
    )
    far = copies(packed, "z")

    raw, sums = call(
        conv_kernel,
        (
            pltpu.HBM((count, width), F32),
            jax.ShapeDtypeStruct((2, count), F32),
        ),
        (normed, project_x, project_other, conv_taps),
        scalars=(place,),
        scratch=(
            pltpu.VMEM((depth, 2 * width), BF16),
            pltpu.VMEM((rows + 8, width), F32),
            pltpu.VMEM((8, rows, width), F32),
        ),
        mib=20,
        flops=4 * count * depth * width,
        bytes_accessed=4 * depth * count,
        transcendentals=0,
    )
    conv_out = conv_finish(raw, sums, channel_gain)

    block = count // parts
    merge_inputs = (y_local, power, reads, conv_out, merge_x, merge_other)

    def products(kernel, blocks, more, arrays):
        return call(
            kernel,
            (jax.ShapeDtypeStruct((blocks, block, depth), BF16), *more),
            (*arrays, *merge_inputs),
            scalars=(place,),
            scratch=(pltpu.VMEM((depth, 2 * width), BF16),),
            flops=4 * block * blocks * depth * width,
            bytes_accessed=4 * depth * count,
            transcendentals=0,
        )

    opposite, h = products(
        functools.partial(opposite_kernel, count),
        1,
        (jax.ShapeDtypeStruct((2, lanes), F32),),
        (far, device["rates"], prefix, start),
    )
    opposite = opposite[0]
    through_ahead = from_ahead(opposite[: block // 2], "tp", 1)
    through_behind = from_ahead(opposite[block // 2 :], "tp", -1)
    ((mine, to_ahead, to_behind),) = products(rest_kernel, 3, (), (h,))
    empty = jnp.zeros((block // 2, depth), F32)
    to_behind = to_behind.astype(F32) + jnp.concatenate([through_ahead.astype(F32), empty])
    to_ahead = to_ahead.astype(F32) + jnp.concatenate([empty, through_behind.astype(F32)])
    from_next = from_ahead(to_behind.astype(BF16), "tp", 1)
    from_last = from_ahead(to_ahead.astype(BF16), "tp", -1)
    return (mine.astype(F32) + from_next.astype(F32) + from_last.astype(F32)).astype(BF16)


def finer_mesh(mesh):
    cores = 2
    return Mesh(mesh.devices.reshape(16, 4, cores, mesh.shape["tp"]), SP_TP)


def solution(mesh):
    return jax.shard_map(
        mixer,
        mesh=finer_mesh(mesh),
        in_specs=(
            P(SP, "tp"),
            P(),
            P(SP, "tp"),
            P(SP, "tp"),
            P(SP, "tp"),
            P("tp", None),
            P("tp", None),
            P("tp"),
            P("tp", SP),
            P(None, "tp", None, None),
            P(None, "tp", None, None),
            P("tp"),
            P(None, "tp", None),
            P(None, "tp"),
            P("tp"),
            P("tp", SP),
            P("tp", SP),
        ),
        out_specs=P(SP_TP, None),
        check_vma=False,
    )
```

```python
import functools

import jax
import jax.numpy as jnp
from jax import lax
from jax.experimental import pallas as pl
from jax.experimental.pallas import tpu as pltpu
from jax.sharding import Mesh
from jax.sharding import PartitionSpec as P


CONV_W = 1024
SP = ("z", "x", "c")
SP_TP = ("z", "x", "c", "tp")
CHUNK = 32
HALO = 32
EPS = 1e-06
EXACT = lax.Precision.HIGHEST
F32 = jnp.float32
BF16 = jnp.bfloat16


def copies(value, axis):
    peers = lax.axis_size(axis)
    return lax.all_to_all(
        jnp.broadcast_to(value[None], (peers, *value.shape)), axis, 0, 0, tiled=True
    )


def next_along(block, axis):
    count = lax.axis_size(axis)
    return lax.ppermute(block, axis, [(i, i + 1) for i in range(count - 1)])


def partner(block):
    return lax.ppermute(block, "c", [(0, 1), (1, 0)])


def from_ahead(block, axis, distance):
    count = lax.axis_size(axis)
    return lax.ppermute(block, axis, [(i, (i - distance) % count) for i in range(count)])


def from_own_on(planes, axis):
    peers = lax.axis_size(axis)
    return [planes] + [from_ahead(planes, axis, d) for d in range(1, peers)]


def far_from_core(*arrays):
    return [pltpu.with_memory_space_constraint(array, pltpu.HBM) for array in arrays]


def whole_specs(arrays):
    return [pl.BlockSpec(memory_space=pltpu.VMEM) for _ in arrays]


def call(body, outs, arrays, apart=(), scalars=(), scratch=(), mib=16, space=pltpu.VMEM, **costs):
    return pl.pallas_call(
        body,
        compiler_params=pltpu.CompilerParams(vmem_limit_bytes=mib * 2**20),
        out_shape=outs,
        in_specs=[pl.BlockSpec(memory_space=pltpu.SMEM) for _ in scalars]
        + whole_specs(arrays)
        + [pl.BlockSpec(memory_space=pl.ANY) for _ in apart],
        out_specs=jax.tree.map(lambda _: pl.BlockSpec(memory_space=space), outs),
        scratch_shapes=list(scratch),
        cost_estimate=pl.CostEstimate(**costs) if costs else None,
    )(*scalars, *arrays, *apart)


def fetch(source, target, done):
    copy = pltpu.make_async_copy(source, target, done)
    copy.start()
    return copy


def natural_order(place_ref, own_ref, other_ref, into_ref, done, first_lane=0, from_own_x=False):
    peers_x, width = own_ref.shape[0], into_ref.shape[-1]
    begun = []
    for side, ref in enumerate((own_ref, other_ref)):
        core = lax.rem(place_ref[0] + side, 2)
        for x in range(peers_x):
            at = lax.rem(x - place_ref[1] + peers_x, peers_x) if from_own_x else x
            source = ref.at[at, :, :, pl.ds(first_lane, width)]
            begun.append(fetch(source, into_ref.at[:, x, core], done.at[side * peers_x + x]))
    return begun


def arrived(copies_begun):
    for copy in copies_begun:
        copy.wait()


def weight_scratch(merged, width):
    peers_x, peers_z, rows, _ = merged.shape
    return [
        pltpu.VMEM((peers_z, peers_x, 2, rows, width), BF16),
        pltpu.SemaphoreType.DMA((2 * peers_x,)),
    ]


def dot_rows(a, b):
    return lax.dot_general(a, b, (((1,), (1,)), ((), ())), preferred_element_type=F32)


def norm_kernel(place_ref, own_ref, ahead_ref, top_ref, bottom_ref, behind_ref, gain_ref, out_ref):
    parts, count, depth = out_ref.shape
    half = count // 2
    part = place_ref[2]

    def rows_of(at, opposite_ref):
        rows = pl.ds(at, half)
        blocks = [
            block.astype(F32)
            for block in (own_ref[rows], ahead_ref[rows], opposite_ref[...], behind_ref[rows])
        ]
        power = sum(jnp.sum(block * block, axis=1, keepdims=True) for block in blocks)
        scale = lax.rsqrt(power / (parts * depth) + EPS)
        for p, block in enumerate(blocks):
            gain = gain_ref[lax.rem(part + p, parts)]
            out_ref[lax.rem(part + p, parts), rows] = (block * scale * gain).astype(BF16)

    rows_of(0, top_ref)
    rows_of(half, bottom_ref)


def projected(normed_ref, weight_ref, rows):
    parts, _, depth = normed_ref.shape
    weights = weight_ref[...].reshape(parts * depth, -1)
    return sum(
        jnp.dot(
            normed_ref[p, rows],
            weights[p * depth : (p + 1) * depth],
            preferred_element_type=F32,
        )
        for p in range(parts)
    )


def state_in_kernel(place_ref, normed_ref, own_ref, other_ref, out_ref, weight_ref, done):
    rows = normed_ref.shape[1]
    arrived(natural_order(place_ref, own_ref, other_ref, weight_ref, done))
    out_ref[...] = projected(normed_ref, weight_ref, slice(HALO, rows)).astype(BF16)


def conv_kernel(
    place_ref,
    normed_ref,
    taps_ref,
    own_ref,
    other_ref,
    raw_ref,
    sums_ref,
    weight_ref,
    done,
    glu_ref,
    shifted_ref,
):
    _, rows, _ = normed_ref.shape
    count, width = raw_ref.shape
    arrived(natural_order(place_ref, own_ref, other_ref, weight_ref, done, first_lane=width))
    both = projected(normed_ref, weight_ref, slice(0, rows))
    value = both[:, :width].astype(BF16).astype(F32)
    gate = both[:, width:].astype(BF16).astype(F32)
    glu_ref[:rows] = (value * jax.nn.sigmoid(gate)).astype(BF16).astype(F32)
    glu_ref[rows:] = jnp.zeros((glu_ref.shape[0] - rows, width), F32)
    taps = taps_ref.shape[0]
    sublanes = 8
    for k in range(sublanes):
        shifted_ref[k] = glu_ref[k : k + rows]
    first = HALO - (taps - 1)
    step = 64

    def some_rows(n, _):
        at = pl.multiple_of(n * step, step)
        total = jnp.zeros((step, width), F32)
        for k in range(taps):
            shift, whole = (first + k) % sublanes, (first + k) // sublanes * sublanes
            total = total + taps_ref[k : k + 1] * shifted_ref[shift, pl.ds(at + whole, step)]
        raw_ref[pl.ds(at, step)] = total
        return 0

    lax.fori_loop(0, count // step, some_rows, 0)
    raw = raw_ref[...]
    ones = jnp.ones((8, width), F32)

    def across(value):
        return lax.dot_general(
            ones, value, (((1,), (1,)), ((), ())), precision=EXACT, preferred_element_type=F32
        )[:1]

    sums_ref[0:1] = across(raw)
    sums_ref[1:2] = across(raw * raw)


def squared(re, im):
    return re * re - im * im, 2.0 * re * im


def times(a, b):
    return a[0] * b[0] - a[1] * b[1], a[0] * b[1] + a[1] * b[0]


def exact_dot(a, b):
    return jnp.dot(a, b, preferred_element_type=F32, precision=EXACT)


def spread_over(groups, each):
    row = lax.broadcasted_iota(jnp.int32, (groups, groups * each), 0)
    col = lax.broadcasted_iota(jnp.int32, (groups, groups * each), 1) // each
    return (row == col).astype(F32)


def write_diagonal(out_ref, at, blocks, groups):
    rows, cols = blocks.shape
    pair = jnp.concatenate([blocks, blocks], axis=1)
    row_group = lax.broadcasted_iota(jnp.int32, pair.shape, 0) // (rows // groups)
    col_group = lax.broadcasted_iota(jnp.int32, pair.shape, 1) // cols
    for k in range(groups // 2):
        mine = row_group == col_group + 2 * k
        out_ref[:, at + 2 * k * cols : at + 2 * (k + 1) * cols] = jnp.where(mine, pair, 0.0).astype(BF16)


def table_kernel(*refs):
    inputs, hbm, vmem, done = refs[:10], refs[10:18], refs[18:26], refs[26]

    def send(*which):
        for k in which:
            pltpu.make_async_copy(vmem[k], hbm[k], done.at[k]).start()

    fill_tables(send, *inputs, *vmem)
    for k in range(len(vmem)):
        pltpu.make_async_copy(vmem[k], hbm[k], done.at[k]).wait()


def fill_tables(
    send,
    shift_ref,
    base_ref,
    cos_ref,
    sin_ref,
    start_cos_ref,
    start_sin_ref,
    b_re_ref,
    b_im_ref,
    c_re_ref,
    c_im_ref,
    grow_ref,
    shrink_ref,
    into_ref,
    out_ref,
    hop_re_ref,
    hop_im_ref,
    power_ref,
    total_ref,
):
    groups, count = shift_ref.shape
    lanes = base_ref.shape[1]
    width = grow_ref.shape[1]
    chunks = count // CHUNK
    base = base_ref[...]
    row = lax.broadcasted_iota(jnp.int32, (count, count), 0)
    col = lax.broadcasted_iota(jnp.int32, (count, count), 1)
    earlier = row >= col
    inside = earlier & (row // CHUNK == col // CHUNK)

    def run(which):
        return lax.dot_general(
            which.astype(F32),
            shift_ref[...],
            (((1,), (1,)), ((), ())),
            precision=EXACT,
            preferred_element_type=F32,
        )

    partial, whole = run(inside), run(earlier)
    narrow = exact_dot(partial, spread_over(groups, width // groups))
    grow_ref[...] = jnp.exp(narrow)
    shrink_ref[...] = jnp.exp(-narrow)
    spread = spread_over(groups, lanes // groups)
    wide = exact_dot(whole, spread)
    send(0, 1)
    same = lax.broadcasted_iota(jnp.int32, (groups, 128), 0)
    same = same == lax.broadcasted_iota(jnp.int32, (groups, 128), 1)
    total_ref[...] = exact_dot(whole[count - 8 :], same.astype(F32))[7:]
    sums = jnp.concatenate([partial[(c + 1) * CHUNK - 1 : (c + 1) * CHUNK] for c in range(chunks)])
    near = exact_dot(sums, spread)
    index = lax.broadcasted_iota(jnp.int32, (chunks, lanes), 0)
    size = jnp.exp(CHUNK * base + near)
    turn = (start_cos_ref[1:2], start_sin_ref[1:2])
    hop_re_ref[0], hop_im_ref[0] = size * turn[0], size * turn[1]
    distance, level = 1, 1
    while distance < chunks:
        size = jnp.where(index >= distance, jnp.exp(distance * CHUNK * base + near), 0.0)
        turn = (start_cos_ref[distance : distance + 1], start_sin_ref[distance : distance + 1])
        hop_re_ref[level], hop_im_ref[level] = size * turn[0], size * turn[1]
        near = near + jnp.where(index >= distance, pltpu.roll(near, distance, 0), 0.0)
        distance, level = distance * 2, level + 1
    send(4, 5, 7)
    counts = lax.broadcasted_iota(jnp.int32, (CHUNK, 1), 0).astype(F32)
    inner = (cos_ref[...], sin_ref[...])
    for c in range(chunks):
        at = slice(c * CHUNK, (c + 1) * CHUNK)
        size = jnp.exp((counts + (c * CHUNK + 1)) * base + wide[at])
        turn = times((start_cos_ref[c : c + 1], start_sin_ref[c : c + 1]), inner)
        power_ref[at, :lanes] = (size * turn[0]).astype(BF16)
        power_ref[at, lanes:] = (size * turn[1]).astype(BF16)
    send(6)
    write_diagonal(into_ref, 0, b_re_ref[...], groups)
    write_diagonal(into_ref, lanes, b_im_ref[...], groups)
    send(2)
    write_diagonal(out_ref, 0, c_re_ref[...], groups)
    write_diagonal(out_ref, lanes, -c_im_ref[...], groups)
    send(3)


def scan_kernel(
    u_ref,
    grow_ref,
    shrink_ref,
    in_ref,
    out_mat_ref,
    fwd_re_ref,
    fwd_im_ref,
    inv_re_ref,
    inv_im_ref,
    hop_re_ref,
    hop_im_ref,
    lower_ref,
    skip_ref,
    shift_ref,
    y_ref,
    last_ref,
    cum_re_ref,
    cum_im_ref,
    end_re_ref,
    end_im_ref,
):
    count, _ = u_ref.shape
    states = fwd_re_ref.shape[1]
    chunks = count // CHUNK
    block = lower_ref.shape[0]
    slab = 256
    u = u_ref[...].astype(F32)
    scaled = (u * shrink_ref[...]).astype(BF16)

    def chunked(value):
        return value.reshape(chunks, CHUNK, slab)

    def summed(value):
        value = value.reshape(count, slab).astype(BF16)
        return jnp.concatenate(
            [
                jnp.dot(lower_ref[...], value[k : k + block], preferred_element_type=F32)
                for k in range(0, count, block)
            ]
        )

    def first_pass(j, _):
        at = pl.ds(pl.multiple_of(j * slab, slab), slab)
        at_im = pl.ds(pl.multiple_of(states + j * slab, slab), slab)
        d_re = chunked(jnp.dot(scaled, in_ref[:, at], preferred_element_type=F32))
        d_im = chunked(jnp.dot(scaled, in_ref[:, at_im], preferred_element_type=F32))
        i_re, i_im = inv_re_ref[:, at][None], inv_im_ref[:, at][None]
        cum_re = summed(i_re * d_re - i_im * d_im)
        cum_im = summed(i_re * d_im + i_im * d_re)
        cum_re_ref[:, at] = cum_re
        cum_im_ref[:, at] = cum_im
        end_re_ref[:, at] = chunked(cum_re)[:, CHUNK - 1]
        end_im_ref[:, at] = chunked(cum_im)[:, CHUNK - 1]
        return 0

    lax.fori_loop(0, states // slab, first_pass, 0)

    h_re, h_im = hop_re_ref[0], hop_im_ref[0]
    t_re, t_im = end_re_ref[...], end_im_ref[...]
    s_re = h_re * t_re - h_im * t_im
    s_im = h_re * t_im + h_im * t_re
    for level in range(1, hop_re_ref.shape[0]):
        h_re, h_im = hop_re_ref[level], hop_im_ref[level]
        p_re, p_im = pltpu.roll(s_re, 1 << (level - 1), 0), pltpu.roll(s_im, 1 << (level - 1), 0)
        s_re, s_im = s_re + h_re * p_re - h_im * p_im, s_im + h_re * p_im + h_im * p_re
    last_ref[:, :states] = s_re[chunks - 1 :]
    last_ref[:, states : 2 * states] = s_im[chunks - 1 :]
    last_ref[:, 2 * states :] = shift_ref[...]
    begins = lax.broadcasted_iota(jnp.int32, s_re.shape, 0) > 0
    end_re_ref[...] = jnp.where(begins, pltpu.roll(s_re, 1, 0), 0.0)
    end_im_ref[...] = jnp.where(begins, pltpu.roll(s_im, 1, 0), 0.0)
    y_ref[...] = jnp.zeros(y_ref.shape, F32)

    def second_pass(j, _):
        at = pl.ds(pl.multiple_of(j * slab, slab), slab)
        at_im = pl.ds(pl.multiple_of(states + j * slab, slab), slab)
        t_re = chunked(cum_re_ref[:, at]) + end_re_ref[:, at][:, None]
        t_im = chunked(cum_im_ref[:, at]) + end_im_ref[:, at][:, None]
        f_re, f_im = fwd_re_ref[:, at][None], fwd_im_ref[:, at][None]
        x_re = (f_re * t_re - f_im * t_im).reshape(count, slab).astype(BF16)
        x_im = (f_re * t_im + f_im * t_re).reshape(count, slab).astype(BF16)
        y_ref[...] += dot_rows(x_re, out_mat_ref[:, at]) + dot_rows(x_im, out_mat_ref[:, at_im])
        return 0

    lax.fori_loop(0, states // slab, second_pass, 0)
    y_ref[...] = y_ref[...] * grow_ref[...] + skip_ref[...] * u


def shares(rows_ref, rates_ref, count):
    peers, lanes = rows_ref.shape[0], rates_ref.shape[1]
    shifts = jnp.concatenate([rows_ref[k][:, 2 * lanes :] for k in range(peers)])
    groups = lanes // 64
    sizes = jnp.exp(
        count * rates_ref[0:1] + exact_dot(shifts[:, :groups], spread_over(groups, lanes // groups))
    )
    states = [(rows_ref[k][:, :lanes], rows_ref[k][:, lanes : 2 * lanes]) for k in range(peers)]
    return shifts, sizes, states


def near_kernel(count, place_ref, near_ref, rates_ref, packed_ref, prefix_ref):
    peers, lanes = near_ref.shape[0], rates_ref.shape[1]
    place = place_ref[1] * 2 + place_ref[0]
    shifts, sizes, states = shares(near_ref, rates_ref, count)
    turn = (rates_ref[1:2], rates_ref[2:3])
    zero = jnp.zeros((1, lanes), F32)
    run = before = (zero, zero)
    decay = (zero + 1.0, zero)
    for k in range(peers):
        step = (sizes[k : k + 1] * turn[0], sizes[k : k + 1] * turn[1])
        passed = k < place
        decay = tuple(jnp.where(passed, n, o) for n, o in zip(times(step, decay), decay))
        run = tuple(m + s for m, s in zip(times(step, run), states[k]))
        before = tuple(jnp.where(passed, n, o) for n, o in zip(run, before))
    packed_ref[:, :lanes], packed_ref[:, lanes : 2 * lanes] = run
    packed_ref[:, 2 * lanes :] = jnp.sum(shifts, axis=0, keepdims=True)
    for k, row in enumerate((*before, *decay)):
        prefix_ref[k : k + 1] = row


def merge_rows(distances, carried, place_ref, conv_ref, refs):
    (y_all, power_all, read_all, own_ref, other_ref, out_ref) = refs[:6]
    weight_ref, weight_done, y_ref, power_ref, read_ref, done = refs[6:]
    block = out_ref.shape[1]
    parts = conv_ref.shape[0] // block
    places = [
        pl.ds(pl.multiple_of(lax.rem(place_ref[2] + distance, parts) * block, block), block)
        for distance in distances
    ]
    begun = [fetch(read_all, read_ref, done.at[0])]
    for k, rows in enumerate(places):
        begun.append(fetch(power_all.at[rows], power_ref.at[k], done.at[1 + 2 * k]))
        begun.append(fetch(y_all.at[rows], y_ref.at[k], done.at[2 + 2 * k]))
    weights_begun = natural_order(
        place_ref, own_ref, other_ref, weight_ref, weight_done, from_own_x=True
    )
    h_re, h_im = carried()
    lanes = h_re.shape[1]
    arrived(begun)
    c_re, c_im = read_ref[:, :lanes].astype(F32), read_ref[:, lanes:].astype(F32)
    blend_re = (c_re * h_re + c_im * h_im).astype(BF16)
    blend_im = (c_im * h_re - c_re * h_im).astype(BF16)
    arrived(weights_begun)
    weights = weight_ref[...].reshape(out_ref.shape[2], -1)
    for k, rows in enumerate(places):
        total = (
            y_ref[k]
            + dot_rows(power_ref[k, :, :lanes], blend_re)
            + dot_rows(power_ref[k, :, lanes:], blend_im)
        )
        ssm = jax.nn.gelu(total).astype(BF16)
        both = jnp.concatenate([ssm, conv_ref[rows]], axis=1)
        out_ref[k] = dot_rows(both, weights).astype(BF16)


def opposite_kernel(count, place_ref, conv_ref, far_ref, rates_ref, prefix_ref, start_ref, *refs):
    *inputs, out_ref, h_ref, weight_ref, weight_done, y_ref, power_ref, read_ref, done = refs
    peers_z, peers_near = far_ref.shape[0], 2 * inputs[-1].shape[0]

    def carried():
        _, sizes, states = shares(far_ref, rates_ref, peers_near * count)
        turn = (rates_ref[1:2], rates_ref[2:3])
        for _ in range(peers_near.bit_length() - 1):
            turn = squared(*turn)
        h = (start_ref[0:1], start_ref[1:2])
        for k in range(peers_z):
            passed = k < place_ref[3]
            step = (sizes[k : k + 1] * turn[0], sizes[k : k + 1] * turn[1])
            moved = times(step, h)
            h = tuple(jnp.where(passed, m + s, o) for m, s, o in zip(moved, states[k], h))
        moved = times((prefix_ref[2:3], prefix_ref[3:4]), h)
        h = (moved[0] + prefix_ref[0:1], moved[1] + prefix_ref[1:2])
        h_ref[0:1], h_ref[1:2] = h
        return h

    merge_rows(
        (2,),
        carried,
        place_ref,
        conv_ref,
        (*inputs, out_ref, weight_ref, weight_done, y_ref, power_ref, read_ref, done),
    )


def rest_kernel(place_ref, conv_ref, h_ref, *refs):
    merge_rows((0, 1, 3), lambda: (h_ref[0:1], h_ref[1:2]), place_ref, conv_ref, refs)


def input_matrix(eigen_real, eigen_imag, step, state_input):
    base = eigen_real * step[:, None]
    theta = eigen_imag * step[:, None]
    magnitude = jnp.exp(base)
    near_re = magnitude * jnp.cos(theta) - 1.0
    near_im = magnitude * jnp.sin(theta)
    modulus = eigen_real * eigen_real + eigen_imag * eigen_imag
    ratio_re = (near_re * eigen_real + near_im * eigen_imag) / modulus
    ratio_im = (near_im * eigen_real - near_re * eigen_imag) / modulus
    in_re, in_im = state_input[0], state_input[1]
    return (
        ratio_re[:, None, :] * in_re - ratio_im[:, None, :] * in_im,
        ratio_re[:, None, :] * in_im + ratio_im[:, None, :] * in_re,
    )


def tables(eigen_real, eigen_imag, log_step, decay_shift, state_input, readout, width):
    groups, states = eigen_real.shape
    lanes = groups * states
    count = decay_shift.shape[1]
    chunks = count // CHUNK
    step = jnp.exp(log_step)
    base = (eigen_real * step[:, None]).reshape(1, lanes)
    theta = (eigen_imag * step[:, None]).reshape(1, lanes)
    inside = jnp.arange(1, CHUNK + 1, dtype=F32)[:, None]
    level, angle = inside * base, inside * theta
    cosine, sine = jnp.cos(angle), jnp.sin(angle)
    grow, shrink = jnp.exp(level), jnp.exp(-level)
    forward = (grow * cosine, grow * sine)
    inverse = (shrink * cosine, -shrink * sine)
    starts = jnp.arange(chunks).astype(F32)[:, None] * CHUNK * theta
    start_cos, start_sin = jnp.cos(starts), jnp.sin(starts)
    whole_turn = (start_cos[chunks // 2], start_sin[chunks // 2])
    b_re, b_im = input_matrix(eigen_real, eigen_imag, step, state_input)
    rows = (groups * state_input.shape[2], states)
    levels = 1 + (chunks - 1).bit_length()
    block = min(count, 256)
    at = jnp.arange(block)
    lower_block = (
        (at[:, None] >= at[None, :]) & (at[:, None] // CHUNK == at[None, :] // CHUNK)
    ).astype(BF16)
    outs = (
        pltpu.HBM((count, width), F32),
        pltpu.HBM((count, width), F32),
        pltpu.HBM((width, 2 * lanes), BF16),
        pltpu.HBM((width, 2 * lanes), BF16),
        pltpu.HBM((levels, chunks, lanes), F32),
        pltpu.HBM((levels, chunks, lanes), F32),
        pltpu.HBM((count, 2 * lanes), BF16),
        pltpu.HBM((1, 128), F32),
    )
    grow, shrink, into, out, hop_re, hop_im, power, total = call(
        table_kernel,
        outs,
        (
            decay_shift,
            base,
            cosine,
            sine,
            start_cos,
            start_sin,
            b_re.reshape(rows),
            b_im.reshape(rows),
            readout[0].reshape(rows),
            readout[1].reshape(rows),
        ),
        scratch=[pltpu.VMEM(o.shape, o.dtype) for o in outs] + [pltpu.SemaphoreType.DMA((len(outs),))],
        mib=24,
        space=pltpu.HBM,
        flops=20 * count * count * groups,
        bytes_accessed=8 * count * lanes,
        transcendentals=count * lanes,
    )
    turn = squared(*(r.reshape(1, -1) for r in whole_turn))
    device = dict(rates=jnp.concatenate([base, *turn]), shift=total)
    scan = (grow, shrink, into, out, *forward, *inverse, hop_re, hop_im, lower_block)
    return scan, power, out, device


def conv_finish(raw, sums, channel_gain):
    others = [from_ahead(sums, "tp", d) for d in range(1, lax.axis_size("tp"))]
    first, second = (row[:, None] for row in sum(others, sums))
    middle = first / CONV_W
    spread = second / CONV_W - middle * middle
    scaled = (raw - middle) * lax.rsqrt(spread + EPS) * channel_gain
    return jax.nn.silu(scaled).astype(BF16)


def mixer(
    tokens,
    norm_gain,
    proj_state,
    proj_value,
    proj_gate,
    eigen_real,
    eigen_imag,
    log_step,
    decay_shift,
    state_input,
    readout,
    skip_gain,
    init_state,
    conv_taps,
    channel_gain,
    merge_state,
    merge_conv,
):
    place = jnp.stack([lax.axis_index(axis) for axis in ("c", "x", "tp", "z")]).astype(jnp.int32)
    parts = lax.axis_size("tp")
    count, depth_part = tokens.shape
    depth = depth_part * parts
    rows = count + HALO
    half = rows // 2
    width = proj_state.shape[1]
    merged = jnp.concatenate([merge_state, merge_conv]).T
    planes = copies(
        jnp.concatenate([proj_state, proj_value, proj_gate, merged], axis=1), "z"
    )
    extended = jnp.concatenate([next_along(tokens[count - HALO :], SP), tokens])
    ahead = from_ahead(extended, "tp", 1)
    behind = from_ahead(extended, "tp", -1)
    top = from_ahead(ahead[:half], "tp", 1)
    bottom = from_ahead(behind[half:], "tp", -1)
    scan_tables, power, reads, device = tables(
        eigen_real, eigen_imag, log_step, decay_shift, state_input, readout, width
    )
    planes, total, rates, start = lax.optimization_barrier(
        (planes, device["shift"], device["rates"], init_state.reshape(2, -1))
    )
    device = dict(shift=total, rates=rates)
    project_x = copies(planes[:, :, : 3 * width], "x")
    normed = call(
        norm_kernel,
        jax.ShapeDtypeStruct((parts, rows, depth_part), BF16),
        (*far_from_core(extended, ahead, top, bottom, behind), norm_gain.reshape(parts, 1, depth_part)),
        scalars=(place,),
        mib=12,
        flops=8 * count * depth,
        bytes_accessed=4 * count * depth,
        transcendentals=count,
    )
    merge_pieces = from_own_on(planes[:, :, 3 * width :], "x")
    project_other = partner(project_x)
    u_in = call(
        state_in_kernel,
        jax.ShapeDtypeStruct((count, width), BF16),
        (normed,),
        apart=far_from_core(project_x, project_other),
        scalars=(place,),
        scratch=weight_scratch(project_x, width),
        mib=12,
        flops=2 * count * depth * width,
        bytes_accessed=4 * depth * count,
        transcendentals=0,
    )
    lanes = eigen_real.size
    chunks = count // CHUNK
    y_local, last = call(
        scan_kernel,
        (
            pltpu.HBM((count, width), F32),
            jax.ShapeDtypeStruct((1, 2 * lanes + 128), F32),
        ),
        (u_in, *scan_tables, skip_gain.reshape(1, -1), device["shift"]),
        scratch=(
            pltpu.VMEM((count, lanes), F32),
            pltpu.VMEM((count, lanes), F32),
            pltpu.VMEM((chunks, lanes), F32),
            pltpu.VMEM((chunks, lanes), F32),
        ),
        mib=24,
        flops=12 * count * width * lanes,
        bytes_accessed=8 * count * lanes,
        transcendentals=0,
    )
    near = copies(last, ("x", "c"))
    *merge_pieces, _ = lax.optimization_barrier((*merge_pieces, last))
    merge_x = jnp.stack(merge_pieces)
    merge_other = partner(merge_x)
    packed, prefix = call(
        functools.partial(near_kernel, count),
        (
            jax.ShapeDtypeStruct((1, 2 * lanes + 128), F32),
            jax.ShapeDtypeStruct((4, lanes), F32),
        ),
        (near, device["rates"]),
        scalars=(place,),
        mib=4,
        flops=100 * lanes,
        bytes_accessed=64 * lanes,
        transcendentals=8 * lanes,
    )
    far = copies(packed, "z")

    raw, sums = call(
        conv_kernel,
        (
            pltpu.HBM((count, width), F32),
            jax.ShapeDtypeStruct((2, count), F32),
        ),
        (normed, conv_taps),
        apart=far_from_core(project_x, project_other),
        scalars=(place,),
        scratch=(
            *weight_scratch(project_x, 2 * width),
            pltpu.VMEM((rows + 8, width), F32),
            pltpu.VMEM((8, rows, width), F32),
        ),
        mib=20,
        flops=4 * count * depth * width,
        bytes_accessed=4 * depth * count,
        transcendentals=0,
    )
    conv_out = conv_finish(raw, sums, channel_gain)

    block = count // parts

    def products(kernel, blocks, more, arrays):
        return call(
            kernel,
            (jax.ShapeDtypeStruct((blocks, block, depth), BF16), *more),
            (conv_out, *arrays),
            apart=(*far_from_core(y_local, power, reads), merge_x, merge_other),
            scalars=(place,),
            scratch=(
                *weight_scratch(merge_x, 2 * width),
                pltpu.VMEM((blocks, block, width), F32),
                pltpu.VMEM((blocks, block, 2 * lanes), BF16),
                pltpu.VMEM((width, 2 * lanes), BF16),
                pltpu.SemaphoreType.DMA((1 + 2 * blocks,)),
            ),
            flops=4 * block * blocks * depth * width,
            bytes_accessed=4 * depth * count,
            transcendentals=0,
        )

    opposite, h = products(
        functools.partial(opposite_kernel, count),
        1,
        (jax.ShapeDtypeStruct((2, lanes), F32),),
        (far, device["rates"], prefix, start),
    )
    opposite = opposite[0]
    through_ahead = from_ahead(opposite[: block // 2], "tp", 1)
    through_behind = from_ahead(opposite[block // 2 :], "tp", -1)
    ((mine, to_ahead, to_behind),) = products(rest_kernel, 3, (), (h,))
    empty = jnp.zeros((block // 2, depth), F32)
    to_behind = to_behind.astype(F32) + jnp.concatenate([through_ahead.astype(F32), empty])
    to_ahead = to_ahead.astype(F32) + jnp.concatenate([empty, through_behind.astype(F32)])
    from_next = from_ahead(to_behind.astype(BF16), "tp", 1)
    from_last = from_ahead(to_ahead.astype(BF16), "tp", -1)
    return (mine.astype(F32) + from_next.astype(F32) + from_last.astype(F32)).astype(BF16)


def finer_mesh(mesh):
    cores = 2
    return Mesh(mesh.devices.reshape(16, 4, cores, mesh.shape["tp"]), SP_TP)


def solution(mesh):
    return jax.shard_map(
        mixer,
        mesh=finer_mesh(mesh),
        in_specs=(
            P(SP, "tp"),
            P(),
            P(SP, "tp"),
            P(SP, "tp"),
            P(SP, "tp"),
            P("tp", None),
            P("tp", None),
            P("tp"),
            P("tp", SP),
            P(None, "tp", None, None),
            P(None, "tp", None, None),
            P("tp"),
            P(None, "tp", None),
            P(None, "tp"),
            P("tp"),
            P("tp", SP),
            P("tp", SP),
        ),
        out_specs=P(SP_TP, None),
        check_vma=False,
    )
```

```python
import functools

import jax
import jax.numpy as jnp
from jax import lax
from jax.experimental import pallas as pl
from jax.experimental.pallas import tpu as pltpu
from jax.sharding import Mesh
from jax.sharding import PartitionSpec as P


CONV_W = 1024
SP = ("z", "x", "c")
SP_TP = ("z", "x", "c", "tp")
CHUNK = 32
HALO = 32
EPS = 1e-06
EXACT = lax.Precision.HIGHEST
F32 = jnp.float32
BF16 = jnp.bfloat16


def copies(value, axis):
    peers = lax.axis_size(axis)
    return lax.all_to_all(
        jnp.broadcast_to(value[None], (peers, *value.shape)), axis, 0, 0, tiled=True
    )


def next_along(block, axis):
    count = lax.axis_size(axis)
    return lax.ppermute(block, axis, [(i, i + 1) for i in range(count - 1)])


def partner(block):
    return lax.ppermute(block, "c", [(0, 1), (1, 0)])


def from_ahead(block, axis, distance):
    count = lax.axis_size(axis)
    return lax.ppermute(block, axis, [(i, (i - distance) % count) for i in range(count)])


def far_from_core(*arrays):
    return [pltpu.with_memory_space_constraint(array, pltpu.HBM) for array in arrays]


def whole_specs(arrays):
    return [pl.BlockSpec(memory_space=pltpu.VMEM) for _ in arrays]


def call(body, outs, arrays, apart=(), scalars=(), scratch=(), mib=16, space=pltpu.VMEM, **costs):
    return pl.pallas_call(
        body,
        compiler_params=pltpu.CompilerParams(vmem_limit_bytes=mib * 2**20),
        out_shape=outs,
        in_specs=[pl.BlockSpec(memory_space=pltpu.SMEM) for _ in scalars]
        + whole_specs(arrays)
        + [pl.BlockSpec(memory_space=pl.ANY) for _ in apart],
        out_specs=jax.tree.map(lambda _: pl.BlockSpec(memory_space=space), outs),
        scratch_shapes=list(scratch),
        cost_estimate=pl.CostEstimate(**costs) if costs else None,
    )(*scalars, *arrays, *apart)


def fetch(source, target, done):
    copy = pltpu.make_async_copy(source, target, done)
    copy.start()
    return copy


def natural_order(place_ref, own_ref, other_ref, into_ref, done, first_lane=0, from_own_x=False):
    peers_x, width = own_ref.shape[0], into_ref.shape[-1]
    begun = []
    for side, ref in enumerate((own_ref, other_ref)):
        core = lax.rem(place_ref[0] + side, 2)
        for x in range(peers_x):
            at = lax.rem(x - place_ref[1] + peers_x, peers_x) if from_own_x else x
            source = ref.at[at, :, :, pl.ds(first_lane, width)]
            begun.append(fetch(source, into_ref.at[:, x, core], done.at[side * peers_x + x]))
    return begun


def arrived(copies_begun):
    for copy in copies_begun:
        copy.wait()


def weight_scratch(merged, width):
    peers_x, peers_z, rows, _ = merged.shape
    return [
        pltpu.VMEM((peers_z, peers_x, 2, rows, width), BF16),
        pltpu.SemaphoreType.DMA((2 * peers_x,)),
    ]


def dot_rows(a, b):
    return lax.dot_general(a, b, (((1,), (1,)), ((), ())), preferred_element_type=F32)


def norm_kernel(place_ref, own_ref, ahead_ref, top_ref, bottom_ref, behind_ref, gain_ref, out_ref):
    parts, count, depth = out_ref.shape
    half = count // 2
    part = place_ref[2]

    def rows_of(at, opposite_ref):
        rows = pl.ds(at, half)
        blocks = [
            block.astype(F32)
            for block in (own_ref[rows], ahead_ref[rows], opposite_ref[...], behind_ref[rows])
        ]
        power = sum(jnp.sum(block * block, axis=1, keepdims=True) for block in blocks)
        scale = lax.rsqrt(power / (parts * depth) + EPS)
        for p, block in enumerate(blocks):
            gain = gain_ref[lax.rem(part + p, parts)]
            out_ref[lax.rem(part + p, parts), rows] = (block * scale * gain).astype(BF16)

    rows_of(0, top_ref)
    rows_of(half, bottom_ref)


def projected(normed_ref, weight_ref, rows):
    parts, _, depth = normed_ref.shape
    weights = weight_ref[...].reshape(parts * depth, -1)
    return sum(
        jnp.dot(
            normed_ref[p, rows],
            weights[p * depth : (p + 1) * depth],
            preferred_element_type=F32,
        )
        for p in range(parts)
    )


def state_in_kernel(place_ref, normed_ref, own_ref, other_ref, out_ref, weight_ref, done):
    rows = normed_ref.shape[1]
    arrived(natural_order(place_ref, own_ref, other_ref, weight_ref, done))
    out_ref[...] = projected(normed_ref, weight_ref, slice(HALO, rows)).astype(BF16)


def conv_kernel(
    place_ref,
    normed_ref,
    taps_ref,
    own_ref,
    other_ref,
    raw_ref,
    sums_ref,
    weight_ref,
    done,
    glu_ref,
    shifted_ref,
):
    _, rows, _ = normed_ref.shape
    count, width = raw_ref.shape
    arrived(natural_order(place_ref, own_ref, other_ref, weight_ref, done, first_lane=width))
    both = projected(normed_ref, weight_ref, slice(0, rows))
    value = both[:, :width].astype(BF16).astype(F32)
    gate = both[:, width:].astype(BF16).astype(F32)
    glu_ref[:rows] = (value * jax.nn.sigmoid(gate)).astype(BF16).astype(F32)
    glu_ref[rows:] = jnp.zeros((glu_ref.shape[0] - rows, width), F32)
    taps = taps_ref.shape[0]
    sublanes = 8
    for k in range(sublanes):
        shifted_ref[k] = glu_ref[k : k + rows]
    first = HALO - (taps - 1)
    step = 64

    def some_rows(n, _):
        at = pl.multiple_of(n * step, step)
        total = jnp.zeros((step, width), F32)
        for k in range(taps):
            shift, whole = (first + k) % sublanes, (first + k) // sublanes * sublanes
            total = total + taps_ref[k : k + 1] * shifted_ref[shift, pl.ds(at + whole, step)]
        raw_ref[pl.ds(at, step)] = total
        return 0

    lax.fori_loop(0, count // step, some_rows, 0)
    raw = raw_ref[...]
    ones = jnp.ones((8, width), F32)

    def across(value):
        return lax.dot_general(
            ones, value, (((1,), (1,)), ((), ())), precision=EXACT, preferred_element_type=F32
        )[:1]

    sums_ref[0:1] = across(raw)
    sums_ref[1:2] = across(raw * raw)


def squared(re, im):
    return re * re - im * im, 2.0 * re * im


def times(a, b):
    return a[0] * b[0] - a[1] * b[1], a[0] * b[1] + a[1] * b[0]


def exact_dot(a, b):
    return jnp.dot(a, b, preferred_element_type=F32, precision=EXACT)


def spread_over(groups, each):
    row = lax.broadcasted_iota(jnp.int32, (groups, groups * each), 0)
    col = lax.broadcasted_iota(jnp.int32, (groups, groups * each), 1) // each
    return (row == col).astype(F32)


def write_diagonal(out_ref, at, blocks, groups):
    rows, cols = blocks.shape
    pair = jnp.concatenate([blocks, blocks], axis=1)
    row_group = lax.broadcasted_iota(jnp.int32, pair.shape, 0) // (rows // groups)
    col_group = lax.broadcasted_iota(jnp.int32, pair.shape, 1) // cols
    for k in range(groups // 2):
        mine = row_group == col_group + 2 * k
        out_ref[:, at + 2 * k * cols : at + 2 * (k + 1) * cols] = jnp.where(mine, pair, 0.0).astype(BF16)


def table_kernel(*refs):
    inputs, hbm, vmem, done = refs[:10], refs[10:18], refs[18:26], refs[26]

    def send(*which):
        for k in which:
            pltpu.make_async_copy(vmem[k], hbm[k], done.at[k]).start()

    fill_tables(send, *inputs, *vmem)
    for k in range(len(vmem)):
        pltpu.make_async_copy(vmem[k], hbm[k], done.at[k]).wait()


def fill_tables(
    send,
    shift_ref,
    base_ref,
    cos_ref,
    sin_ref,
    start_cos_ref,
    start_sin_ref,
    b_re_ref,
    b_im_ref,
    c_re_ref,
    c_im_ref,
    grow_ref,
    shrink_ref,
    into_ref,
    out_ref,
    hop_re_ref,
    hop_im_ref,
    power_ref,
    total_ref,
):
    groups, count = shift_ref.shape
    lanes = base_ref.shape[1]
    width = grow_ref.shape[1]
    chunks = count // CHUNK
    base = base_ref[...]
    row = lax.broadcasted_iota(jnp.int32, (count, count), 0)
    col = lax.broadcasted_iota(jnp.int32, (count, count), 1)
    earlier = row >= col
    inside = earlier & (row // CHUNK == col // CHUNK)

    def run(which):
        return lax.dot_general(
            which.astype(F32),
            shift_ref[...],
            (((1,), (1,)), ((), ())),
            precision=EXACT,
            preferred_element_type=F32,
        )

    partial, whole = run(inside), run(earlier)
    narrow = exact_dot(partial, spread_over(groups, width // groups))
    grow_ref[...] = jnp.exp(narrow)
    shrink_ref[...] = jnp.exp(-narrow)
    spread = spread_over(groups, lanes // groups)
    wide = exact_dot(whole, spread)
    send(0, 1)
    same = lax.broadcasted_iota(jnp.int32, (groups, 128), 0)
    same = same == lax.broadcasted_iota(jnp.int32, (groups, 128), 1)
    total_ref[...] = exact_dot(whole[count - 8 :], same.astype(F32))[7:]
    sums = jnp.concatenate([partial[(c + 1) * CHUNK - 1 : (c + 1) * CHUNK] for c in range(chunks)])
    near = exact_dot(sums, spread)
    index = lax.broadcasted_iota(jnp.int32, (chunks, lanes), 0)
    size = jnp.exp(CHUNK * base + near)
    turn = (start_cos_ref[1:2], start_sin_ref[1:2])
    hop_re_ref[0], hop_im_ref[0] = size * turn[0], size * turn[1]
    distance, level = 1, 1
    while distance < chunks:
        size = jnp.where(index >= distance, jnp.exp(distance * CHUNK * base + near), 0.0)
        turn = (start_cos_ref[distance : distance + 1], start_sin_ref[distance : distance + 1])
        hop_re_ref[level], hop_im_ref[level] = size * turn[0], size * turn[1]
        near = near + jnp.where(index >= distance, pltpu.roll(near, distance, 0), 0.0)
        distance, level = distance * 2, level + 1
    send(4, 5, 7)
    counts = lax.broadcasted_iota(jnp.int32, (CHUNK, 1), 0).astype(F32)
    inner = (cos_ref[...], sin_ref[...])
    for c in range(chunks):
        at = slice(c * CHUNK, (c + 1) * CHUNK)
        size = jnp.exp((counts + (c * CHUNK + 1)) * base + wide[at])
        turn = times((start_cos_ref[c : c + 1], start_sin_ref[c : c + 1]), inner)
        power_ref[at, :lanes] = (size * turn[0]).astype(BF16)
        power_ref[at, lanes:] = (size * turn[1]).astype(BF16)
    send(6)
    write_diagonal(into_ref, 0, b_re_ref[...], groups)
    write_diagonal(into_ref, lanes, b_im_ref[...], groups)
    send(2)
    write_diagonal(out_ref, 0, c_re_ref[...], groups)
    write_diagonal(out_ref, lanes, -c_im_ref[...], groups)
    send(3)


def scan_kernel(
    u_ref,
    grow_ref,
    shrink_ref,
    in_ref,
    out_mat_ref,
    fwd_re_ref,
    fwd_im_ref,
    inv_re_ref,
    inv_im_ref,
    hop_re_ref,
    hop_im_ref,
    lower_ref,
    skip_ref,
    shift_ref,
    y_ref,
    last_ref,
    cum_re_ref,
    cum_im_ref,
    end_re_ref,
    end_im_ref,
):
    count, _ = u_ref.shape
    states = fwd_re_ref.shape[1]
    chunks = count // CHUNK
    block = lower_ref.shape[0]
    slab = 256
    u = u_ref[...].astype(F32)
    scaled = (u * shrink_ref[...]).astype(BF16)

    def chunked(value):
        return value.reshape(chunks, CHUNK, slab)

    def summed(value):
        value = value.reshape(count, slab).astype(BF16)
        return jnp.concatenate(
            [
                jnp.dot(lower_ref[...], value[k : k + block], preferred_element_type=F32)
                for k in range(0, count, block)
            ]
        )

    def first_pass(j, _):
        at = pl.ds(pl.multiple_of(j * slab, slab), slab)
        at_im = pl.ds(pl.multiple_of(states + j * slab, slab), slab)
        d_re = chunked(jnp.dot(scaled, in_ref[:, at], preferred_element_type=F32))
        d_im = chunked(jnp.dot(scaled, in_ref[:, at_im], preferred_element_type=F32))
        i_re, i_im = inv_re_ref[:, at][None], inv_im_ref[:, at][None]
        cum_re = summed(i_re * d_re - i_im * d_im)
        cum_im = summed(i_re * d_im + i_im * d_re)
        cum_re_ref[:, at] = cum_re
        cum_im_ref[:, at] = cum_im
        end_re_ref[:, at] = chunked(cum_re)[:, CHUNK - 1]
        end_im_ref[:, at] = chunked(cum_im)[:, CHUNK - 1]
        return 0

    lax.fori_loop(0, states // slab, first_pass, 0)

    h_re, h_im = hop_re_ref[0], hop_im_ref[0]
    t_re, t_im = end_re_ref[...], end_im_ref[...]
    s_re = h_re * t_re - h_im * t_im
    s_im = h_re * t_im + h_im * t_re
    for level in range(1, hop_re_ref.shape[0]):
        h_re, h_im = hop_re_ref[level], hop_im_ref[level]
        p_re, p_im = pltpu.roll(s_re, 1 << (level - 1), 0), pltpu.roll(s_im, 1 << (level - 1), 0)
        s_re, s_im = s_re + h_re * p_re - h_im * p_im, s_im + h_re * p_im + h_im * p_re
    last_ref[:, :states] = s_re[chunks - 1 :]
    last_ref[:, states : 2 * states] = s_im[chunks - 1 :]
    last_ref[:, 2 * states :] = shift_ref[...]
    begins = lax.broadcasted_iota(jnp.int32, s_re.shape, 0) > 0
    end_re_ref[...] = jnp.where(begins, pltpu.roll(s_re, 1, 0), 0.0)
    end_im_ref[...] = jnp.where(begins, pltpu.roll(s_im, 1, 0), 0.0)
    y_ref[...] = jnp.zeros(y_ref.shape, F32)

    def second_pass(j, _):
        at = pl.ds(pl.multiple_of(j * slab, slab), slab)
        at_im = pl.ds(pl.multiple_of(states + j * slab, slab), slab)
        t_re = chunked(cum_re_ref[:, at]) + end_re_ref[:, at][:, None]
        t_im = chunked(cum_im_ref[:, at]) + end_im_ref[:, at][:, None]
        f_re, f_im = fwd_re_ref[:, at][None], fwd_im_ref[:, at][None]
        x_re = (f_re * t_re - f_im * t_im).reshape(count, slab).astype(BF16)
        x_im = (f_re * t_im + f_im * t_re).reshape(count, slab).astype(BF16)
        y_ref[...] += dot_rows(x_re, out_mat_ref[:, at]) + dot_rows(x_im, out_mat_ref[:, at_im])
        return 0

    lax.fori_loop(0, states // slab, second_pass, 0)
    y_ref[...] = y_ref[...] * grow_ref[...] + skip_ref[...] * u


def shares(rows_ref, rates_ref, count):
    peers, lanes = rows_ref.shape[0], rates_ref.shape[1]
    shifts = jnp.concatenate([rows_ref[k][:, 2 * lanes :] for k in range(peers)])
    groups = lanes // 64
    sizes = jnp.exp(
        count * rates_ref[0:1] + exact_dot(shifts[:, :groups], spread_over(groups, lanes // groups))
    )
    states = [(rows_ref[k][:, :lanes], rows_ref[k][:, lanes : 2 * lanes]) for k in range(peers)]
    return shifts, sizes, states


def near_kernel(count, place_ref, near_ref, rates_ref, packed_ref, prefix_ref):
    peers, lanes = near_ref.shape[0], rates_ref.shape[1]
    place = place_ref[1] * 2 + place_ref[0]
    shifts, sizes, states = shares(near_ref, rates_ref, count)
    turn = (rates_ref[1:2], rates_ref[2:3])
    zero = jnp.zeros((1, lanes), F32)
    run = before = (zero, zero)
    decay = (zero + 1.0, zero)
    for k in range(peers):
        step = (sizes[k : k + 1] * turn[0], sizes[k : k + 1] * turn[1])
        passed = k < place
        decay = tuple(jnp.where(passed, n, o) for n, o in zip(times(step, decay), decay))
        run = tuple(m + s for m, s in zip(times(step, run), states[k]))
        before = tuple(jnp.where(passed, n, o) for n, o in zip(run, before))
    packed_ref[:, :lanes], packed_ref[:, lanes : 2 * lanes] = run
    packed_ref[:, 2 * lanes :] = jnp.sum(shifts, axis=0, keepdims=True)
    for k, row in enumerate((*before, *decay)):
        prefix_ref[k : k + 1] = row


def channel_norm(raw, first, second, gain):
    row = lax.broadcasted_iota(jnp.int32, (raw.shape[0], raw.shape[0]), 0)
    same = row == lax.broadcasted_iota(jnp.int32, row.shape, 1)

    def upright(line):
        return jnp.sum(jnp.where(same, line, 0.0), axis=1, keepdims=True)

    middle = upright(first) / CONV_W
    spread = upright(second) / CONV_W - middle * middle
    scaled = (raw - middle) * lax.rsqrt(spread + EPS) * gain
    return jax.nn.silu(scaled).astype(BF16)


def merge_rows(distances, carried, place_ref, channel, refs):
    gain_ref, *sums_refs = channel
    raw_all, y_all, power_all, read_all, own_ref, other_ref, out_ref = refs[:7]
    weight_ref, weight_done, raw_ref, y_ref, power_ref, read_ref, done = refs[7:]
    block = out_ref.shape[1]
    parts = len(sums_refs)
    sums = sum((ref[...] for ref in sums_refs[1:]), sums_refs[0][...])
    places = [
        pl.ds(pl.multiple_of(lax.rem(place_ref[2] + distance, parts) * block, block), block)
        for distance in distances
    ]
    begun = [fetch(read_all, read_ref, done.at[0])]
    for k, rows in enumerate(places):
        begun.append(fetch(power_all.at[rows], power_ref.at[k], done.at[1 + 3 * k]))
        begun.append(fetch(y_all.at[rows], y_ref.at[k], done.at[2 + 3 * k]))
        begun.append(fetch(raw_all.at[rows], raw_ref.at[k], done.at[3 + 3 * k]))
    weights_begun = natural_order(
        place_ref, own_ref, other_ref, weight_ref, weight_done, from_own_x=True
    )
    h_re, h_im = carried()
    lanes = h_re.shape[1]
    arrived(begun)
    c_re, c_im = read_ref[:, :lanes].astype(F32), read_ref[:, lanes:].astype(F32)
    blend_re = (c_re * h_re + c_im * h_im).astype(BF16)
    blend_im = (c_im * h_re - c_re * h_im).astype(BF16)
    arrived(weights_begun)
    weights = weight_ref[...].reshape(out_ref.shape[2], -1)
    for k, distance in enumerate(distances):
        mine = lax.rem(place_ref[2] + distance, parts)
        first, second = jnp.zeros((1, block), F32), jnp.zeros((1, block), F32)
        for part in range(parts):
            lines = sums[:, part * block : (part + 1) * block]
            first = jnp.where(mine == part, lines[0:1], first)
            second = jnp.where(mine == part, lines[1:2], second)
        conv = channel_norm(raw_ref[k], first, second, gain_ref[...])
        total = (
            y_ref[k]
            + dot_rows(power_ref[k, :, :lanes], blend_re)
            + dot_rows(power_ref[k, :, lanes:], blend_im)
        )
        ssm = jax.nn.gelu(total).astype(BF16)
        both = jnp.concatenate([ssm, conv], axis=1)
        out_ref[k] = dot_rows(both, weights).astype(BF16)


def opposite_kernel(count, place_ref, *refs):
    channel, (far_ref, rates_ref, prefix_ref, start_ref) = refs[:5], refs[5:9]
    *inputs, out_ref, h_ref, weight_ref, weight_done, raw_ref, y_ref, power_ref, read_ref, done = refs[9:]
    peers_z, peers_near = far_ref.shape[0], 2 * inputs[-1].shape[0]

    def carried():
        _, sizes, states = shares(far_ref, rates_ref, peers_near * count)
        turn = (rates_ref[1:2], rates_ref[2:3])
        for _ in range(peers_near.bit_length() - 1):
            turn = squared(*turn)
        h = (start_ref[0:1], start_ref[1:2])
        for k in range(peers_z):
            passed = k < place_ref[3]
            step = (sizes[k : k + 1] * turn[0], sizes[k : k + 1] * turn[1])
            moved = times(step, h)
            h = tuple(jnp.where(passed, m + s, o) for m, s, o in zip(moved, states[k], h))
        moved = times((prefix_ref[2:3], prefix_ref[3:4]), h)
        h = (moved[0] + prefix_ref[0:1], moved[1] + prefix_ref[1:2])
        h_ref[0:1], h_ref[1:2] = h
        return h

    merge_rows(
        (2,),
        carried,
        place_ref,
        channel,
        (*inputs, out_ref, weight_ref, weight_done, raw_ref, y_ref, power_ref, read_ref, done),
    )


def rest_kernel(place_ref, *refs):
    channel, h_ref = refs[:5], refs[5]
    merge_rows((0, 1, 3), lambda: (h_ref[0:1], h_ref[1:2]), place_ref, channel, refs[6:])


def input_matrix(eigen_real, eigen_imag, step, state_input):
    base = eigen_real * step[:, None]
    theta = eigen_imag * step[:, None]
    magnitude = jnp.exp(base)
    near_re = magnitude * jnp.cos(theta) - 1.0
    near_im = magnitude * jnp.sin(theta)
    modulus = eigen_real * eigen_real + eigen_imag * eigen_imag
    ratio_re = (near_re * eigen_real + near_im * eigen_imag) / modulus
    ratio_im = (near_im * eigen_real - near_re * eigen_imag) / modulus
    in_re, in_im = state_input[0], state_input[1]
    return (
        ratio_re[:, None, :] * in_re - ratio_im[:, None, :] * in_im,
        ratio_re[:, None, :] * in_im + ratio_im[:, None, :] * in_re,
    )


def tables(eigen_real, eigen_imag, log_step, decay_shift, state_input, readout, width):
    groups, states = eigen_real.shape
    lanes = groups * states
    count = decay_shift.shape[1]
    chunks = count // CHUNK
    step = jnp.exp(log_step)
    base = (eigen_real * step[:, None]).reshape(1, lanes)
    theta = (eigen_imag * step[:, None]).reshape(1, lanes)
    inside = jnp.arange(1, CHUNK + 1, dtype=F32)[:, None]
    level, angle = inside * base, inside * theta
    cosine, sine = jnp.cos(angle), jnp.sin(angle)
    grow, shrink = jnp.exp(level), jnp.exp(-level)
    forward = (grow * cosine, grow * sine)
    inverse = (shrink * cosine, -shrink * sine)
    starts = jnp.arange(chunks).astype(F32)[:, None] * CHUNK * theta
    start_cos, start_sin = jnp.cos(starts), jnp.sin(starts)
    whole_turn = (start_cos[chunks // 2], start_sin[chunks // 2])
    b_re, b_im = input_matrix(eigen_real, eigen_imag, step, state_input)
    rows = (groups * state_input.shape[2], states)
    levels = 1 + (chunks - 1).bit_length()
    block = min(count, 256)
    at = jnp.arange(block)
    lower_block = (
        (at[:, None] >= at[None, :]) & (at[:, None] // CHUNK == at[None, :] // CHUNK)
    ).astype(BF16)
    outs = (
        pltpu.HBM((count, width), F32),
        pltpu.HBM((count, width), F32),
        pltpu.HBM((width, 2 * lanes), BF16),
        pltpu.HBM((width, 2 * lanes), BF16),
        pltpu.HBM((levels, chunks, lanes), F32),
        pltpu.HBM((levels, chunks, lanes), F32),
        pltpu.HBM((count, 2 * lanes), BF16),
        pltpu.HBM((1, 128), F32),
    )
    grow, shrink, into, out, hop_re, hop_im, power, total = call(
        table_kernel,
        outs,
        (
            decay_shift,
            base,
            cosine,
            sine,
            start_cos,
            start_sin,
            b_re.reshape(rows),
            b_im.reshape(rows),
            readout[0].reshape(rows),
            readout[1].reshape(rows),
        ),
        scratch=[pltpu.VMEM(o.shape, o.dtype) for o in outs] + [pltpu.SemaphoreType.DMA((len(outs),))],
        mib=24,
        space=pltpu.HBM,
        flops=20 * count * count * groups,
        bytes_accessed=8 * count * lanes,
        transcendentals=count * lanes,
    )
    turn = squared(*(r.reshape(1, -1) for r in whole_turn))
    device = dict(rates=jnp.concatenate([base, *turn]), shift=total)
    scan = (grow, shrink, into, out, *forward, *inverse, hop_re, hop_im, lower_block)
    return scan, power, out, device


def mixer(
    tokens,
    norm_gain,
    proj_state,
    proj_value,
    proj_gate,
    eigen_real,
    eigen_imag,
    log_step,
    decay_shift,
    state_input,
    readout,
    skip_gain,
    init_state,
    conv_taps,
    channel_gain,
    merge_state,
    merge_conv,
):
    place = jnp.stack([lax.axis_index(axis) for axis in ("c", "x", "tp", "z")]).astype(jnp.int32)
    parts = lax.axis_size("tp")
    count, depth_part = tokens.shape
    depth = depth_part * parts
    rows = count + HALO
    half = rows // 2
    width = proj_state.shape[1]
    merged = jnp.concatenate([merge_state, merge_conv]).T
    planes = copies(
        jnp.concatenate([proj_state, proj_value, proj_gate, merged], axis=1), "z"
    )
    extended = jnp.concatenate([next_along(tokens[count - HALO :], SP), tokens])
    ahead = from_ahead(extended, "tp", 1)
    behind = from_ahead(extended, "tp", -1)
    top = from_ahead(ahead[:half], "tp", 1)
    bottom = from_ahead(behind[half:], "tp", -1)
    scan_tables, power, reads, device = tables(
        eigen_real, eigen_imag, log_step, decay_shift, state_input, readout, width
    )
    planes, total, rates, start = lax.optimization_barrier(
        (planes, device["shift"], device["rates"], init_state.reshape(2, -1))
    )
    device = dict(shift=total, rates=rates)
    project_x = copies(planes[:, :, : 3 * width], "x")
    normed = call(
        norm_kernel,
        jax.ShapeDtypeStruct((parts, rows, depth_part), BF16),
        (*far_from_core(extended, ahead, top, bottom, behind), norm_gain.reshape(parts, 1, depth_part)),
        scalars=(place,),
        mib=12,
        flops=8 * count * depth,
        bytes_accessed=4 * count * depth,
        transcendentals=count,
    )
    merge_planes, normed = lax.optimization_barrier((planes[:, :, 3 * width :], normed))
    merge_ahead = from_ahead(merge_planes, "x", 1)
    merge_behind = from_ahead(merge_planes, "x", -1)
    merge_across = from_ahead(merge_planes, "x", 2)
    merge_pieces = (merge_planes, merge_ahead, merge_across, merge_behind)
    project_other = partner(project_x)
    u_in = call(
        state_in_kernel,
        jax.ShapeDtypeStruct((count, width), BF16),
        (normed,),
        apart=far_from_core(project_x, project_other),
        scalars=(place,),
        scratch=weight_scratch(project_x, width),
        mib=12,
        flops=2 * count * depth * width,
        bytes_accessed=4 * depth * count,
        transcendentals=0,
    )
    lanes = eigen_real.size
    chunks = count // CHUNK
    y_local, last = call(
        scan_kernel,
        (
            pltpu.HBM((count, width), F32),
            jax.ShapeDtypeStruct((1, 2 * lanes + 128), F32),
        ),
        (u_in, *scan_tables, skip_gain.reshape(1, -1), device["shift"]),
        scratch=(
            pltpu.VMEM((count, lanes), F32),
            pltpu.VMEM((count, lanes), F32),
            pltpu.VMEM((chunks, lanes), F32),
            pltpu.VMEM((chunks, lanes), F32),
        ),
        mib=24,
        flops=12 * count * width * lanes,
        bytes_accessed=8 * count * lanes,
        transcendentals=0,
    )
    near = copies(last, ("x", "c"))
    *merge_pieces, _ = lax.optimization_barrier((*merge_pieces, last))
    merge_x = jnp.stack(merge_pieces)
    merge_other = partner(merge_x)
    packed, prefix = call(
        functools.partial(near_kernel, count),
        (
            jax.ShapeDtypeStruct((1, 2 * lanes + 128), F32),
            jax.ShapeDtypeStruct((4, lanes), F32),
        ),
        (near, device["rates"]),
        scalars=(place,),
        mib=4,
        flops=100 * lanes,
        bytes_accessed=64 * lanes,
        transcendentals=8 * lanes,
    )
    far = copies(packed, "z")

    raw, sums = call(
        conv_kernel,
        (
            pltpu.HBM((count, width), F32),
            jax.ShapeDtypeStruct((2, count), F32),
        ),
        (normed, conv_taps),
        apart=far_from_core(project_x, project_other),
        scalars=(place,),
        scratch=(
            *weight_scratch(project_x, 2 * width),
            pltpu.VMEM((rows + 8, width), F32),
            pltpu.VMEM((8, rows, width), F32),
        ),
        mib=20,
        flops=4 * count * depth * width,
        bytes_accessed=4 * depth * count,
        transcendentals=0,
    )
    all_sums = [sums] + [from_ahead(sums, "tp", d) for d in range(1, parts)]

    block = count // parts

    def products(kernel, blocks, more, arrays):
        return call(
            kernel,
            (jax.ShapeDtypeStruct((blocks, block, depth), BF16), *more),
            (channel_gain.reshape(1, -1), *all_sums, *arrays),
            apart=(*far_from_core(raw, y_local, power, reads), merge_x, merge_other),
            scalars=(place,),
            scratch=(
                *weight_scratch(merge_x, 2 * width),
                pltpu.VMEM((blocks, block, width), F32),
                pltpu.VMEM((blocks, block, width), F32),
                pltpu.VMEM((blocks, block, 2 * lanes), BF16),
                pltpu.VMEM((width, 2 * lanes), BF16),
                pltpu.SemaphoreType.DMA((1 + 3 * blocks,)),
            ),
            flops=4 * block * blocks * depth * width,
            bytes_accessed=4 * depth * count,
            transcendentals=0,
        )

    opposite, h = products(
        functools.partial(opposite_kernel, count),
        1,
        (jax.ShapeDtypeStruct((2, lanes), F32),),
        (far, device["rates"], prefix, start),
    )
    opposite = opposite[0]
    through_ahead = from_ahead(opposite[: block // 2], "tp", 1)
    through_behind = from_ahead(opposite[block // 2 :], "tp", -1)
    ((mine, to_ahead, to_behind),) = products(rest_kernel, 3, (), (h,))
    empty = jnp.zeros((block // 2, depth), F32)
    to_behind = to_behind.astype(F32) + jnp.concatenate([through_ahead.astype(F32), empty])
    to_ahead = to_ahead.astype(F32) + jnp.concatenate([empty, through_behind.astype(F32)])
    from_next = from_ahead(to_behind.astype(BF16), "tp", 1)
    from_last = from_ahead(to_ahead.astype(BF16), "tp", -1)
    return (mine.astype(F32) + from_next.astype(F32) + from_last.astype(F32)).astype(BF16)


def finer_mesh(mesh):
    cores = 2
    return Mesh(mesh.devices.reshape(16, 4, cores, mesh.shape["tp"]), SP_TP)


def solution(mesh):
    return jax.shard_map(
        mixer,
        mesh=finer_mesh(mesh),
        in_specs=(
            P(SP, "tp"),
            P(),
            P(SP, "tp"),
            P(SP, "tp"),
            P(SP, "tp"),
            P("tp", None),
            P("tp", None),
            P("tp"),
            P("tp", SP),
            P(None, "tp", None, None),
            P(None, "tp", None, None),
            P("tp"),
            P(None, "tp", None),
            P(None, "tp"),
            P("tp"),
            P("tp", SP),
            P("tp", SP),
        ),
        out_specs=P(SP_TP, None),
        check_vma=False,
    )
```

```python
import functools

import jax
import jax.numpy as jnp
from jax import lax
from jax.experimental import pallas as pl
from jax.experimental.pallas import tpu as pltpu
from jax.sharding import Mesh
from jax.sharding import PartitionSpec as P


CONV_W = 1024
SP = ("z", "x", "c")
SP_TP = ("z", "x", "c", "tp")
CHUNK = 32
HALO = 32
EPS = 1e-06
EXACT = lax.Precision.HIGHEST
F32 = jnp.float32
BF16 = jnp.bfloat16


def copies(value, axis):
    peers = lax.axis_size(axis)
    return lax.all_to_all(
        jnp.broadcast_to(value[None], (peers, *value.shape)), axis, 0, 0, tiled=True
    )


def next_along(block, axis):
    count = lax.axis_size(axis)
    return lax.ppermute(block, axis, [(i, i + 1) for i in range(count - 1)])


def partner(block):
    return lax.ppermute(block, "c", [(0, 1), (1, 0)])


def from_ahead(block, axis, distance):
    count = lax.axis_size(axis)
    return lax.ppermute(block, axis, [(i, (i - distance) % count) for i in range(count)])


def far_from_core(*arrays):
    return [pltpu.with_memory_space_constraint(array, pltpu.HBM) for array in arrays]


def whole_specs(arrays):
    return [pl.BlockSpec(memory_space=pltpu.VMEM) for _ in arrays]


def call(body, outs, arrays, apart=(), scalars=(), scratch=(), mib=16, space=pltpu.VMEM, **costs):
    return pl.pallas_call(
        body,
        compiler_params=pltpu.CompilerParams(vmem_limit_bytes=mib * 2**20),
        out_shape=outs,
        in_specs=[pl.BlockSpec(memory_space=pltpu.SMEM) for _ in scalars]
        + whole_specs(arrays)
        + [pl.BlockSpec(memory_space=pl.ANY) for _ in apart],
        out_specs=jax.tree.map(lambda _: pl.BlockSpec(memory_space=space), outs),
        scratch_shapes=list(scratch),
        cost_estimate=pl.CostEstimate(**costs) if costs else None,
    )(*scalars, *arrays, *apart)


def fetch(source, target, done):
    copy = pltpu.make_async_copy(source, target, done)
    copy.start()
    return copy


def natural_order(place_ref, own_ref, other_ref, into_ref, done, first_lane=0, from_own_x=False):
    peers_x, width = own_ref.shape[0], into_ref.shape[-1]
    begun = []
    for side, ref in enumerate((own_ref, other_ref)):
        core = lax.rem(place_ref[0] + side, 2)
        for x in range(peers_x):
            at = lax.rem(x - place_ref[1] + peers_x, peers_x) if from_own_x else x
            source = ref.at[at, :, :, pl.ds(first_lane, width)]
            begun.append(fetch(source, into_ref.at[:, x, core], done.at[side * peers_x + x]))
    return begun


def arrived(copies_begun):
    for copy in copies_begun:
        copy.wait()


def weight_scratch(merged, width):
    peers_x, peers_z, rows, _ = merged.shape
    return [
        pltpu.VMEM((peers_z, peers_x, 2, rows, width), BF16),
        pltpu.SemaphoreType.DMA((2 * peers_x,)),
    ]


def dot_rows(a, b):
    return lax.dot_general(a, b, (((1,), (1,)), ((), ())), preferred_element_type=F32)


def norm_kernel(place_ref, own_ref, ahead_ref, top_ref, bottom_ref, behind_ref, gain_ref, out_ref):
    parts, count, depth = out_ref.shape
    half = count // 2
    part = place_ref[2]

    def rows_of(at, opposite_ref):
        rows = pl.ds(at, half)
        blocks = [
            block.astype(F32)
            for block in (own_ref[rows], ahead_ref[rows], opposite_ref[...], behind_ref[rows])
        ]
        power = sum(jnp.sum(block * block, axis=1, keepdims=True) for block in blocks)
        scale = lax.rsqrt(power / (parts * depth) + EPS)
        for p, block in enumerate(blocks):
            gain = gain_ref[lax.rem(part + p, parts)]
            out_ref[lax.rem(part + p, parts), rows] = (block * scale * gain).astype(BF16)

    rows_of(0, top_ref)
    rows_of(half, bottom_ref)


def projected(normed_ref, weight_ref, rows):
    parts, _, depth = normed_ref.shape
    weights = weight_ref[...].reshape(parts * depth, -1)
    return sum(
        jnp.dot(
            normed_ref[p, rows],
            weights[p * depth : (p + 1) * depth],
            preferred_element_type=F32,
        )
        for p in range(parts)
    )


def state_in_kernel(place_ref, normed_ref, own_ref, other_ref, out_ref, weight_ref, done):
    rows = normed_ref.shape[1]
    arrived(natural_order(place_ref, own_ref, other_ref, weight_ref, done))
    out_ref[...] = projected(normed_ref, weight_ref, slice(HALO, rows)).astype(BF16)


def conv_kernel(
    place_ref,
    normed_ref,
    taps_ref,
    own_ref,
    other_ref,
    raw_ref,
    sums_ref,
    weight_ref,
    done,
    glu_ref,
    shifted_ref,
):
    _, rows, _ = normed_ref.shape
    count, width = raw_ref.shape
    arrived(natural_order(place_ref, own_ref, other_ref, weight_ref, done, first_lane=width))
    both = projected(normed_ref, weight_ref, slice(0, rows))
    value = both[:, :width].astype(BF16).astype(F32)
    gate = both[:, width:].astype(BF16).astype(F32)
    glu_ref[:rows] = (value * jax.nn.sigmoid(gate)).astype(BF16).astype(F32)
    glu_ref[rows:] = jnp.zeros((glu_ref.shape[0] - rows, width), F32)
    taps = taps_ref.shape[0]
    sublanes = 8
    for k in range(sublanes):
        shifted_ref[k] = glu_ref[k : k + rows]
    first = HALO - (taps - 1)
    step = 64

    def some_rows(n, _):
        at = pl.multiple_of(n * step, step)
        total = jnp.zeros((step, width), F32)
        for k in range(taps):
            shift, whole = (first + k) % sublanes, (first + k) // sublanes * sublanes
            total = total + taps_ref[k : k + 1] * shifted_ref[shift, pl.ds(at + whole, step)]
        raw_ref[pl.ds(at, step)] = total
        return 0

    lax.fori_loop(0, count // step, some_rows, 0)
    raw = raw_ref[...]
    ones = jnp.ones((8, width), F32)

    def across(value):
        return lax.dot_general(
            ones, value, (((1,), (1,)), ((), ())), precision=EXACT, preferred_element_type=F32
        )[:1]

    sums_ref[0:1] = across(raw)
    sums_ref[1:2] = across(raw * raw)


def squared(re, im):
    return re * re - im * im, 2.0 * re * im


def times(a, b):
    return a[0] * b[0] - a[1] * b[1], a[0] * b[1] + a[1] * b[0]


def exact_dot(a, b):
    return jnp.dot(a, b, preferred_element_type=F32, precision=EXACT)


def spread_over(groups, each):
    row = lax.broadcasted_iota(jnp.int32, (groups, groups * each), 0)
    col = lax.broadcasted_iota(jnp.int32, (groups, groups * each), 1) // each
    return (row == col).astype(F32)


def write_diagonal(out_ref, at, blocks, groups):
    rows, cols = blocks.shape
    pair = jnp.concatenate([blocks, blocks], axis=1)
    row_group = lax.broadcasted_iota(jnp.int32, pair.shape, 0) // (rows // groups)
    col_group = lax.broadcasted_iota(jnp.int32, pair.shape, 1) // cols
    for k in range(groups // 2):
        mine = row_group == col_group + 2 * k
        out_ref[:, at + 2 * k * cols : at + 2 * (k + 1) * cols] = jnp.where(mine, pair, 0.0).astype(BF16)


def table_kernel(*refs):
    inputs, hbm, vmem, done = refs[:10], refs[10:18], refs[18:26], refs[26]

    def send(*which):
        for k in which:
            pltpu.make_async_copy(vmem[k], hbm[k], done.at[k]).start()

    fill_tables(send, *inputs, *vmem)
    for k in range(len(vmem)):
        pltpu.make_async_copy(vmem[k], hbm[k], done.at[k]).wait()


def fill_tables(
    send,
    shift_ref,
    base_ref,
    cos_ref,
    sin_ref,
    start_cos_ref,
    start_sin_ref,
    b_re_ref,
    b_im_ref,
    c_re_ref,
    c_im_ref,
    grow_ref,
    shrink_ref,
    into_ref,
    out_ref,
    hop_re_ref,
    hop_im_ref,
    power_ref,
    total_ref,
):
    groups, count = shift_ref.shape
    lanes = base_ref.shape[1]
    width = grow_ref.shape[1]
    chunks = count // CHUNK
    base = base_ref[...]
    row = lax.broadcasted_iota(jnp.int32, (count, count), 0)
    col = lax.broadcasted_iota(jnp.int32, (count, count), 1)
    earlier = row >= col
    inside = earlier & (row // CHUNK == col // CHUNK)

    def run(which):
        return lax.dot_general(
            which.astype(F32),
            shift_ref[...],
            (((1,), (1,)), ((), ())),
            precision=EXACT,
            preferred_element_type=F32,
        )

    partial, whole = run(inside), run(earlier)
    narrow = exact_dot(partial, spread_over(groups, width // groups))
    grow_ref[...] = jnp.exp(narrow)
    shrink_ref[...] = jnp.exp(-narrow)
    spread = spread_over(groups, lanes // groups)
    wide = exact_dot(whole, spread)
    send(0, 1)
    same = lax.broadcasted_iota(jnp.int32, (groups, 128), 0)
    same = same == lax.broadcasted_iota(jnp.int32, (groups, 128), 1)
    total_ref[...] = exact_dot(whole[count - 8 :], same.astype(F32))[7:]
    sums = jnp.concatenate([partial[(c + 1) * CHUNK - 1 : (c + 1) * CHUNK] for c in range(chunks)])
    near = exact_dot(sums, spread)
    index = lax.broadcasted_iota(jnp.int32, (chunks, lanes), 0)
    size = jnp.exp(CHUNK * base + near)
    turn = (start_cos_ref[1:2], start_sin_ref[1:2])
    hop_re_ref[0], hop_im_ref[0] = size * turn[0], size * turn[1]
    distance, level = 1, 1
    while distance < chunks:
        size = jnp.where(index >= distance, jnp.exp(distance * CHUNK * base + near), 0.0)
        turn = (start_cos_ref[distance : distance + 1], start_sin_ref[distance : distance + 1])
        hop_re_ref[level], hop_im_ref[level] = size * turn[0], size * turn[1]
        near = near + jnp.where(index >= distance, pltpu.roll(near, distance, 0), 0.0)
        distance, level = distance * 2, level + 1
    send(4, 5, 7)
    counts = lax.broadcasted_iota(jnp.int32, (CHUNK, 1), 0).astype(F32)
    inner = (cos_ref[...], sin_ref[...])
    for c in range(chunks):
        at = slice(c * CHUNK, (c + 1) * CHUNK)
        size = jnp.exp((counts + (c * CHUNK + 1)) * base + wide[at])
        turn = times((start_cos_ref[c : c + 1], start_sin_ref[c : c + 1]), inner)
        power_ref[at, :lanes] = (size * turn[0]).astype(BF16)
        power_ref[at, lanes:] = (size * turn[1]).astype(BF16)
    send(6)
    write_diagonal(into_ref, 0, b_re_ref[...], groups)
    write_diagonal(into_ref, lanes, b_im_ref[...], groups)
    send(2)
    write_diagonal(out_ref, 0, c_re_ref[...], groups)
    write_diagonal(out_ref, lanes, -c_im_ref[...], groups)
    send(3)


def scan_kernel(
    u_ref,
    grow_ref,
    shrink_ref,
    in_ref,
    out_mat_ref,
    fwd_re_ref,
    fwd_im_ref,
    inv_re_ref,
    inv_im_ref,
    hop_re_ref,
    hop_im_ref,
    lower_ref,
    skip_ref,
    shift_ref,
    y_ref,
    last_ref,
    cum_re_ref,
    cum_im_ref,
    end_re_ref,
    end_im_ref,
):
    count, _ = u_ref.shape
    states = fwd_re_ref.shape[1]
    chunks = count // CHUNK
    block = lower_ref.shape[0]
    slab = 256
    u = u_ref[...].astype(F32)
    scaled = (u * shrink_ref[...]).astype(BF16)

    def chunked(value):
        return value.reshape(chunks, CHUNK, slab)

    def summed(value):
        value = value.reshape(count, slab).astype(BF16)
        return jnp.concatenate(
            [
                jnp.dot(lower_ref[...], value[k : k + block], preferred_element_type=F32)
                for k in range(0, count, block)
            ]
        )

    def first_pass(j, _):
        at = pl.ds(pl.multiple_of(j * slab, slab), slab)
        at_im = pl.ds(pl.multiple_of(states + j * slab, slab), slab)
        d_re = chunked(jnp.dot(scaled, in_ref[:, at], preferred_element_type=F32))
        d_im = chunked(jnp.dot(scaled, in_ref[:, at_im], preferred_element_type=F32))
        i_re, i_im = inv_re_ref[:, at][None], inv_im_ref[:, at][None]
        cum_re = summed(i_re * d_re - i_im * d_im)
        cum_im = summed(i_re * d_im + i_im * d_re)
        cum_re_ref[:, at] = cum_re
        cum_im_ref[:, at] = cum_im
        end_re_ref[:, at] = chunked(cum_re)[:, CHUNK - 1]
        end_im_ref[:, at] = chunked(cum_im)[:, CHUNK - 1]
        return 0

    lax.fori_loop(0, states // slab, first_pass, 0)

    h_re, h_im = hop_re_ref[0], hop_im_ref[0]
    t_re, t_im = end_re_ref[...], end_im_ref[...]
    s_re = h_re * t_re - h_im * t_im
    s_im = h_re * t_im + h_im * t_re
    for level in range(1, hop_re_ref.shape[0]):
        h_re, h_im = hop_re_ref[level], hop_im_ref[level]
        p_re, p_im = pltpu.roll(s_re, 1 << (level - 1), 0), pltpu.roll(s_im, 1 << (level - 1), 0)
        s_re, s_im = s_re + h_re * p_re - h_im * p_im, s_im + h_re * p_im + h_im * p_re
    last_ref[:, :states] = s_re[chunks - 1 :]
    last_ref[:, states : 2 * states] = s_im[chunks - 1 :]
    last_ref[:, 2 * states :] = shift_ref[...]
    begins = lax.broadcasted_iota(jnp.int32, s_re.shape, 0) > 0
    end_re_ref[...] = jnp.where(begins, pltpu.roll(s_re, 1, 0), 0.0)
    end_im_ref[...] = jnp.where(begins, pltpu.roll(s_im, 1, 0), 0.0)
    y_ref[...] = jnp.zeros(y_ref.shape, F32)

    def second_pass(j, _):
        at = pl.ds(pl.multiple_of(j * slab, slab), slab)
        at_im = pl.ds(pl.multiple_of(states + j * slab, slab), slab)
        t_re = chunked(cum_re_ref[:, at]) + end_re_ref[:, at][:, None]
        t_im = chunked(cum_im_ref[:, at]) + end_im_ref[:, at][:, None]
        f_re, f_im = fwd_re_ref[:, at][None], fwd_im_ref[:, at][None]
        x_re = (f_re * t_re - f_im * t_im).reshape(count, slab).astype(BF16)
        x_im = (f_re * t_im + f_im * t_re).reshape(count, slab).astype(BF16)
        y_ref[...] += dot_rows(x_re, out_mat_ref[:, at]) + dot_rows(x_im, out_mat_ref[:, at_im])
        return 0

    lax.fori_loop(0, states // slab, second_pass, 0)
    y_ref[...] = y_ref[...] * grow_ref[...] + skip_ref[...] * u


def shares(rows_ref, rates_ref, count):
    peers, lanes = rows_ref.shape[0], rates_ref.shape[1]
    shifts = jnp.concatenate([rows_ref[k][:, 2 * lanes :] for k in range(peers)])
    groups = lanes // 64
    sizes = jnp.exp(
        count * rates_ref[0:1] + exact_dot(shifts[:, :groups], spread_over(groups, lanes // groups))
    )
    states = [(rows_ref[k][:, :lanes], rows_ref[k][:, lanes : 2 * lanes]) for k in range(peers)]
    return shifts, sizes, states


def near_kernel(count, place_ref, near_ref, rates_ref, packed_ref, prefix_ref):
    peers, lanes = near_ref.shape[0], rates_ref.shape[1]
    place = place_ref[1] * 2 + place_ref[0]
    shifts, sizes, states = shares(near_ref, rates_ref, count)
    turn = (rates_ref[1:2], rates_ref[2:3])
    zero = jnp.zeros((1, lanes), F32)
    run = before = (zero, zero)
    decay = (zero + 1.0, zero)
    for k in range(peers):
        step = (sizes[k : k + 1] * turn[0], sizes[k : k + 1] * turn[1])
        passed = k < place
        decay = tuple(jnp.where(passed, n, o) for n, o in zip(times(step, decay), decay))
        run = tuple(m + s for m, s in zip(times(step, run), states[k]))
        before = tuple(jnp.where(passed, n, o) for n, o in zip(run, before))
    packed_ref[:, :lanes], packed_ref[:, lanes : 2 * lanes] = run
    packed_ref[:, 2 * lanes :] = jnp.sum(shifts, axis=0, keepdims=True)
    for k, row in enumerate((*before, *decay)):
        prefix_ref[k : k + 1] = row


def channel_norm(raw, first, second, gain):
    row = lax.broadcasted_iota(jnp.int32, (raw.shape[0], raw.shape[0]), 0)
    same = row == lax.broadcasted_iota(jnp.int32, row.shape, 1)

    def upright(line):
        return jnp.sum(jnp.where(same, line, 0.0), axis=1, keepdims=True)

    middle = upright(first) / CONV_W
    spread = upright(second) / CONV_W - middle * middle
    scaled = (raw - middle) * lax.rsqrt(spread + EPS) * gain
    return jax.nn.silu(scaled).astype(BF16)


def merge_rows(distances, carried, place_ref, channel, refs):
    gain_ref, sums_ref = channel
    raw_all, y_all, power_all, read_all, own_ref, other_ref, out_ref = refs[:7]
    weight_ref, weight_done, raw_ref, y_ref, power_ref, read_ref, done = refs[7:]
    block = out_ref.shape[1]
    parts = sums_ref.shape[1] // block
    sums = sums_ref[...]
    places = [
        pl.ds(pl.multiple_of(lax.rem(place_ref[2] + distance, parts) * block, block), block)
        for distance in distances
    ]
    begun = [fetch(read_all, read_ref, done.at[0])]
    for k, rows in enumerate(places):
        begun.append(fetch(power_all.at[rows], power_ref.at[k], done.at[1 + 3 * k]))
        begun.append(fetch(y_all.at[rows], y_ref.at[k], done.at[2 + 3 * k]))
        begun.append(fetch(raw_all.at[rows], raw_ref.at[k], done.at[3 + 3 * k]))
    weights_begun = natural_order(
        place_ref, own_ref, other_ref, weight_ref, weight_done, from_own_x=True
    )
    h_re, h_im = carried()
    lanes = h_re.shape[1]
    arrived(begun)
    c_re, c_im = read_ref[:, :lanes].astype(F32), read_ref[:, lanes:].astype(F32)
    blend_re = (c_re * h_re + c_im * h_im).astype(BF16)
    blend_im = (c_im * h_re - c_re * h_im).astype(BF16)
    arrived(weights_begun)
    weights = weight_ref[...].reshape(out_ref.shape[2], -1)
    for k, distance in enumerate(distances):
        mine = lax.rem(place_ref[2] + distance, parts)
        first, second = jnp.zeros((1, block), F32), jnp.zeros((1, block), F32)
        for part in range(parts):
            lines = sums[:, part * block : (part + 1) * block]
            first = jnp.where(mine == part, lines[0:1], first)
            second = jnp.where(mine == part, lines[1:2], second)
        conv = channel_norm(raw_ref[k], first, second, gain_ref[...])
        total = (
            y_ref[k]
            + dot_rows(power_ref[k, :, :lanes], blend_re)
            + dot_rows(power_ref[k, :, lanes:], blend_im)
        )
        ssm = jax.nn.gelu(total).astype(BF16)
        both = jnp.concatenate([ssm, conv], axis=1)
        out_ref[k] = dot_rows(both, weights).astype(BF16)


def opposite_kernel(count, place_ref, *refs):
    channel, (far_ref, rates_ref, prefix_ref, start_ref) = refs[:2], refs[2:6]
    *inputs, out_ref, h_ref, weight_ref, weight_done, raw_ref, y_ref, power_ref, read_ref, done = refs[6:]
    peers_z, peers_near = far_ref.shape[0], 2 * inputs[-1].shape[0]

    def carried():
        _, sizes, states = shares(far_ref, rates_ref, peers_near * count)
        turn = (rates_ref[1:2], rates_ref[2:3])
        for _ in range(peers_near.bit_length() - 1):
            turn = squared(*turn)
        h = (start_ref[0:1], start_ref[1:2])
        for k in range(peers_z):
            passed = k < place_ref[3]
            step = (sizes[k : k + 1] * turn[0], sizes[k : k + 1] * turn[1])
            moved = times(step, h)
            h = tuple(jnp.where(passed, m + s, o) for m, s, o in zip(moved, states[k], h))
        moved = times((prefix_ref[2:3], prefix_ref[3:4]), h)
        h = (moved[0] + prefix_ref[0:1], moved[1] + prefix_ref[1:2])
        h_ref[0:1], h_ref[1:2] = h
        return h

    merge_rows(
        (2,),
        carried,
        place_ref,
        channel,
        (*inputs, out_ref, weight_ref, weight_done, raw_ref, y_ref, power_ref, read_ref, done),
    )


def rest_kernel(place_ref, *refs):
    channel, h_ref = refs[:2], refs[2]
    merge_rows((0, 1, 3), lambda: (h_ref[0:1], h_ref[1:2]), place_ref, channel, refs[3:])


def input_matrix(eigen_real, eigen_imag, step, state_input):
    base = eigen_real * step[:, None]
    theta = eigen_imag * step[:, None]
    magnitude = jnp.exp(base)
    near_re = magnitude * jnp.cos(theta) - 1.0
    near_im = magnitude * jnp.sin(theta)
    modulus = eigen_real * eigen_real + eigen_imag * eigen_imag
    ratio_re = (near_re * eigen_real + near_im * eigen_imag) / modulus
    ratio_im = (near_im * eigen_real - near_re * eigen_imag) / modulus
    in_re, in_im = state_input[0], state_input[1]
    return (
        ratio_re[:, None, :] * in_re - ratio_im[:, None, :] * in_im,
        ratio_re[:, None, :] * in_im + ratio_im[:, None, :] * in_re,
    )


def tables(eigen_real, eigen_imag, log_step, decay_shift, state_input, readout, width):
    groups, states = eigen_real.shape
    lanes = groups * states
    count = decay_shift.shape[1]
    chunks = count // CHUNK
    step = jnp.exp(log_step)
    base = (eigen_real * step[:, None]).reshape(1, lanes)
    theta = (eigen_imag * step[:, None]).reshape(1, lanes)
    inside = jnp.arange(1, CHUNK + 1, dtype=F32)[:, None]
    level, angle = inside * base, inside * theta
    cosine, sine = jnp.cos(angle), jnp.sin(angle)
    grow, shrink = jnp.exp(level), jnp.exp(-level)
    forward = (grow * cosine, grow * sine)
    inverse = (shrink * cosine, -shrink * sine)
    starts = jnp.arange(chunks).astype(F32)[:, None] * CHUNK * theta
    start_cos, start_sin = jnp.cos(starts), jnp.sin(starts)
    whole_turn = (start_cos[chunks // 2], start_sin[chunks // 2])
    b_re, b_im = input_matrix(eigen_real, eigen_imag, step, state_input)
    rows = (groups * state_input.shape[2], states)
    levels = 1 + (chunks - 1).bit_length()
    block = min(count, 256)
    at = jnp.arange(block)
    lower_block = (
        (at[:, None] >= at[None, :]) & (at[:, None] // CHUNK == at[None, :] // CHUNK)
    ).astype(BF16)
    outs = (
        pltpu.HBM((count, width), F32),
        pltpu.HBM((count, width), F32),
        pltpu.HBM((width, 2 * lanes), BF16),
        pltpu.HBM((width, 2 * lanes), BF16),
        pltpu.HBM((levels, chunks, lanes), F32),
        pltpu.HBM((levels, chunks, lanes), F32),
        pltpu.HBM((count, 2 * lanes), BF16),
        pltpu.HBM((1, 128), F32),
    )
    grow, shrink, into, out, hop_re, hop_im, power, total = call(
        table_kernel,
        outs,
        (
            decay_shift,
            base,
            cosine,
            sine,
            start_cos,
            start_sin,
            b_re.reshape(rows),
            b_im.reshape(rows),
            readout[0].reshape(rows),
            readout[1].reshape(rows),
        ),
        scratch=[pltpu.VMEM(o.shape, o.dtype) for o in outs] + [pltpu.SemaphoreType.DMA((len(outs),))],
        mib=24,
        space=pltpu.HBM,
        flops=20 * count * count * groups,
        bytes_accessed=8 * count * lanes,
        transcendentals=count * lanes,
    )
    turn = squared(*(r.reshape(1, -1) for r in whole_turn))
    device = dict(rates=jnp.concatenate([base, *turn]), shift=total)
    scan = (grow, shrink, into, out, *forward, *inverse, hop_re, hop_im, lower_block)
    return scan, power, out, device


def mixer(
    tokens,
    norm_gain,
    proj_state,
    proj_value,
    proj_gate,
    eigen_real,
    eigen_imag,
    log_step,
    decay_shift,
    state_input,
    readout,
    skip_gain,
    init_state,
    conv_taps,
    channel_gain,
    merge_state,
    merge_conv,
):
    place = jnp.stack([lax.axis_index(axis) for axis in ("c", "x", "tp", "z")]).astype(jnp.int32)
    parts = lax.axis_size("tp")
    count, depth_part = tokens.shape
    depth = depth_part * parts
    rows = count + HALO
    half = rows // 2
    width = proj_state.shape[1]
    merged = jnp.concatenate([merge_state, merge_conv]).T
    planes = copies(
        jnp.concatenate([proj_state, proj_value, proj_gate, merged], axis=1), "z"
    )
    extended = jnp.concatenate([next_along(tokens[count - HALO :], SP), tokens])
    ahead = from_ahead(extended, "tp", 1)
    behind = from_ahead(extended, "tp", -1)
    top = from_ahead(ahead[:half], "tp", 1)
    bottom = from_ahead(behind[half:], "tp", -1)
    scan_tables, power, reads, device = tables(
        eigen_real, eigen_imag, log_step, decay_shift, state_input, readout, width
    )
    planes, total, rates, start = lax.optimization_barrier(
        (planes, device["shift"], device["rates"], init_state.reshape(2, -1))
    )
    device = dict(shift=total, rates=rates)
    project_x = copies(planes[:, :, : 3 * width], "x")
    normed = call(
        norm_kernel,
        jax.ShapeDtypeStruct((parts, rows, depth_part), BF16),
        (*far_from_core(extended, ahead, top, bottom, behind), norm_gain.reshape(parts, 1, depth_part)),
        scalars=(place,),
        mib=12,
        flops=8 * count * depth,
        bytes_accessed=4 * count * depth,
        transcendentals=count,
    )
    merge_planes, normed = lax.optimization_barrier((planes[:, :, 3 * width :], normed))
    merge_ahead = from_ahead(merge_planes, "x", 1)
    merge_behind = from_ahead(merge_planes, "x", -1)
    merge_across = from_ahead(merge_planes, "x", 2)
    merge_pieces = (merge_planes, merge_ahead, merge_across, merge_behind)
    project_other = partner(project_x)
    u_in = call(
        state_in_kernel,
        jax.ShapeDtypeStruct((count, width), BF16),
        (normed,),
        apart=far_from_core(project_x, project_other),
        scalars=(place,),
        scratch=weight_scratch(project_x, width),
        mib=12,
        flops=2 * count * depth * width,
        bytes_accessed=4 * depth * count,
        transcendentals=0,
    )
    lanes = eigen_real.size
    chunks = count // CHUNK
    y_local, last = call(
        scan_kernel,
        (
            pltpu.HBM((count, width), F32),
            jax.ShapeDtypeStruct((1, 2 * lanes + 128), F32),
        ),
        (u_in, *scan_tables, skip_gain.reshape(1, -1), device["shift"]),
        scratch=(
            pltpu.VMEM((count, lanes), F32),
            pltpu.VMEM((count, lanes), F32),
            pltpu.VMEM((chunks, lanes), F32),
            pltpu.VMEM((chunks, lanes), F32),
        ),
        mib=24,
        flops=12 * count * width * lanes,
        bytes_accessed=8 * count * lanes,
        transcendentals=0,
    )
    near = copies(last, ("x", "c"))
    packed, prefix = call(
        functools.partial(near_kernel, count),
        (
            jax.ShapeDtypeStruct((1, 2 * lanes + 128), F32),
            jax.ShapeDtypeStruct((4, lanes), F32),
        ),
        (near, device["rates"]),
        scalars=(place,),
        mib=4,
        flops=100 * lanes,
        bytes_accessed=64 * lanes,
        transcendentals=8 * lanes,
    )
    *merge_pieces, _ = lax.optimization_barrier((*merge_pieces, packed))
    merge_x = jnp.stack(merge_pieces)
    merge_other = partner(merge_x)
    far = copies(packed, "z")

    raw, sums = call(
        conv_kernel,
        (
            pltpu.HBM((count, width), F32),
            jax.ShapeDtypeStruct((2, count), F32),
        ),
        (normed, conv_taps),
        apart=far_from_core(project_x, project_other),
        scalars=(place,),
        scratch=(
            *weight_scratch(project_x, 2 * width),
            pltpu.VMEM((rows + 8, width), F32),
            pltpu.VMEM((8, rows, width), F32),
        ),
        mib=20,
        flops=4 * count * depth * width,
        bytes_accessed=4 * depth * count,
        transcendentals=0,
    )
    sums = lax.psum(sums, "tp")

    block = count // parts

    def products(kernel, blocks, more, arrays):
        return call(
            kernel,
            (jax.ShapeDtypeStruct((blocks, block, depth), BF16), *more),
            (channel_gain.reshape(1, -1), sums, *arrays),
            apart=(*far_from_core(raw, y_local, power, reads), merge_x, merge_other),
            scalars=(place,),
            scratch=(
                *weight_scratch(merge_x, 2 * width),
                pltpu.VMEM((blocks, block, width), F32),
                pltpu.VMEM((blocks, block, width), F32),
                pltpu.VMEM((blocks, block, 2 * lanes), BF16),
                pltpu.VMEM((width, 2 * lanes), BF16),
                pltpu.SemaphoreType.DMA((1 + 3 * blocks,)),
            ),
            flops=4 * block * blocks * depth * width,
            bytes_accessed=4 * depth * count,
            transcendentals=0,
        )

    opposite, h = products(
        functools.partial(opposite_kernel, count),
        1,
        (jax.ShapeDtypeStruct((2, lanes), F32),),
        (far, device["rates"], prefix, start),
    )
    opposite = opposite[0]
    through_ahead = from_ahead(opposite[: block // 2], "tp", 1)
    through_behind = from_ahead(opposite[block // 2 :], "tp", -1)
    ((mine, to_ahead, to_behind),) = products(rest_kernel, 3, (), (h,))
    empty = jnp.zeros((block // 2, depth), F32)
    to_behind = to_behind.astype(F32) + jnp.concatenate([through_ahead.astype(F32), empty])
    to_ahead = to_ahead.astype(F32) + jnp.concatenate([empty, through_behind.astype(F32)])
    from_next = from_ahead(to_behind.astype(BF16), "tp", 1)
    from_last = from_ahead(to_ahead.astype(BF16), "tp", -1)
    return (mine.astype(F32) + from_next.astype(F32) + from_last.astype(F32)).astype(BF16)


def finer_mesh(mesh):
    cores = 2
    return Mesh(mesh.devices.reshape(16, 4, cores, mesh.shape["tp"]), SP_TP)


def solution(mesh):
    return jax.shard_map(
        mixer,
        mesh=finer_mesh(mesh),
        in_specs=(
            P(SP, "tp"),
            P(),
            P(SP, "tp"),
            P(SP, "tp"),
            P(SP, "tp"),
            P("tp", None),
            P("tp", None),
            P("tp"),
            P("tp", SP),
            P(None, "tp", None, None),
            P(None, "tp", None, None),
            P("tp"),
            P(None, "tp", None),
            P(None, "tp"),
            P("tp"),
            P("tp", SP),
            P("tp", SP),
        ),
        out_specs=P(SP_TP, None),
        check_vma=False,
    )
```

```python
import functools

import jax
import jax.numpy as jnp
from jax import lax
from jax.experimental import pallas as pl
from jax.experimental.pallas import tpu as pltpu
from jax.sharding import Mesh
from jax.sharding import PartitionSpec as P


CONV_W = 1024
SP = ("z", "x", "c")
SP_TP = ("z", "x", "c", "tp")
CHUNK = 32
HALO = 32
EPS = 1e-06
EXACT = lax.Precision.HIGHEST
F32 = jnp.float32
BF16 = jnp.bfloat16


def copies(value, axis):
    peers = lax.axis_size(axis)
    return lax.all_to_all(
        jnp.broadcast_to(value[None], (peers, *value.shape)), axis, 0, 0, tiled=True
    )


def next_along(block, axis):
    count = lax.axis_size(axis)
    return lax.ppermute(block, axis, [(i, i + 1) for i in range(count - 1)])


def partner(block):
    return lax.ppermute(block, "c", [(0, 1), (1, 0)])


def from_ahead(block, axis, distance):
    count = lax.axis_size(axis)
    return lax.ppermute(block, axis, [(i, (i - distance) % count) for i in range(count)])


def far_from_core(*arrays):
    return [pltpu.with_memory_space_constraint(array, pltpu.HBM) for array in arrays]


def whole_specs(arrays):
    return [pl.BlockSpec(memory_space=pltpu.VMEM) for _ in arrays]


def call(body, outs, arrays, apart=(), scalars=(), scratch=(), mib=16, space=pltpu.VMEM, **costs):
    return pl.pallas_call(
        body,
        compiler_params=pltpu.CompilerParams(vmem_limit_bytes=mib * 2**20),
        out_shape=outs,
        in_specs=[pl.BlockSpec(memory_space=pltpu.SMEM) for _ in scalars]
        + whole_specs(arrays)
        + [pl.BlockSpec(memory_space=pl.ANY) for _ in apart],
        out_specs=jax.tree.map(lambda _: pl.BlockSpec(memory_space=space), outs),
        scratch_shapes=list(scratch),
        cost_estimate=pl.CostEstimate(**costs) if costs else None,
    )(*scalars, *arrays, *apart)


def fetch(source, target, done):
    copy = pltpu.make_async_copy(source, target, done)
    copy.start()
    return copy


def natural_order(place_ref, own_ref, other_ref, into_ref, done, first_lane=0, from_own_x=False):
    peers_x, width = own_ref.shape[0], into_ref.shape[-1]
    begun = []
    for side, ref in enumerate((own_ref, other_ref)):
        core = lax.rem(place_ref[0] + side, 2)
        for x in range(peers_x):
            at = lax.rem(x - place_ref[1] + peers_x, peers_x) if from_own_x else x
            source = ref.at[at, :, :, pl.ds(first_lane, width)]
            begun.append(fetch(source, into_ref.at[:, x, core], done.at[side * peers_x + x]))
    return begun


def arrived(copies_begun):
    for copy in copies_begun:
        copy.wait()


def weight_scratch(merged, width):
    peers_x, peers_z, rows, _ = merged.shape
    return [
        pltpu.VMEM((peers_z, peers_x, 2, rows, width), BF16),
        pltpu.SemaphoreType.DMA((2 * peers_x,)),
    ]


def dot_rows(a, b):
    return lax.dot_general(a, b, (((1,), (1,)), ((), ())), preferred_element_type=F32)


def norm_kernel(place_ref, own_ref, ahead_ref, top_ref, bottom_ref, behind_ref, gain_ref, out_ref):
    parts, count, depth = out_ref.shape
    half = count // 2
    part = place_ref[2]

    def rows_of(at, opposite_ref):
        rows = pl.ds(at, half)
        blocks = [
            block.astype(F32)
            for block in (own_ref[rows], ahead_ref[rows], opposite_ref[...], behind_ref[rows])
        ]
        power = sum(jnp.sum(block * block, axis=1, keepdims=True) for block in blocks)
        scale = lax.rsqrt(power / (parts * depth) + EPS)
        for p, block in enumerate(blocks):
            gain = gain_ref[lax.rem(part + p, parts)]
            out_ref[lax.rem(part + p, parts), rows] = (block * scale * gain).astype(BF16)

    rows_of(0, top_ref)
    rows_of(half, bottom_ref)


def projected(normed_ref, weight_ref, rows):
    parts, _, depth = normed_ref.shape
    weights = weight_ref[...].reshape(parts * depth, -1)
    return sum(
        jnp.dot(
            normed_ref[p, rows],
            weights[p * depth : (p + 1) * depth],
            preferred_element_type=F32,
        )
        for p in range(parts)
    )


def state_in_kernel(
    place_ref, normed_all, own_ref, other_ref, out_ref, weight_ref, done, normed_ref, normed_done
):
    rows = normed_ref.shape[1]
    whole = fetch(normed_all, normed_ref, normed_done.at[0])
    arrived([*natural_order(place_ref, own_ref, other_ref, weight_ref, done), whole])
    out_ref[...] = projected(normed_ref, weight_ref, slice(HALO, rows)).astype(BF16)


def conv_kernel(
    place_ref,
    taps_ref,
    normed_all,
    own_ref,
    other_ref,
    raw_ref,
    sums_ref,
    weight_ref,
    done,
    normed_ref,
    normed_done,
    glu_ref,
    shifted_ref,
):
    _, rows, _ = normed_ref.shape
    count, width = raw_ref.shape
    whole = fetch(normed_all, normed_ref, normed_done.at[0])
    weights_begun = natural_order(place_ref, own_ref, other_ref, weight_ref, done, first_lane=width)
    arrived([*weights_begun, whole])
    both = projected(normed_ref, weight_ref, slice(0, rows))
    value = both[:, :width].astype(BF16).astype(F32)
    gate = both[:, width:].astype(BF16).astype(F32)
    glu_ref[:rows] = (value * jax.nn.sigmoid(gate)).astype(BF16).astype(F32)
    glu_ref[rows:] = jnp.zeros((glu_ref.shape[0] - rows, width), F32)
    taps = taps_ref.shape[0]
    sublanes = 8
    for k in range(sublanes):
        shifted_ref[k] = glu_ref[k : k + rows]
    first = HALO - (taps - 1)
    step = 64

    def some_rows(n, _):
        at = pl.multiple_of(n * step, step)
        total = jnp.zeros((step, width), F32)
        for k in range(taps):
            shift, whole = (first + k) % sublanes, (first + k) // sublanes * sublanes
            total = total + taps_ref[k : k + 1] * shifted_ref[shift, pl.ds(at + whole, step)]
        raw_ref[pl.ds(at, step)] = total
        return 0

    lax.fori_loop(0, count // step, some_rows, 0)
    raw = raw_ref[...]
    ones = jnp.ones((8, width), F32)

    def across(value):
        return lax.dot_general(
            ones, value, (((1,), (1,)), ((), ())), precision=EXACT, preferred_element_type=F32
        )[:1]

    sums_ref[0:1] = across(raw)
    sums_ref[1:2] = across(raw * raw)


def squared(re, im):
    return re * re - im * im, 2.0 * re * im


def times(a, b):
    return a[0] * b[0] - a[1] * b[1], a[0] * b[1] + a[1] * b[0]


def exact_dot(a, b):
    return jnp.dot(a, b, preferred_element_type=F32, precision=EXACT)


def spread_over(groups, each):
    row = lax.broadcasted_iota(jnp.int32, (groups, groups * each), 0)
    col = lax.broadcasted_iota(jnp.int32, (groups, groups * each), 1) // each
    return (row == col).astype(F32)


def write_diagonal(out_ref, at, blocks, groups):
    rows, cols = blocks.shape
    pair = jnp.concatenate([blocks, blocks], axis=1)
    row_group = lax.broadcasted_iota(jnp.int32, pair.shape, 0) // (rows // groups)
    col_group = lax.broadcasted_iota(jnp.int32, pair.shape, 1) // cols
    for k in range(groups // 2):
        mine = row_group == col_group + 2 * k
        out_ref[:, at + 2 * k * cols : at + 2 * (k + 1) * cols] = jnp.where(mine, pair, 0.0).astype(BF16)


def table_kernel(*refs):
    inputs, hbm, vmem, done = refs[:10], refs[10:18], refs[18:26], refs[26]

    def send(*which):
        for k in which:
            pltpu.make_async_copy(vmem[k], hbm[k], done.at[k]).start()

    fill_tables(send, *inputs, *vmem)
    for k in range(len(vmem)):
        pltpu.make_async_copy(vmem[k], hbm[k], done.at[k]).wait()


def fill_tables(
    send,
    shift_ref,
    base_ref,
    cos_ref,
    sin_ref,
    start_cos_ref,
    start_sin_ref,
    b_re_ref,
    b_im_ref,
    c_re_ref,
    c_im_ref,
    grow_ref,
    shrink_ref,
    into_ref,
    out_ref,
    hop_re_ref,
    hop_im_ref,
    power_ref,
    total_ref,
):
    groups, count = shift_ref.shape
    lanes = base_ref.shape[1]
    width = grow_ref.shape[1]
    chunks = count // CHUNK
    base = base_ref[...]
    row = lax.broadcasted_iota(jnp.int32, (count, count), 0)
    col = lax.broadcasted_iota(jnp.int32, (count, count), 1)
    earlier = row >= col
    inside = earlier & (row // CHUNK == col // CHUNK)

    def run(which):
        return lax.dot_general(
            which.astype(F32),
            shift_ref[...],
            (((1,), (1,)), ((), ())),
            precision=EXACT,
            preferred_element_type=F32,
        )

    partial, whole = run(inside), run(earlier)
    narrow = exact_dot(partial, spread_over(groups, width // groups))
    grow_ref[...] = jnp.exp(narrow)
    shrink_ref[...] = jnp.exp(-narrow)
    spread = spread_over(groups, lanes // groups)
    wide = exact_dot(whole, spread)
    send(0, 1)
    same = lax.broadcasted_iota(jnp.int32, (groups, 128), 0)
    same = same == lax.broadcasted_iota(jnp.int32, (groups, 128), 1)
    total_ref[...] = exact_dot(whole[count - 8 :], same.astype(F32))[7:]
    sums = jnp.concatenate([partial[(c + 1) * CHUNK - 1 : (c + 1) * CHUNK] for c in range(chunks)])
    near = exact_dot(sums, spread)
    index = lax.broadcasted_iota(jnp.int32, (chunks, lanes), 0)
    size = jnp.exp(CHUNK * base + near)
    turn = (start_cos_ref[1:2], start_sin_ref[1:2])
    hop_re_ref[0], hop_im_ref[0] = size * turn[0], size * turn[1]
    distance, level = 1, 1
    while distance < chunks:
        size = jnp.where(index >= distance, jnp.exp(distance * CHUNK * base + near), 0.0)
        turn = (start_cos_ref[distance : distance + 1], start_sin_ref[distance : distance + 1])
        hop_re_ref[level], hop_im_ref[level] = size * turn[0], size * turn[1]
        near = near + jnp.where(index >= distance, pltpu.roll(near, distance, 0), 0.0)
        distance, level = distance * 2, level + 1
    send(4, 5, 7)
    counts = lax.broadcasted_iota(jnp.int32, (CHUNK, 1), 0).astype(F32)
    inner = (cos_ref[...], sin_ref[...])
    for c in range(chunks):
        at = slice(c * CHUNK, (c + 1) * CHUNK)
        size = jnp.exp((counts + (c * CHUNK + 1)) * base + wide[at])
        turn = times((start_cos_ref[c : c + 1], start_sin_ref[c : c + 1]), inner)
        power_ref[at, :lanes] = (size * turn[0]).astype(BF16)
        power_ref[at, lanes:] = (size * turn[1]).astype(BF16)
    send(6)
    write_diagonal(into_ref, 0, b_re_ref[...], groups)
    write_diagonal(into_ref, lanes, b_im_ref[...], groups)
    send(2)
    write_diagonal(out_ref, 0, c_re_ref[...], groups)
    write_diagonal(out_ref, lanes, -c_im_ref[...], groups)
    send(3)


def scan_kernel(
    u_ref,
    grow_ref,
    shrink_ref,
    in_ref,
    out_mat_ref,
    fwd_re_ref,
    fwd_im_ref,
    inv_re_ref,
    inv_im_ref,
    hop_re_ref,
    hop_im_ref,
    lower_ref,
    skip_ref,
    shift_ref,
    y_ref,
    last_ref,
    cum_re_ref,
    cum_im_ref,
    end_re_ref,
    end_im_ref,
):
    count, _ = u_ref.shape
    states = fwd_re_ref.shape[1]
    chunks = count // CHUNK
    block = lower_ref.shape[0]
    slab = 256
    u = u_ref[...].astype(F32)
    scaled = (u * shrink_ref[...]).astype(BF16)

    def chunked(value):
        return value.reshape(chunks, CHUNK, slab)

    def summed(value):
        value = value.reshape(count, slab).astype(BF16)
        return jnp.concatenate(
            [
                jnp.dot(lower_ref[...], value[k : k + block], preferred_element_type=F32)
                for k in range(0, count, block)
            ]
        )

    def first_pass(j, _):
        at = pl.ds(pl.multiple_of(j * slab, slab), slab)
        at_im = pl.ds(pl.multiple_of(states + j * slab, slab), slab)
        d_re = chunked(jnp.dot(scaled, in_ref[:, at], preferred_element_type=F32))
        d_im = chunked(jnp.dot(scaled, in_ref[:, at_im], preferred_element_type=F32))
        i_re, i_im = inv_re_ref[:, at][None], inv_im_ref[:, at][None]
        cum_re = summed(i_re * d_re - i_im * d_im)
        cum_im = summed(i_re * d_im + i_im * d_re)
        cum_re_ref[:, at] = cum_re
        cum_im_ref[:, at] = cum_im
        end_re_ref[:, at] = chunked(cum_re)[:, CHUNK - 1]
        end_im_ref[:, at] = chunked(cum_im)[:, CHUNK - 1]
        return 0

    lax.fori_loop(0, states // slab, first_pass, 0)

    h_re, h_im = hop_re_ref[0], hop_im_ref[0]
    t_re, t_im = end_re_ref[...], end_im_ref[...]
    s_re = h_re * t_re - h_im * t_im
    s_im = h_re * t_im + h_im * t_re
    for level in range(1, hop_re_ref.shape[0]):
        h_re, h_im = hop_re_ref[level], hop_im_ref[level]
        p_re, p_im = pltpu.roll(s_re, 1 << (level - 1), 0), pltpu.roll(s_im, 1 << (level - 1), 0)
        s_re, s_im = s_re + h_re * p_re - h_im * p_im, s_im + h_re * p_im + h_im * p_re
    last_ref[:, :states] = s_re[chunks - 1 :]
    last_ref[:, states : 2 * states] = s_im[chunks - 1 :]
    last_ref[:, 2 * states :] = shift_ref[...]
    begins = lax.broadcasted_iota(jnp.int32, s_re.shape, 0) > 0
    end_re_ref[...] = jnp.where(begins, pltpu.roll(s_re, 1, 0), 0.0)
    end_im_ref[...] = jnp.where(begins, pltpu.roll(s_im, 1, 0), 0.0)
    y_ref[...] = jnp.zeros(y_ref.shape, F32)

    def second_pass(j, _):
        at = pl.ds(pl.multiple_of(j * slab, slab), slab)
        at_im = pl.ds(pl.multiple_of(states + j * slab, slab), slab)
        t_re = chunked(cum_re_ref[:, at]) + end_re_ref[:, at][:, None]
        t_im = chunked(cum_im_ref[:, at]) + end_im_ref[:, at][:, None]
        f_re, f_im = fwd_re_ref[:, at][None], fwd_im_ref[:, at][None]
        x_re = (f_re * t_re - f_im * t_im).reshape(count, slab).astype(BF16)
        x_im = (f_re * t_im + f_im * t_re).reshape(count, slab).astype(BF16)
        y_ref[...] += dot_rows(x_re, out_mat_ref[:, at]) + dot_rows(x_im, out_mat_ref[:, at_im])
        return 0

    lax.fori_loop(0, states // slab, second_pass, 0)
    y_ref[...] = y_ref[...] * grow_ref[...] + skip_ref[...] * u


def shares(rows_ref, rates_ref, count):
    peers, lanes = rows_ref.shape[0], rates_ref.shape[1]
    shifts = jnp.concatenate([rows_ref[k][:, 2 * lanes :] for k in range(peers)])
    groups = lanes // 64
    sizes = jnp.exp(
        count * rates_ref[0:1] + exact_dot(shifts[:, :groups], spread_over(groups, lanes // groups))
    )
    states = [(rows_ref[k][:, :lanes], rows_ref[k][:, lanes : 2 * lanes]) for k in range(peers)]
    return shifts, sizes, states


def near_kernel(count, place_ref, near_ref, rates_ref, packed_ref, prefix_ref):
    peers, lanes = near_ref.shape[0], rates_ref.shape[1]
    place = place_ref[1] * 2 + place_ref[0]
    shifts, sizes, states = shares(near_ref, rates_ref, count)
    turn = (rates_ref[1:2], rates_ref[2:3])
    zero = jnp.zeros((1, lanes), F32)
    run = before = (zero, zero)
    decay = (zero + 1.0, zero)
    for k in range(peers):
        step = (sizes[k : k + 1] * turn[0], sizes[k : k + 1] * turn[1])
        passed = k < place
        decay = tuple(jnp.where(passed, n, o) for n, o in zip(times(step, decay), decay))
        run = tuple(m + s for m, s in zip(times(step, run), states[k]))
        before = tuple(jnp.where(passed, n, o) for n, o in zip(run, before))
    packed_ref[:, :lanes], packed_ref[:, lanes : 2 * lanes] = run
    packed_ref[:, 2 * lanes :] = jnp.sum(shifts, axis=0, keepdims=True)
    for k, row in enumerate((*before, *decay)):
        prefix_ref[k : k + 1] = row


def channel_norm(raw, first, second, gain):
    row = lax.broadcasted_iota(jnp.int32, (raw.shape[0], raw.shape[0]), 0)
    same = row == lax.broadcasted_iota(jnp.int32, row.shape, 1)

    def upright(line):
        return jnp.sum(jnp.where(same, line, 0.0), axis=1, keepdims=True)

    middle = upright(first) / CONV_W
    spread = upright(second) / CONV_W - middle * middle
    scaled = (raw - middle) * lax.rsqrt(spread + EPS) * gain
    return jax.nn.silu(scaled).astype(BF16)


def merge_rows(distances, carried, place_ref, channel, refs):
    gain_ref, *sums_refs = channel
    raw_all, y_all, power_all, read_all, own_ref, other_ref, out_ref = refs[:7]
    weight_ref, weight_done, raw_ref, y_ref, power_ref, read_ref, done = refs[7:]
    block = out_ref.shape[1]
    parts = len(sums_refs)
    sums = sum((ref[...] for ref in sums_refs[1:]), sums_refs[0][...])
    places = [
        pl.ds(pl.multiple_of(lax.rem(place_ref[2] + distance, parts) * block, block), block)
        for distance in distances
    ]
    begun = [fetch(read_all, read_ref, done.at[0])]
    for k, rows in enumerate(places):
        begun.append(fetch(power_all.at[rows], power_ref.at[k], done.at[1 + 3 * k]))
        begun.append(fetch(y_all.at[rows], y_ref.at[k], done.at[2 + 3 * k]))
        begun.append(fetch(raw_all.at[rows], raw_ref.at[k], done.at[3 + 3 * k]))
    weights_begun = natural_order(
        place_ref, own_ref, other_ref, weight_ref, weight_done, from_own_x=True
    )
    h_re, h_im = carried()
    lanes = h_re.shape[1]
    arrived(begun)
    c_re, c_im = read_ref[:, :lanes].astype(F32), read_ref[:, lanes:].astype(F32)
    blend_re = (c_re * h_re + c_im * h_im).astype(BF16)
    blend_im = (c_im * h_re - c_re * h_im).astype(BF16)
    arrived(weights_begun)
    weights = weight_ref[...].reshape(out_ref.shape[2], -1)
    for k, distance in enumerate(distances):
        mine = lax.rem(place_ref[2] + distance, parts)
        first, second = jnp.zeros((1, block), F32), jnp.zeros((1, block), F32)
        for part in range(parts):
            lines = sums[:, part * block : (part + 1) * block]
            first = jnp.where(mine == part, lines[0:1], first)
            second = jnp.where(mine == part, lines[1:2], second)
        conv = channel_norm(raw_ref[k], first, second, gain_ref[...])
        total = (
            y_ref[k]
            + dot_rows(power_ref[k, :, :lanes], blend_re)
            + dot_rows(power_ref[k, :, lanes:], blend_im)
        )
        ssm = jax.nn.gelu(total).astype(BF16)
        both = jnp.concatenate([ssm, conv], axis=1)
        out_ref[k] = dot_rows(both, weights).astype(BF16)


def opposite_kernel(count, place_ref, *refs):
    channel, (far_ref, rates_ref, prefix_ref, start_ref) = refs[:5], refs[5:9]
    *inputs, out_ref, h_ref, weight_ref, weight_done, raw_ref, y_ref, power_ref, read_ref, done = refs[9:]
    peers_z, peers_near = far_ref.shape[0], 2 * inputs[-1].shape[0]

    def carried():
        _, sizes, states = shares(far_ref, rates_ref, peers_near * count)
        turn = (rates_ref[1:2], rates_ref[2:3])
        for _ in range(peers_near.bit_length() - 1):
            turn = squared(*turn)
        h = (start_ref[0:1], start_ref[1:2])
        for k in range(peers_z):
            passed = k < place_ref[3]
            step = (sizes[k : k + 1] * turn[0], sizes[k : k + 1] * turn[1])
            moved = times(step, h)
            h = tuple(jnp.where(passed, m + s, o) for m, s, o in zip(moved, states[k], h))
        moved = times((prefix_ref[2:3], prefix_ref[3:4]), h)
        h = (moved[0] + prefix_ref[0:1], moved[1] + prefix_ref[1:2])
        h_ref[0:1], h_ref[1:2] = h
        return h

    merge_rows(
        (2,),
        carried,
        place_ref,
        channel,
        (*inputs, out_ref, weight_ref, weight_done, raw_ref, y_ref, power_ref, read_ref, done),
    )


def rest_kernel(place_ref, *refs):
    channel, h_ref = refs[:5], refs[5]
    merge_rows((0, 1, 3), lambda: (h_ref[0:1], h_ref[1:2]), place_ref, channel, refs[6:])


def input_matrix(eigen_real, eigen_imag, step, state_input):
    base = eigen_real * step[:, None]
    theta = eigen_imag * step[:, None]
    magnitude = jnp.exp(base)
    near_re = magnitude * jnp.cos(theta) - 1.0
    near_im = magnitude * jnp.sin(theta)
    modulus = eigen_real * eigen_real + eigen_imag * eigen_imag
    ratio_re = (near_re * eigen_real + near_im * eigen_imag) / modulus
    ratio_im = (near_im * eigen_real - near_re * eigen_imag) / modulus
    in_re, in_im = state_input[0], state_input[1]
    return (
        ratio_re[:, None, :] * in_re - ratio_im[:, None, :] * in_im,
        ratio_re[:, None, :] * in_im + ratio_im[:, None, :] * in_re,
    )


def tables(eigen_real, eigen_imag, log_step, decay_shift, state_input, readout, width):
    groups, states = eigen_real.shape
    lanes = groups * states
    count = decay_shift.shape[1]
    chunks = count // CHUNK
    step = jnp.exp(log_step)
    base = (eigen_real * step[:, None]).reshape(1, lanes)
    theta = (eigen_imag * step[:, None]).reshape(1, lanes)
    inside = jnp.arange(1, CHUNK + 1, dtype=F32)[:, None]
    level, angle = inside * base, inside * theta
    cosine, sine = jnp.cos(angle), jnp.sin(angle)
    grow, shrink = jnp.exp(level), jnp.exp(-level)
    forward = (grow * cosine, grow * sine)
    inverse = (shrink * cosine, -shrink * sine)
    starts = jnp.arange(chunks).astype(F32)[:, None] * CHUNK * theta
    start_cos, start_sin = jnp.cos(starts), jnp.sin(starts)
    whole_turn = (start_cos[chunks // 2], start_sin[chunks // 2])
    b_re, b_im = input_matrix(eigen_real, eigen_imag, step, state_input)
    rows = (groups * state_input.shape[2], states)
    levels = 1 + (chunks - 1).bit_length()
    block = min(count, 256)
    at = jnp.arange(block)
    lower_block = (
        (at[:, None] >= at[None, :]) & (at[:, None] // CHUNK == at[None, :] // CHUNK)
    ).astype(BF16)
    outs = (
        pltpu.HBM((count, width), F32),
        pltpu.HBM((count, width), F32),
        pltpu.HBM((width, 2 * lanes), BF16),
        pltpu.HBM((width, 2 * lanes), BF16),
        pltpu.HBM((levels, chunks, lanes), F32),
        pltpu.HBM((levels, chunks, lanes), F32),
        pltpu.HBM((count, 2 * lanes), BF16),
        pltpu.HBM((1, 128), F32),
    )
    grow, shrink, into, out, hop_re, hop_im, power, total = call(
        table_kernel,
        outs,
        (
            decay_shift,
            base,
            cosine,
            sine,
            start_cos,
            start_sin,
            b_re.reshape(rows),
            b_im.reshape(rows),
            readout[0].reshape(rows),
            readout[1].reshape(rows),
        ),
        scratch=[pltpu.VMEM(o.shape, o.dtype) for o in outs] + [pltpu.SemaphoreType.DMA((len(outs),))],
        mib=24,
        space=pltpu.HBM,
        flops=20 * count * count * groups,
        bytes_accessed=8 * count * lanes,
        transcendentals=count * lanes,
    )
    turn = squared(*(r.reshape(1, -1) for r in whole_turn))
    device = dict(rates=jnp.concatenate([base, *turn]), shift=total)
    scan = (grow, shrink, into, out, *forward, *inverse, hop_re, hop_im, lower_block)
    return scan, power, out, device


def mixer(
    tokens,
    norm_gain,
    proj_state,
    proj_value,
    proj_gate,
    eigen_real,
    eigen_imag,
    log_step,
    decay_shift,
    state_input,
    readout,
    skip_gain,
    init_state,
    conv_taps,
    channel_gain,
    merge_state,
    merge_conv,
):
    place = jnp.stack([lax.axis_index(axis) for axis in ("c", "x", "tp", "z")]).astype(jnp.int32)
    parts = lax.axis_size("tp")
    count, depth_part = tokens.shape
    depth = depth_part * parts
    rows = count + HALO
    half = rows // 2
    width = proj_state.shape[1]
    merged = jnp.concatenate([merge_state, merge_conv]).T
    planes = copies(
        jnp.concatenate([proj_state, proj_value, proj_gate, merged], axis=1), "z"
    )
    extended = jnp.concatenate([next_along(tokens[count - HALO :], SP), tokens])
    ahead = from_ahead(extended, "tp", 1)
    behind = from_ahead(extended, "tp", -1)
    top = from_ahead(ahead[:half], "tp", 1)
    bottom = from_ahead(behind[half:], "tp", -1)
    scan_tables, power, reads, device = tables(
        eigen_real, eigen_imag, log_step, decay_shift, state_input, readout, width
    )
    planes, total, rates, start = lax.optimization_barrier(
        (planes, device["shift"], device["rates"], init_state.reshape(2, -1))
    )
    device = dict(shift=total, rates=rates)
    project_x = copies(planes[:, :, : 3 * width], "x")
    normed_scratch = [
        pltpu.VMEM((parts, rows, depth_part), BF16),
        pltpu.SemaphoreType.DMA((1,)),
    ]
    normed = call(
        norm_kernel,
        pltpu.HBM((parts, rows, depth_part), BF16),
        (*far_from_core(extended, ahead, top, bottom, behind), norm_gain.reshape(parts, 1, depth_part)),
        scalars=(place,),
        mib=12,
        flops=8 * count * depth,
        bytes_accessed=4 * count * depth,
        transcendentals=count,
    )
    merge_planes, normed = lax.optimization_barrier((planes[:, :, 3 * width :], normed))
    merge_ahead = from_ahead(merge_planes, "x", 1)
    merge_behind = from_ahead(merge_planes, "x", -1)
    merge_across = from_ahead(merge_planes, "x", 2)
    merge_pieces = (merge_planes, merge_ahead, merge_across, merge_behind)
    project_other = partner(project_x)
    u_in = call(
        state_in_kernel,
        jax.ShapeDtypeStruct((count, width), BF16),
        (),
        apart=far_from_core(normed, project_x, project_other),
        scalars=(place,),
        scratch=(*weight_scratch(project_x, width), *normed_scratch),
        mib=12,
        flops=2 * count * depth * width,
        bytes_accessed=4 * depth * count,
        transcendentals=0,
    )
    lanes = eigen_real.size
    chunks = count // CHUNK
    y_local, last = call(
        scan_kernel,
        (
            pltpu.HBM((count, width), F32),
            jax.ShapeDtypeStruct((1, 2 * lanes + 128), F32),
        ),
        (u_in, *scan_tables, skip_gain.reshape(1, -1), device["shift"]),
        scratch=(
            pltpu.VMEM((count, lanes), F32),
            pltpu.VMEM((count, lanes), F32),
            pltpu.VMEM((chunks, lanes), F32),
            pltpu.VMEM((chunks, lanes), F32),
        ),
        mib=24,
        flops=12 * count * width * lanes,
        bytes_accessed=8 * count * lanes,
        transcendentals=0,
    )
    near = copies(last, ("x", "c"))
    *merge_pieces, _ = lax.optimization_barrier((*merge_pieces, last))
    merge_x = jnp.stack(merge_pieces)
    merge_other = partner(merge_x)
    packed, prefix = call(
        functools.partial(near_kernel, count),
        (
            jax.ShapeDtypeStruct((1, 2 * lanes + 128), F32),
            jax.ShapeDtypeStruct((4, lanes), F32),
        ),
        (near, device["rates"]),
        scalars=(place,),
        mib=4,
        flops=100 * lanes,
        bytes_accessed=64 * lanes,
        transcendentals=8 * lanes,
    )
    far = copies(packed, "z")

    raw, sums = call(
        conv_kernel,
        (
            pltpu.HBM((count, width), F32),
            jax.ShapeDtypeStruct((2, count), F32),
        ),
        (conv_taps,),
        apart=far_from_core(normed, project_x, project_other),
        scalars=(place,),
        scratch=(
            *weight_scratch(project_x, 2 * width),
            *normed_scratch,
            pltpu.VMEM((rows + 8, width), F32),
            pltpu.VMEM((8, rows, width), F32),
        ),
        mib=20,
        flops=4 * count * depth * width,
        bytes_accessed=4 * depth * count,
        transcendentals=0,
    )
    all_sums = [sums] + [from_ahead(sums, "tp", d) for d in range(1, parts)]

    block = count // parts

    def products(kernel, blocks, more, arrays):
        return call(
            kernel,
            (jax.ShapeDtypeStruct((blocks, block, depth), BF16), *more),
            (channel_gain.reshape(1, -1), *all_sums, *arrays),
            apart=(*far_from_core(raw, y_local, power, reads), merge_x, merge_other),
            scalars=(place,),
            scratch=(
                *weight_scratch(merge_x, 2 * width),
                pltpu.VMEM((blocks, block, width), F32),
                pltpu.VMEM((blocks, block, width), F32),
                pltpu.VMEM((blocks, block, 2 * lanes), BF16),
                pltpu.VMEM((width, 2 * lanes), BF16),
                pltpu.SemaphoreType.DMA((1 + 3 * blocks,)),
            ),
            flops=4 * block * blocks * depth * width,
            bytes_accessed=4 * depth * count,
            transcendentals=0,
        )

    opposite, h = products(
        functools.partial(opposite_kernel, count),
        1,
        (jax.ShapeDtypeStruct((2, lanes), F32),),
        (far, device["rates"], prefix, start),
    )
    opposite = opposite[0]
    through_ahead = from_ahead(opposite[: block // 2], "tp", 1)
    through_behind = from_ahead(opposite[block // 2 :], "tp", -1)
    ((mine, to_ahead, to_behind),) = products(rest_kernel, 3, (), (h,))
    empty = jnp.zeros((block // 2, depth), F32)
    to_behind = to_behind.astype(F32) + jnp.concatenate([through_ahead.astype(F32), empty])
    to_ahead = to_ahead.astype(F32) + jnp.concatenate([empty, through_behind.astype(F32)])
    from_next = from_ahead(to_behind.astype(BF16), "tp", 1)
    from_last = from_ahead(to_ahead.astype(BF16), "tp", -1)
    return (mine.astype(F32) + from_next.astype(F32) + from_last.astype(F32)).astype(BF16)


def finer_mesh(mesh):
    cores = 2
    return Mesh(mesh.devices.reshape(16, 4, cores, mesh.shape["tp"]), SP_TP)


def solution(mesh):
    return jax.shard_map(
        mixer,
        mesh=finer_mesh(mesh),
        in_specs=(
            P(SP, "tp"),
            P(),
            P(SP, "tp"),
            P(SP, "tp"),
            P(SP, "tp"),
            P("tp", None),
            P("tp", None),
            P("tp"),
            P("tp", SP),
            P(None, "tp", None, None),
            P(None, "tp", None, None),
            P("tp"),
            P(None, "tp", None),
            P(None, "tp"),
            P("tp"),
            P("tp", SP),
            P("tp", SP),
        ),
        out_specs=P(SP_TP, None),
        check_vma=False,
    )
```
